128 devices in a mesh: sp: 16 (over z, x), tp: 8 (over y, core).
Axes of the slice: x: 4, y: 4, z: 4, core: 2. Of those that a mesh axis runs over, the one named last changes fastest.
Arguments:
- residual: bfloat16 [12288, 4096], P('sp', 'tp'), may hold values from -40 to 40
- values: bfloat16 [12288, 2048], P('sp', 'tp'), may hold values from -6 to 6
- forget_onward: bfloat16 [12288, 2048], P('sp', 'tp'), may hold values from -5.5 to 5.5
- forget_reverse: bfloat16 [12288, 2048], P('sp', 'tp'), may hold values from -5.5 to 5.5
- surge_log_decay: float32 [12288, 16], P('sp', 'tp'), may hold values from -2.1 to 0
- gate_limit_complement: float32 [2, 2048], P(None, 'tp'), may hold values from 2.4414062e-05 to 0.1
- readout_query: bfloat16 [12288, 2048], P('sp', 'tp'), may hold values from -6 to 6
- output_gate: bfloat16 [12288, 2048], P('sp', 'tp'), may hold values from -6 to 6
- head_norm_gain: float32 [128], replicated, may hold values from 0.1 to 1.9
- output_weight: bfloat16 [2048, 4096], P('tp'), may hold values from -0.125 to 0.125
- mixer_norm_gain: float32 [4096], replicated, may hold values from 0.1 to 1.9
- up_weight: bfloat16 [4096, 8192], P('sp', 'tp'), may hold values from -0.09375 to 0.09375
- down_weight: bfloat16 [4096, 8192], P('sp', 'tp'), may hold values from -0.0625 to 0.0625
Outputs:
- output: bfloat16 [12288, 4096], P('sp', 'tp')
The draws below stay inside these ranges and needn't reach their ends.
All inputs are finite; a program needn't handle non-finite values.
Results may differ from the reference program's by a relative error of at most 0.015.
Values may be sent and summed in bfloat16 or wider, within the bound.
A program may use at most 192 MiB of HBM per device.

```python
import math
import jax
import jax.numpy as jnp
from jax import lax

D = 4096
HEADS = 16
HEAD_DIM = 128
HGW = 2048
FF = 8192
TOK_DEV = 768
TOKENS = 12288
N_TP = 8


def draw_residual(key, part):
    key_one, key_two, key_three = jax.random.split(jax.random.fold_in(key, 11), 3)
    columns = jnp.arange(D, dtype=jnp.float32) / D
    col_power = 0.5 * columns + 0.5 * jax.random.uniform(key_one, (D,), jnp.float32) - 0.5
    row_power = jax.random.uniform(key_two, (TOKENS, 1), jnp.float32) - 0.5
    base_draw = jax.random.truncated_normal(key_three, -4.0, 4.0, (TOKENS, D), jnp.float32)
    return (base_draw * 10.0 ** (col_power[None, :] + row_power)).astype(jnp.bfloat16)


def forget_draw(key, salt):
    key_one, key_two = jax.random.split(jax.random.fold_in(key, salt))
    shards = TOKENS // TOK_DEV
    offset = jax.random.uniform(key_one, (shards, 1), jnp.float32, minval=-1.5, maxval=1.5)
    offset = jnp.repeat(offset, TOK_DEV, axis=0, total_repeat_length=TOKENS)
    base_draw = jax.random.truncated_normal(key_two, -4.0, 4.0, (TOKENS, HGW), jnp.float32)
    return (base_draw + offset).astype(jnp.bfloat16)


def draw_forget_onward(key, part):
    return forget_draw(key, 41)


def draw_forget_reverse(key, part):
    return forget_draw(key, 43)


def draw_gate_limit_complement(key, part):
    key_one, key_two, key_three = jax.random.split(jax.random.fold_in(key, 23), 3)
    slow_share = 0.5
    slow_heads = jax.random.uniform(key_one, (2, HEADS, 1), jnp.float32) < slow_share
    slow_gap = jnp.exp(jax.random.uniform(key_two, (2, HEADS, HEAD_DIM), jnp.float32, minval=math.log(0.3), maxval=math.log(1.5))) / TOKENS
    fast_gap = jnp.exp(jax.random.uniform(key_three, (2, HEADS, HEAD_DIM), jnp.float32, minval=math.log(0.04), maxval=math.log(0.1)))
    return jnp.where(slow_heads, slow_gap, fast_gap).reshape(2, HEADS * HEAD_DIM)


def draw_surge_log_decay(key, part):
    key_one, key_two = jax.random.split(jax.random.fold_in(key, 31))
    where_at = jax.random.randint(key_one, (3, HEADS), 0, TOKENS)
    strength = jax.random.uniform(key_two, (3, HEADS), jnp.float32, minval=math.log(0.5), maxval=math.log(0.8))
    positions = jnp.arange(TOKENS)[:, None]
    total = jnp.zeros((TOKENS, HEADS), jnp.float32)
    for turn_index in range(3):
        total = total + jnp.where(positions == where_at[turn_index][None, :], strength[turn_index][None, :], 0.0)
    return total


def block_levels(key, extent, cuts, least, high):
    loudness, own = 1.0, jax.random.fold_in(key, 6)
    for dim, parts in cuts:
        heights = jnp.exp(jax.random.uniform(jax.random.fold_in(own, dim), (parts,), jnp.float32, least / len(cuts), high / len(cuts)))
        loudness = loudness * jnp.repeat(heights, extent[dim] // parts).reshape([-1 if axis == dim else 1 for axis in range(len(extent))])
    return loudness


def centred(key, extent, spread, reach, cuts=(), kind=jnp.bfloat16):
    gain = block_levels(key, extent, cuts, -0.22, 0.18) if cuts else 1.0
    values = jax.random.normal(key, extent, jnp.float32) * spread * gain
    return jnp.minimum(jnp.maximum(values, -reach), reach).astype(kind)


def setup_inputs(seed: int = 0) -> dict:
    streams_of = jax.random.split(jax.random.key(seed), 14)
    return {
        "residual": draw_residual(jax.random.fold_in(streams_of[13], 71), 0),
        "values": centred(streams_of[1], (TOKENS, HGW), 1.0, 6.0, ((0, 16), (1, 8))),
        "forget_onward": draw_forget_onward(jax.random.fold_in(streams_of[13], 71), 0),
        "forget_reverse": draw_forget_reverse(jax.random.fold_in(streams_of[13], 71), 0),
        "surge_log_decay": draw_surge_log_decay(jax.random.fold_in(streams_of[13], 71), 0),
        "gate_limit_complement": draw_gate_limit_complement(jax.random.fold_in(streams_of[13], 71), 0),
        "readout_query": centred(streams_of[6], (TOKENS, HGW), 1.0, 6.0, ((0, 16), (1, 8))),
        "output_gate": centred(streams_of[7], (TOKENS, HGW), 1.0, 6.0, ((0, 16), (1, 8))),
        "head_norm_gain": jnp.clip(1.0 + 0.18 * jax.random.normal(streams_of[8], (HEAD_DIM,), jnp.float32), 0.1, 1.9),
        "output_weight": centred(streams_of[9], (HGW, D), HGW ** -0.5, 0.125, ((0, 8),)),
        "mixer_norm_gain": jnp.clip(1.0 + 0.18 * jax.random.normal(streams_of[10], (D,), jnp.float32), 0.1, 1.9),
        "up_weight": centred(streams_of[11], (D, FF), D ** -0.5, 0.09375, ((0, 16), (1, 8))),
        "down_weight": centred(streams_of[12], (D, FF), FF ** -0.5, 0.0625, ((0, 16), (1, 8))),
    }


epsilon = 1e-06
top_precision = lax.Precision.HIGHEST

def forget_gate_value(gate_logits, gate_lower_limit, surge_decay, head_layout):
    key_gate_random = gate_lower_limit[None, :] * jax.nn.sigmoid(-gate_logits.astype(jnp.float32))
    logarithm_decay = jnp.log1p(-key_gate_random).reshape(head_layout) + surge_decay
    return (key_gate_random.reshape(head_layout), logarithm_decay)

def sweep(queries, key_gate_random, value_rows, logarithm_decay):

    def advance(memory_state, item):
        query_at_step, key_t, value_t, decay_t = item
        memory_state = jnp.exp(decay_t)[:, :, None] * memory_state + key_t[:, :, None] * value_t[:, None, :]
        return (memory_state, jnp.einsum('mw,mwp->mp', query_at_step, memory_state, precision=top_precision))
    initial = jnp.zeros((HEADS, HEAD_DIM, HEAD_DIM), jnp.float32)
    _, outputs = lax.scan(advance, initial, (queries, key_gate_random, value_rows, logarithm_decay))
    return outputs

def grouped_sum(left, right, right_axis):
    span = left.shape[1] // N_TP
    total = jnp.zeros((left.shape[0], right.shape[1 - right_axis]), jnp.float32)
    for group in range(N_TP):
        piece = left[:, group * span:(group + 1) * span]
        if right_axis == 0:
            weight = right[group * span:(group + 1) * span]
            dims = (((1,), (0,)), ((), ()))
        else:
            weight = right[:, group * span:(group + 1) * span]
            dims = (((1,), (1,)), ((), ()))
        term = lax.dot_general(piece, weight, dims, preferred_element_type=jnp.float32)
        total = total + lax.optimization_barrier(term.astype(jnp.bfloat16)).astype(jnp.float32)
    return total

def reference(residual, values, forget_onward, forget_reverse, surge_log_decay, gate_limit_complement, readout_query, output_gate, head_norm_gain, output_weight, mixer_norm_gain, up_weight, down_weight):
    tokens = residual.shape[0]
    head_layout = (tokens, HEADS, HEAD_DIM)
    queries = (jax.nn.silu(readout_query.astype(jnp.float32)) * HEAD_DIM ** (-0.5)).reshape(head_layout)
    value_rows = values.astype(jnp.float32).reshape(head_layout)
    surge_decay = surge_log_decay[:, :, None]
    key_onward, logarithm_onward = forget_gate_value(forget_onward, gate_limit_complement[0], surge_decay, head_layout)
    key_reverse, logarithm_reverse = forget_gate_value(forget_reverse, gate_limit_complement[1], surge_decay, head_layout)
    forward = sweep(queries, key_onward, value_rows, logarithm_onward)
    backward = jnp.flip(sweep(jnp.flip(queries, 0), jnp.flip(key_reverse, 0), jnp.flip(value_rows, 0), jnp.flip(logarithm_reverse, 0)), 0)
    mixed_out = forward + backward
    normed = mixed_out * lax.rsqrt(lax.optimization_barrier(jnp.mean(mixed_out * mixed_out, axis=-1, keepdims=True)) + epsilon) * head_norm_gain
    gated_rows = (normed.reshape(tokens, HEADS * HEAD_DIM) * jax.nn.silu(output_gate.astype(jnp.float32))).astype(jnp.bfloat16)
    attention = grouped_sum(gated_rows, output_weight, 0)
    middle = (residual.astype(jnp.float32) + attention).astype(jnp.bfloat16)
    middle_f = middle.astype(jnp.float32)
    scale_rows = lax.rsqrt(lax.optimization_barrier(jnp.mean(middle_f * middle_f, axis=1, keepdims=True)) + epsilon)
    normalized = (middle_f * scale_rows * mixer_norm_gain).astype(jnp.bfloat16)
    lifted = jnp.dot(normalized, up_weight, preferred_element_type=jnp.float32)
    hidden = jnp.square(jax.nn.relu(lifted)).astype(jnp.bfloat16)
    channel = grouped_sum(hidden, down_weight, 1)
    return (middle_f + channel).astype(jnp.bfloat16)
```

```python
import functools

import jax
import jax.numpy as jnp
from jax import lax
from jax.experimental import pallas as pl
from jax.experimental.pallas import tpu as pltpu
from jax.sharding import PartitionSpec as P

D = 4096
HD = 128
HEADS = 2
CH = HEADS * HD
TOK = 768
BLK = 64
NB = TOK // BLK
OC = 512
FFL = 1024
SHARD = 256
QUARTER = 64
EPS = 1e-06
MESH = pl.DeviceIdType.MESH
F32 = jnp.float32
BF16 = jnp.bfloat16
ST_ROWS = 272


def dot(a, b, dims=(((1,), (0,)), ((), ()))):
    return lax.dot_general(a, b, dims, preferred_element_type=F32)


LAST = (((1,), (1,)), ((), ()))
FIRST = (((0,), (0,)), ((), ()))


def sigmoid(x):
    return 1.0 / (1.0 + jnp.exp(-x))


def kernel(
    residual, values, f_on, f_rev, surge, glc, query, gate, head_gain, out_w,
    norm_gain, up_w, down_w,
    out,
    res_v, val_v, fon_v, frev_v, sur_v, glc_v, que_v, gat_v, hg_v, ng_v,
    wu, wd, owc, ga, xa,
    qd, kr, sx, em, elx, run_state, run_log, st, st_in, sin, o_v, att,
    xg, ss, acc, hid,
    d2s, d2r, cs, ra, e1, e2,
    in_sem, w_send, w_recv, ow_send, ow_recv, st_send, st_recv,
    g_send, g_recv, x_send, x_recv, c_send, c_recv, r_send, r_recv, e_send, e_recv,
):
    sp, tp = lax.axis_index("sp"), lax.axis_index("tp")
    x, z = lax.rem(sp, 4), lax.div(sp, 4)
    core, y = lax.rem(tp, 2), lax.div(tp, 2)
    other = 1 - core

    def ring(v, k):
        return lax.rem(v + (k % 4), 4)

    yp, ym, y2 = ring(y, 1), ring(y, 3), ring(y, 2)
    partner = 2 * y + other

    barrier = pltpu.get_barrier_semaphore()
    for o in range(1, 16):
        pl.semaphore_signal(barrier, inc=1, device_id=(lax.rem(sp + o, 16), tp), device_id_type=MESH)
    for o in range(1, 8):
        pl.semaphore_signal(barrier, inc=1, device_id=(sp, lax.rem(tp + o, 8)), device_id_type=MESH)

    own_rows = pl.ds(pl.multiple_of(sp * SHARD, SHARD), SHARD)
    ow_rows = pl.ds(pl.multiple_of(tp * 256, 256), 256)
    own_cols = pl.ds(pl.multiple_of(tp * OC, OC), OC)
    loads = [
        (f_on, fon_v), (f_rev, frev_v), (surge, sur_v), (glc, glc_v), (query, que_v),
        (values, val_v), (gate, gat_v), (head_gain, hg_v), (residual, res_v), (norm_gain, ng_v),
        (up_w, wu.at[own_rows]), (down_w, wd.at[own_rows]),
        (out_w.at[:, own_cols], owc.at[ow_rows]),
    ]
    loads = [pltpu.make_async_copy(a, b, in_sem.at[i]) for i, (a, b) in enumerate(loads)]
    for copy in loads:
        copy.start()

    pl.semaphore_wait(barrier, 22)

    def remote(src, dst, ss_, rs_, dev):
        return pltpu.make_async_remote_copy(
            src_ref=src, dst_ref=dst, send_sem=ss_, recv_sem=rs_, device_id=dev, device_id_type=MESH
        )

    started = []

    def send(*args):
        copy = remote(*args)
        copy.start()
        started.append(copy)

    weights = ((up_w, wu), (down_w, wd))

    def sp_at(half, i, j):
        return ring(z, j) * 4 + ring(x, i) if half == 0 else ring(z, i) * 4 + ring(x, j)

    def piece(t, half, i, j, part):
        start, size = (0, 2 * QUARTER) if part is None else (part * QUARTER, QUARTER)
        first = sp_at(half, i, j) * SHARD + half * 2 * QUARTER + start
        return weights[t][1].at[pl.ds(pl.multiple_of(first, QUARTER), size)]

    FWD = (0, -1, 1, 2)

    def w_copy(t, half, slot, i, j, part, to, src=None):
        ref = piece(t, half, i, j, part)
        return remote(
            ref if src is None else src, ref, w_send.at[t, half, slot], w_recv.at[t, half, slot],
            (sp_at(half, *to), tp),
        )

    def w_go(*args, **kw):
        copy = w_copy(*args, **kw)
        copy.start()
        started.append(copy)

    def w_got(t, half, slot, i, j, part):
        w_copy(t, half, slot, i, j, part, (1, 0)).wait_recv()

    def w_second(t, half, n, src=None):
        i = FWD[n]
        w_go(t, half, 4 + 4 * n, i, 0, None, (0, 1), src=src)
        w_go(t, half, 5 + 4 * n, i, 0, None, (0, -1), src=src)

    def w_second_forward(t, half, n):
        i = FWD[n]
        w_got(t, half, 4 + 4 * n, i, -1, None)
        w_go(t, half, 6 + 4 * n, i, -1, 0, (0, 1))
        w_got(t, half, 5 + 4 * n, i, 1, None)
        w_go(t, half, 7 + 4 * n, i, 1, 1, (0, -1))

    def level0(t):
        for half in range(2):
            src = weights[t][0].at[pl.ds(half * 2 * QUARTER, 2 * QUARTER)]
            w_go(t, half, 0, 0, 0, None, (1, 0), src=src)
            w_go(t, half, 1, 0, 0, None, (-1, 0), src=src)
        for half in range(2):
            src = weights[t][0].at[pl.ds(half * 2 * QUARTER, 2 * QUARTER)]
            w_second(t, half, 0, src=src)

    def level1(t):
        for half in range(2):
            w_got(t, half, 0, -1, 0, None)
            w_go(t, half, 2, -1, 0, 0, (1, 0))
            w_got(t, half, 1, 1, 0, None)
            w_go(t, half, 3, 1, 0, 1, (-1, 0))
        for half in range(2):
            w_second(t, half, 1)
            w_second(t, half, 2)
        for half in range(2):
            w_second_forward(t, half, 0)

    def level2(t):
        for half in range(2):
            w_got(t, half, 2, 2, 0, 0)
            w_got(t, half, 3, 2, 0, 1)
            w_second(t, half, 3)
        for half in range(2):
            w_second_forward(t, half, 1)
            w_second_forward(t, half, 2)

    def level3(t):
        for half in range(2):
            w_second_forward(t, half, 3)

    def level4(t):
        for half in range(2):
            for n in range(4):
                w_got(t, half, 6 + 4 * n, FWD[n], 2, 0)
                w_got(t, half, 7 + 4 * n, FWD[n], 2, 1)

    level0(0)

    def ow_copy(o):
        to = lax.rem(tp + o, 8)
        return remote(
            out_w.at[:, pl.ds(pl.multiple_of(to * OC, OC), OC)], owc.at[ow_rows],
            ow_send.at[o - 1], ow_recv.at[o - 1], (sp, to),
        )

    for o in range(1, 8):
        copy = ow_copy(o)
        copy.start()
        started.append(copy)

    for copy in loads[:7]:
        copy.wait()

    row_id = lax.broadcasted_iota(jnp.int32, (BLK, BLK), 0)
    col_id = lax.broadcasted_iota(jnp.int32, (BLK, BLK), 1)
    lower, upper = row_id >= col_id, row_id <= col_id
    run_state[...] = jnp.zeros_like(run_state)
    run_log[...] = jnp.zeros_like(run_log)

    def pass1(step, carry):
        for d, (logits, tri, mid_at, end_at) in enumerate(
            ((fon_v, lower, BLK // 2 - 1, BLK - 1), (frev_v, upper, BLK // 2, 0))
        ):
            blk = step if d == 0 else NB - 1 - step
            rows = pl.ds(pl.multiple_of(blk * BLK, BLK), BLK)
            key = glc_v[d : d + 1, :] / (1.0 + jnp.exp(logits[rows, :].astype(F32)))
            sg = sur_v[rows, :]
            sg = jnp.concatenate(
                [jnp.broadcast_to(sg[:, h : h + 1], (BLK, HD)) for h in range(HEADS)], axis=1
            )
            logs = jnp.log1p(-key) + sg
            run = lax.dot_general(
                jnp.where(tri, 1.0, 0.0).astype(F32), logs, (((1,), (0,)), ((), ())),
                precision=lax.Precision.HIGHEST, preferred_element_type=F32,
            )
            mid, end = run[mid_at : mid_at + 1, :], run[end_at : end_at + 1, :]
            q = que_v[rows, :].astype(F32)
            q = q * sigmoid(q) * (HD ** -0.5)
            qd[d, rows, :] = (q * jnp.exp(run - mid)).astype(BF16)
            k = key * jnp.exp(mid - run)
            kr[d, rows, :] = k.astype(BF16)
            tail = (k * jnp.exp(end - mid)).astype(BF16)
            v = val_v[rows, :]
            gone = run_log[d, 0:1, :]
            em[d, blk] = jnp.broadcast_to(jnp.exp(mid), (8, CH))
            elx[d, blk] = jnp.broadcast_to(jnp.exp(gone), (8, CH))
            run_log[d] = jnp.broadcast_to(gone + end, (8, CH))
            decay = jnp.exp(end)
            for h in range(HEADS):
                hs = slice(h * HD, (h + 1) * HD)
                state = run_state[d, hs, :]
                sx[d, blk, hs, :] = state.astype(BF16)
                run_state[d, hs, :] = state * decay[:, hs] + dot(v[:, hs], tail[:, hs], FIRST)
        return carry

    lax.fori_loop(0, NB, pass1, 0)

    for d in range(2):
        st[d, 0:CH, :] = run_state[d].astype(BF16)
        total = run_log[d, 0:1, :]
        high = total.astype(BF16).astype(F32)
        low = total - high
        st[d, CH:ST_ROWS, :] = jnp.concatenate(
            [high[:, :HD], high[:, HD:], low[:, :HD], low[:, HD:], jnp.zeros((12, HD), F32)], axis=0
        ).astype(BF16)

    def st_copy(o):
        return remote(
            st.at[lax.div(sp + o, 16)], st_in.at[o - 1], st_send.at[o - 1], st_recv.at[o - 1],
            (lax.rem(sp + o, 16), tp),
        )

    for o in range(1, 16):
        copy = st_copy(o)
        copy.start()
        started.append(copy)

    def pass2(blk, carry):
        rows = pl.ds(pl.multiple_of(blk * BLK, BLK), BLK)
        v = val_v[rows, :]
        for h in range(HEADS):
            hs = slice(h * HD, (h + 1) * HD)
            fwd = dot(qd[0, rows, hs], kr[0, rows, hs], LAST)
            bwd = dot(qd[1, rows, hs], kr[1, rows, hs], LAST)
            score = jnp.where(lower, fwd, 0.0) + jnp.where(upper, bwd, 0.0)
            o_v[rows, hs] = dot(score.astype(BF16), v[:, hs])
        return carry

    lax.fori_loop(0, NB, pass2, 0)

    level1(0)
    level0(1)

    sin[...] = jnp.zeros_like(sin)
    for o in range(1, 16):
        st_copy(o).wait_recv()

    def combine(i, carry):
        d = lax.div(i + 16 - sp, 16)
        slot = (1 - d) * (sp - 1 - i) + d * i
        tail = st_in[slot, CH:ST_ROWS, :].astype(F32)
        for h in range(HEADS):
            hs = slice(h * HD, (h + 1) * HD)
            decay = jnp.exp(tail[h : h + 1, :] + tail[2 + h : 3 + h, :])
            sin[d, hs, :] = sin[d, hs, :] * decay + st_in[slot, hs, :].astype(F32)
        return carry

    lax.fori_loop(0, 15, combine, 0)

    for copy in loads[6:10]:
        if copy is not loads[6]:
            copy.wait()

    def pass3(blk, carry):
        rows = pl.ds(pl.multiple_of(blk * BLK, BLK), BLK)
        for h in range(HEADS):
            hs = slice(h * HD, (h + 1) * HD)
            mixed = o_v[rows, hs]
            for d in range(2):
                qs = (qd[d, rows, hs].astype(F32) * em[d, blk, 0:1, hs]).astype(BF16)
                state = sx[d, blk, hs, :].astype(F32) + elx[d, blk, 0:1, hs] * sin[d, hs, :]
                mixed = mixed + dot(qs, state.astype(BF16), LAST)
            norm = mixed * lax.rsqrt(jnp.mean(mixed * mixed, axis=-1, keepdims=True) + EPS)
            g = gat_v[rows, hs].astype(F32)
            ga[tp, rows, hs] = (norm * hg_v[0:1, :] * (g * sigmoid(g))).astype(BF16)
        return carry

    lax.fori_loop(0, NB, pass3, 0)

    HALF = TOK // 2

    class Gather:
        def __init__(self, buf, send_sem, recv_sem):
            self.buf, self.ss, self.rs = buf, send_sem, recv_sem

        def copy(self, k, slot, part, to):
            ref = self.buf.at[slot]
            if part is not None:
                ref = self.buf.at[slot, pl.ds(part * HALF, HALF)]
            return remote(ref, ref, self.ss.at[k], self.rs.at[k], (sp, to))

        def go(self, *args):
            copy = self.copy(*args)
            copy.start()
            started.append(copy)

        def got(self, k, slot, part):
            self.copy(k, slot, part, partner).wait_recv()

        def own(self):
            self.go(0, tp, None, 2 * yp + core)
            self.go(1, tp, None, 2 * ym + core)
            self.go(4, tp, None, partner)

        def from_side(self):
            left, right = 2 * ym + core, 2 * yp + core
            self.got(0, left, None)
            self.go(2, left, 0, right)
            self.go(5, left, None, partner)
            self.got(1, right, None)
            self.go(3, right, 1, left)
            self.go(6, right, None, partner)

        def from_far(self):
            far = 2 * y2 + core
            self.got(2, far, 0)
            self.go(7, far, 0, partner)
            self.got(3, far, 1)
            self.go(8, far, 1, partner)

    gathered = Gather(ga, g_send, g_recv)
    gathered.own()

    for copy in loads[10:13]:
        copy.wait()
    for o in range(1, 8):
        ow_copy(o).wait_recv()

    def project(block, first=False):
        def tile(n, carry):
            cols = pl.ds(pl.multiple_of(n * 256, 256), 256)
            part = dot(ga[block], owc[pl.ds(pl.multiple_of(block * 256, 256), 256), cols])
            att[:, cols] = part if first else att[:, cols] + part
            return carry

        lax.fori_loop(0, OC // 256, tile, 0)

    project(tp, True)
    gathered.got(4, partner, None)
    project(partner)
    gathered.from_side()
    project(2 * ym + core)
    project(2 * yp + core)
    level2(0)
    level1(1)
    gathered.got(5, 2 * ym + other, None)
    project(2 * ym + other)
    gathered.got(6, 2 * yp + other, None)
    project(2 * yp + other)
    gathered.from_far()
    project(2 * y2 + core)
    gathered.got(7, 2 * y2 + other, 0)
    gathered.got(8, 2 * y2 + other, 1)
    project(2 * y2 + other)

    TILE = 128

    def middle(i, carry):
        rows = pl.ds(pl.multiple_of(i * TILE, TILE), TILE)
        xa[tp, rows, :] = (res_v[rows, :].astype(F32) + att[rows, :]).astype(BF16)
        return carry

    lax.fori_loop(0, TOK // TILE, middle, 0)

    spread = Gather(xa, x_send, x_recv)
    spread.own()
    level3(0)
    level2(1)
    level4(0)

    def lift(block, first=False):
        gain = ng_v[pl.ds(block, 1), :]

        def scale(i, carry):
            rows = pl.ds(pl.multiple_of(i * TILE, TILE), TILE)
            v = xa[block, rows, :].astype(F32)
            sq = v * v
            sq = (sq[:, 0:128] + sq[:, 128:256]) + (sq[:, 256:384] + sq[:, 384:512])
            ss[rows, :] = sq if first else ss[rows, :] + sq
            xg[rows, :] = (v * gain).astype(BF16)
            return carry

        lax.fori_loop(0, TOK // TILE, scale, 0)

        def tile(n, carry):
            cols = pl.ds(pl.multiple_of(n * 256, 256), 256)
            part = dot(xg[...], wu[pl.ds(pl.multiple_of(block * OC, OC), OC), cols])
            acc[:, cols] = part if first else acc[:, cols] + part
            return carry

        lax.fori_loop(0, FFL // 256, tile, 0)

    lift(tp, True)
    spread.got(4, partner, None)
    lift(partner)
    spread.from_side()
    lift(2 * ym + core)
    lift(2 * yp + core)
    spread.got(5, 2 * ym + other, None)
    lift(2 * ym + other)
    spread.got(6, 2 * yp + other, None)
    lift(2 * yp + other)
    spread.from_far()
    lift(2 * y2 + core)
    spread.got(7, 2 * y2 + other, 0)
    spread.got(8, 2 * y2 + other, 1)
    lift(2 * y2 + other)

    def activate(i, carry):
        rows = pl.ds(pl.multiple_of(i * TILE, TILE), TILE)
        total = jnp.sum(ss[rows, :], axis=-1, keepdims=True)
        v = jnp.maximum(acc[rows, :] * lax.rsqrt(total / D + EPS), 0.0)
        hid[rows, :] = (v * v).astype(BF16)
        return carry

    lax.fori_loop(0, TOK // TILE, activate, 0)

    level3(1)
    level4(1)

    def down(dest, to_ref):
        def tile(n, carry):
            cols = pl.ds(pl.multiple_of(n * 256, 256), 256)
            first = pl.multiple_of(dest * OC + n * 256, 256)
            to_ref[:, cols] = dot(hid[...], wd[pl.ds(first, 256), :], LAST).astype(BF16)
            return carry

        lax.fori_loop(0, OC // 256, tile, 0)

    def c_copy(n):
        return remote(d2s.at[n], d2r.at[n], c_send.at[n], c_recv.at[n], (sp, partner))

    def chip_sum(n):
        c_copy(n).wait_recv()

        def add(i, carry):
            rows = pl.ds(pl.multiple_of(i * TILE, TILE), TILE)
            cs[n, rows, :] = (cs[n, rows, :].astype(F32) + d2r[n, rows, :].astype(F32)).astype(BF16)
            return carry

        lax.fori_loop(0, TOK // TILE, add, 0)

    dests = (y2, yp, ym, y)

    def pair(n):
        down(2 * dests[n] + other, d2s.at[n])
        copy = c_copy(n)
        copy.start()
        started.append(copy)
        down(2 * dests[n] + core, cs.at[n])

    low, high = pl.ds(0, HALF), pl.ds(HALF, HALF)
    right, left = (sp, 2 * yp + core), (sp, 2 * ym + core)

    def r_copy(k):
        half, to = ((low, right), (high, left))[k]
        return remote(cs.at[0, half], ra.at[k], r_send.at[k], r_recv.at[k], to)

    def e_copy(k):
        n, buf, half, to = (
            (1, e1, high, right), (2, e2, low, left), (1, e1, low, right), (2, e2, high, left)
        )[k]
        return remote(cs.at[n, half], buf.at[half], e_send.at[k], e_recv.at[k], to)

    def go(copy):
        copy.start()
        started.append(copy)

    pair(0)
    pair(1)
    chip_sum(0)
    go(r_copy(0))
    go(r_copy(1))
    pair(2)
    chip_sum(1)
    go(e_copy(0))
    chip_sum(2)
    go(e_copy(1))
    pair(3)

    def join(k):
        r_copy(k).wait_recv()
        n = 1 + k

        def add(i, carry):
            rows = pl.ds(pl.multiple_of(k * HALF + i * TILE, TILE), TILE)
            got = ra[k, pl.ds(pl.multiple_of(i * TILE, TILE), TILE), :]
            cs[n, rows, :] = (cs[n, rows, :].astype(F32) + got.astype(F32)).astype(BF16)
            return carry

        lax.fori_loop(0, HALF // TILE, add, 0)

    join(0)
    go(e_copy(2))
    join(1)
    go(e_copy(3))

    c_copy(3).wait_recv()
    for k in range(4):
        e_copy(k).wait_recv()

    def finish(i, carry):
        rows = pl.ds(pl.multiple_of(i * TILE, TILE), TILE)
        total = cs[3, rows, :].astype(F32) + d2r[3, rows, :].astype(F32)
        total = total + (e1[rows, :].astype(F32) + e2[rows, :].astype(F32))
        res_v[rows, :] = (xa[tp, rows, :].astype(F32) + total).astype(BF16)
        return carry

    lax.fori_loop(0, TOK // TILE, finish, 0)
    final = pltpu.make_async_copy(res_v, out, in_sem.at[0])
    final.start()
    for copy in started:
        copy.wait_send()
    final.wait()


def per_device(
    residual, values, forget_onward, forget_reverse, surge_log_decay, gate_limit_complement,
    readout_query, output_gate, head_norm_gain, output_weight, mixer_norm_gain, up_weight,
    down_weight,
):
    any_spec = pl.BlockSpec(memory_space=pl.ANY)
    vmem, dma = pltpu.VMEM, pltpu.SemaphoreType.DMA
    scratch = [
        vmem((TOK, OC), BF16), vmem((TOK, CH), BF16), vmem((TOK, CH), BF16), vmem((TOK, CH), BF16),
        vmem((TOK, HEADS), F32), vmem((2, CH), F32), vmem((TOK, CH), BF16), vmem((TOK, CH), BF16),
        vmem((1, HD), F32), vmem((8, OC), F32),
        vmem((D, FFL), BF16), vmem((D, FFL), BF16), vmem((2048, OC), BF16),
        vmem((8, TOK, CH), BF16), vmem((8, TOK, OC), BF16),
        vmem((2, TOK, CH), BF16), vmem((2, TOK, CH), BF16), vmem((2, NB, CH, HD), BF16),
        vmem((2, NB, 8, CH), F32), vmem((2, NB, 8, CH), F32),
        vmem((2, CH, HD), F32), vmem((2, 8, CH), F32),
        vmem((2, ST_ROWS, HD), BF16), vmem((15, ST_ROWS, HD), BF16), vmem((2, CH, HD), F32),
        vmem((TOK, CH), F32), vmem((TOK, OC), F32),
        vmem((TOK, OC), BF16), vmem((TOK, HD), F32), vmem((TOK, FFL), F32), vmem((TOK, FFL), BF16),
        vmem((4, TOK, OC), BF16), vmem((4, TOK, OC), BF16), vmem((4, TOK, OC), BF16),
        vmem((2, TOK // 2, OC), BF16), vmem((TOK, OC), BF16), vmem((TOK, OC), BF16),
        dma((13,)), dma((2, 2, 20)), dma((2, 2, 20)), dma((7,)), dma((7,)), dma((15,)), dma((15,)),
        dma((9,)), dma((9,)), dma((9,)), dma((9,)), dma((4,)), dma((4,)), dma((2,)), dma((2,)),
        dma((4,)), dma((4,)),
    ]
    return pl.pallas_call(
        kernel,
        out_shape=jax.ShapeDtypeStruct((TOK, OC), BF16),
        in_specs=[any_spec] * 13,
        out_specs=any_spec,
        scratch_shapes=scratch,
        compiler_params=pltpu.CompilerParams(
            collective_id=0, has_side_effects=True, vmem_limit_bytes=66_000_000
        ),
        name="layer",
    )(
        residual, values, forget_onward, forget_reverse, surge_log_decay, gate_limit_complement,
        readout_query, output_gate, head_norm_gain.reshape(1, HD), output_weight,
        mixer_norm_gain.reshape(8, OC), up_weight, down_weight,
    )


def solution(mesh):
    both = P("sp", "tp")
    placed = (
        both, both, both, both, both, P(None, "tp"), both, both, P(), P("tp", None), P(), both, both,
    )
    return jax.shard_map(
        per_device, mesh=mesh, in_specs=placed, out_specs=both, check_vma=False
    )
```

```python
import functools

import jax
import jax.numpy as jnp
from jax import lax
from jax.experimental import pallas as pl
from jax.experimental.pallas import tpu as pltpu
from jax.sharding import PartitionSpec as P

D = 4096
HD = 128
HEADS = 2
CH = HEADS * HD
TOK = 768
BLK = 64
UNROLL = 3
NB = TOK // BLK
OC = 512
FFL = 1024
SHARD = 256
QUARTER = 64
EPS = 1e-06
MESH = pl.DeviceIdType.MESH
F32 = jnp.float32
BF16 = jnp.bfloat16
ST_ROWS = 272


def dot(a, b, dims=(((1,), (0,)), ((), ()))):
    return lax.dot_general(a, b, dims, preferred_element_type=F32)


LAST = (((1,), (1,)), ((), ()))
FIRST = (((0,), (0,)), ((), ()))


def sigmoid(x):
    return 1.0 / (1.0 + jnp.exp(-x))


def kernel(
    residual, values, f_on, f_rev, surge, glc, query, gate, head_gain, out_w,
    norm_gain, up_w, down_w,
    out,
    res_v, val_v, fon_v, frev_v, sur_t, sur_v, glc_v, que_v, gat_v, hg_v, ng_v,
    wu, wd, owc, ga, xa,
    qd, kr, sx, em, elx, run_state, run_log, row_in, col_in, sin, o_v, att,
    xg, ss, acc, hid,
    pp, d2r, ra, ee,
    in_sem, w_send, w_recv, ow_send, ow_recv, st_send, st_recv,
    g_send, g_recv, x_send, x_recv, c_send, c_recv, r_send, r_recv, e_send, e_recv,
):
    sp, tp = lax.axis_index("sp"), lax.axis_index("tp")
    x, z = lax.rem(sp, 4), lax.div(sp, 4)
    core, y = lax.rem(tp, 2), lax.div(tp, 2)
    other = 1 - core

    cur = [None]

    def mark(name):
        if cur[0] is not None:
            cur[0].__exit__(None, None, None)
        cur[0] = jax.named_scope(name) if name else None
        if name:
            cur[0].__enter__()

    mark("start")

    def ring(v, k):
        return lax.rem(v + (k % 4), 4)

    yp, ym, y2 = ring(y, 1), ring(y, 3), ring(y, 2)
    partner = 2 * y + other

    barrier = pltpu.get_barrier_semaphore()
    for o in range(1, 16):
        pl.semaphore_signal(barrier, inc=1, device_id=(lax.rem(sp + o, 16), tp), device_id_type=MESH)
    for o in range(1, 8):
        pl.semaphore_signal(barrier, inc=1, device_id=(sp, lax.rem(tp + o, 8)), device_id_type=MESH)

    own_rows = pl.ds(pl.multiple_of(sp * SHARD, SHARD), SHARD)
    ow_rows = pl.ds(pl.multiple_of(tp * 256, 256), 256)
    own_cols = pl.ds(pl.multiple_of(tp * OC, OC), OC)
    loads = [
        (f_on, fon_v), (f_rev, frev_v), (surge, sur_t.at[pl.ds(0, HEADS)]), (glc, glc_v), (query, que_v),
        (values, val_v), (gate, gat_v), (head_gain, hg_v), (residual, res_v), (norm_gain, ng_v),
        (up_w, wu.at[own_rows]), (down_w, wd.at[own_rows]),
        (out_w.at[:, own_cols], owc.at[ow_rows]),
    ]
    loads = [pltpu.make_async_copy(a, b, in_sem.at[i]) for i, (a, b) in enumerate(loads)]
    for copy in loads:
        copy.start()

    pl.semaphore_wait(barrier, 22)

    def remote(src, dst, ss_, rs_, dev):
        return pltpu.make_async_remote_copy(
            src_ref=src, dst_ref=dst, send_sem=ss_, recv_sem=rs_, device_id=dev, device_id_type=MESH
        )

    started = []

    def send(*args):
        copy = remote(*args)
        copy.start()
        started.append(copy)

    weights = ((up_w, wu), (down_w, wd))

    def sp_at(half, i, j):
        return ring(z, j) * 4 + ring(x, i) if half == 0 else ring(z, i) * 4 + ring(x, j)

    def piece(t, half, i, j, part):
        start, size = (0, 2 * QUARTER) if part is None else (part * QUARTER, QUARTER)
        first = sp_at(half, i, j) * SHARD + half * 2 * QUARTER + start
        return weights[t][1].at[pl.ds(pl.multiple_of(first, QUARTER), size)]

    FWD = (0, -1, 1, 2)

    def w_copy(t, half, slot, i, j, part, to, src=None):
        ref = piece(t, half, i, j, part)
        return remote(
            ref if src is None else src, ref, w_send.at[t, half, slot], w_recv.at[t, half, slot],
            (sp_at(half, *to), tp),
        )

    def w_go(*args, **kw):
        copy = w_copy(*args, **kw)
        copy.start()
        started.append(copy)

    def w_got(t, half, slot, i, j, part):
        w_copy(t, half, slot, i, j, part, (1, 0)).wait_recv()

    def w_second(t, half, n, src=None):
        i = FWD[n]
        w_go(t, half, 4 + 4 * n, i, 0, None, (0, 1), src=src)
        w_go(t, half, 5 + 4 * n, i, 0, None, (0, -1), src=src)

    def w_second_forward(t, half, n):
        i = FWD[n]
        w_got(t, half, 4 + 4 * n, i, -1, None)
        w_go(t, half, 6 + 4 * n, i, -1, 0, (0, 1))
        w_got(t, half, 5 + 4 * n, i, 1, None)
        w_go(t, half, 7 + 4 * n, i, 1, 1, (0, -1))

    def level0a(t):
        for half in range(2):
            src = weights[t][0].at[pl.ds(half * 2 * QUARTER, 2 * QUARTER)]
            w_go(t, half, 0, 0, 0, None, (1, 0), src=src)
            w_go(t, half, 1, 0, 0, None, (-1, 0), src=src)

    def level0b(t, half):
        src = weights[t][0].at[pl.ds(half * 2 * QUARTER, 2 * QUARTER)]
        w_second(t, half, 0, src=src)

    def level1a(t):
        for half in range(2):
            w_got(t, half, 0, -1, 0, None)
            w_go(t, half, 2, -1, 0, 0, (1, 0))
            w_got(t, half, 1, 1, 0, None)
            w_go(t, half, 3, 1, 0, 1, (-1, 0))
        for half in range(2):
            w_second(t, half, 1)
            w_second(t, half, 2)

    def level1b(t):
        for half in range(2):
            w_second_forward(t, half, 0)

    def level2(t):
        for half in range(2):
            w_got(t, half, 2, 2, 0, 0)
            w_got(t, half, 3, 2, 0, 1)
            w_second(t, half, 3)
        for half in range(2):
            w_second_forward(t, half, 1)
            w_second_forward(t, half, 2)

    def level3(t):
        for half in range(2):
            w_second_forward(t, half, 3)

    def level4(t, blocks=(0, 1, 2, 3)):
        for half in range(2):
            for n in blocks:
                w_got(t, half, 6 + 4 * n, FWD[n], 2, 0)
                w_got(t, half, 7 + 4 * n, FWD[n], 2, 1)

    mark("w0")
    level0a(0)

    def ow_copy(o):
        to = lax.rem(tp + o, 8)
        return remote(
            out_w.at[:, pl.ds(pl.multiple_of(to * OC, OC), OC)], owc.at[ow_rows],
            ow_send.at[o - 1], ow_recv.at[o - 1], (sp, to),
        )

    for o in range(1, 8):
        copy = ow_copy(o)
        copy.start()
        started.append(copy)

    mark("loadwait")
    for copy in loads[:7]:
        copy.wait()

    mark("pass1")
    row_id = lax.broadcasted_iota(jnp.int32, (BLK, BLK), 0)
    col_id = lax.broadcasted_iota(jnp.int32, (BLK, BLK), 1)
    lower, upper = row_id >= col_id, row_id <= col_id
    run_state[...] = jnp.zeros_like(run_state)
    run_log[...] = jnp.zeros_like(run_log)
    sur_v[...] = jnp.concatenate([sur_t[0:HEADS, :], jnp.zeros((8 - HEADS, TOK), F32)], axis=0).T
    sums = tuple(
        jnp.concatenate([jnp.where(tri, 1.0, 0.0)] * 3, axis=1).astype(BF16) for tri in (lower, upper)
    )

    def split3(v):
        a = v.astype(BF16)
        rest = v - a.astype(F32)
        b = rest.astype(BF16)
        return jnp.concatenate([a, b, (rest - b.astype(F32)).astype(BF16)], axis=0)

    def pass1_block(d, blk):
        logits = (fon_v, frev_v)[d]
        mid_at, end_at = ((BLK // 2 - 1, BLK - 1), (BLK // 2, 0))[d]
        rows = pl.ds(pl.multiple_of(blk * BLK, BLK), BLK)
        key = glc_v[d : d + 1, :] / (1.0 + jnp.exp(logits[rows, :].astype(F32)))
        sg = sur_v[rows, :]
        sg = jnp.concatenate(
            [jnp.broadcast_to(sg[:, h : h + 1], (BLK, HD)) for h in range(HEADS)], axis=1
        )
        run = dot(sums[d], split3(jnp.log1p(-key) + sg))
        mid, end = run[mid_at : mid_at + 1, :], run[end_at : end_at + 1, :]
        q = que_v[rows, :].astype(F32)
        q = q * sigmoid(q) * (HD ** -0.5)
        qd[d, rows, :] = (q * jnp.exp(run - mid)).astype(BF16)
        k = key * jnp.exp(mid - run)
        kr[d, rows, :] = k.astype(BF16)
        tail = (k * jnp.exp(end - mid)).astype(BF16)
        v = val_v[rows, :]
        new = [
            dot(v[:, h * HD : (h + 1) * HD], tail[:, h * HD : (h + 1) * HD], FIRST)
            for h in range(HEADS)
        ]
        em[d, blk] = jnp.broadcast_to(jnp.exp(mid), (8, CH))
        return end, new

    def pass1(step, carry):
        blocks = [
            (d, step * UNROLL + u if d == 0 else NB - 1 - (step * UNROLL + u))
            for u in range(UNROLL)
            for d in range(2)
        ]
        parts = [pass1_block(d, blk) for d, blk in blocks]
        for (d, blk), (end, new) in zip(blocks, parts):
            gone = run_log[d, 0:1, :]
            elx[d, blk] = jnp.broadcast_to(jnp.exp(gone), (8, CH))
            run_log[d] = jnp.broadcast_to(gone + end, (8, CH))
            decay = jnp.exp(end)
            for h in range(HEADS):
                hs = slice(h * HD, (h + 1) * HD)
                state = run_state[d, hs, :]
                sx[d, blk, hs, :] = state.astype(BF16)
                run_state[d, hs, :] = state * decay[:, hs] + new[h]
        return carry

    lax.fori_loop(0, NB // UNROLL, pass1, 0)

    mark("stsend")
    def store_state(ref, at, d, state, log):
        ref[at, d, 0:CH, :] = state.astype(BF16)
        high = log.astype(BF16).astype(F32)
        rest = log - high
        ref[at, d, CH:ST_ROWS, :] = jnp.concatenate(
            [high[:, :HD], high[:, HD:], rest[:, :HD], rest[:, HD:], jnp.zeros((12, HD), F32)], axis=0
        ).astype(BF16)

    def load_log(ref, at, d):
        tail = ref[at, d, CH:ST_ROWS, :].astype(F32)
        return [tail[h : h + 1, :] + tail[2 + h : 3 + h, :] for h in range(HEADS)]

    for d in range(2):
        store_state(row_in, x, d, run_state[d], run_log[d, 0:1, :])

    def row_copy(o):
        return remote(
            row_in.at[x], row_in.at[x], st_send.at[o - 1], st_recv.at[o - 1],
            (z * 4 + ring(x, o), tp),
        )

    def row_got(o):
        ref = row_in.at[ring(x, -o)]
        remote(ref, ref, st_send.at[o - 1], st_recv.at[o - 1], (z * 4 + ring(x, o), tp)).wait_recv()

    def col_copy(o):
        ref = col_in.at[z, lax.div(z + o, 4)]
        return remote(
            ref, ref, st_send.at[o + 2], st_recv.at[o + 2], (ring(z, o) * 4 + x, tp)
        )

    def col_got(o):
        ref = col_in.at[ring(z, -o), lax.div(z + 4 - o, 4) * -1 + 1]
        remote(ref, ref, st_send.at[o + 2], st_recv.at[o + 2], (ring(z, o) * 4 + x, tp)).wait_recv()

    for o in (1, 3, 2):
        copy = row_copy(o)
        copy.start()
        started.append(copy)
    mark("l0b")
    level0b(0, 0)

    def pass2_block(blk):
        rows = pl.ds(pl.multiple_of(blk * BLK, BLK), BLK)
        v = val_v[rows, :]
        for h in range(HEADS):
            hs = slice(h * HD, (h + 1) * HD)
            fwd = dot(qd[0, rows, hs], kr[0, rows, hs], LAST)
            bwd = dot(qd[1, rows, hs], kr[1, rows, hs], LAST)
            score = jnp.where(lower, fwd, 0.0) + jnp.where(upper, bwd, 0.0)
            o_v[rows, hs] = dot(score.astype(BF16), v[:, hs])

    def by_blocks(body):
        def step(i, carry):
            for u in range(UNROLL):
                body(i * UNROLL + u)
            return carry

        lax.fori_loop(0, NB // UNROLL, step, 0)

    mark("pass2")
    by_blocks(pass2_block)


    mark("roww")
    for o in (1, 3, 2):
        row_got(o)
    mark("rowc")
    for d in range(2):
        state = jnp.zeros((CH, HD), F32)
        log = [jnp.zeros((1, HD), F32)] * HEADS
        for j in range(4) if d == 0 else range(3, -1, -1):
            own = load_log(row_in, j, d)
            state = jnp.concatenate(
                [
                    state[h * HD : (h + 1) * HD] * jnp.exp(own[h])
                    + row_in[j, d, h * HD : (h + 1) * HD, :].astype(F32)
                    for h in range(HEADS)
                ],
                axis=0,
            )
            log = [log[h] + own[h] for h in range(HEADS)]
        store_state(col_in, z, d, state, jnp.concatenate(log, axis=1))
    for o in (1, 3, 2):
        copy = col_copy(o)
        copy.start()
        started.append(copy)
    level0b(0, 1)
    sin[...] = jnp.zeros_like(sin)
    mark("colw")
    for o in (1, 3, 2):
        col_got(o)
    level1a(0)
    mark("combine")

    def chain(ref, at):
        def body(i, carry):
            d = lax.div(i + 4 - at, 4)
            j = (1 - d) * i + d * (3 + at - i)
            own = load_log(ref, j, d)
            for h in range(HEADS):
                hs = slice(h * HD, (h + 1) * HD)
                sin[d, hs, :] = sin[d, hs, :] * jnp.exp(own[h]) + ref[j, d, hs, :].astype(F32)
            return carry

        lax.fori_loop(0, 3, body, 0)

    chain(col_in, z)
    chain(row_in, x)

    for copy in loads[6:10]:
        if copy is not loads[6]:
            copy.wait()

    def pass3_block(blk):
        rows = pl.ds(pl.multiple_of(blk * BLK, BLK), BLK)
        for h in range(HEADS):
            hs = slice(h * HD, (h + 1) * HD)
            mixed = o_v[rows, hs]
            for d in range(2):
                qs = (qd[d, rows, hs].astype(F32) * em[d, blk, 0:1, hs]).astype(BF16)
                state = sx[d, blk, hs, :].astype(F32) + elx[d, blk, 0:1, hs] * sin[d, hs, :]
                mixed = mixed + dot(qs, state.astype(BF16), LAST)
            norm = mixed * lax.rsqrt(jnp.mean(mixed * mixed, axis=-1, keepdims=True) + EPS)
            g = gat_v[rows, hs].astype(F32)
            ga[tp, rows, hs] = (norm * hg_v[0:1, :] * (g * sigmoid(g))).astype(BF16)

    mark("pass3")
    by_blocks(pass3_block)

    HALF = TOK // 2

    class Gather:
        def __init__(self, buf, send_sem, recv_sem):
            self.buf, self.ss, self.rs = buf, send_sem, recv_sem

        def copy(self, k, slot, part, to):
            ref = self.buf.at[slot]
            if part is not None:
                ref = self.buf.at[slot, pl.ds(part * HALF, HALF)]
            return remote(ref, ref, self.ss.at[k], self.rs.at[k], (sp, to))

        def go(self, *args):
            copy = self.copy(*args)
            copy.start()
            started.append(copy)

        def got(self, k, slot, part):
            self.copy(k, slot, part, partner).wait_recv()

        def own(self):
            self.go(0, tp, None, 2 * yp + core)
            self.go(1, tp, None, 2 * ym + core)
            self.go(4, tp, None, partner)

        def from_side(self):
            left, right = 2 * ym + core, 2 * yp + core
            self.got(0, left, None)
            self.go(2, left, 0, right)
            self.go(5, left, None, partner)
            self.got(1, right, None)
            self.go(3, right, 1, left)
            self.go(6, right, None, partner)

        def from_far(self):
            far = 2 * y2 + core
            self.got(2, far, 0)
            self.go(7, far, 0, partner)
            self.got(3, far, 1)
            self.go(8, far, 1, partner)

    gathered = Gather(ga, g_send, g_recv)
    mark("gown")
    gathered.own()

    mark("owwait")
    for copy in loads[10:13]:
        copy.wait()
    for o in range(1, 8):
        ow_copy(o).wait_recv()

    def project(block, first=False):
        def tile(n, carry):
            cols = pl.ds(pl.multiple_of(n * 256, 256), 256)
            part = dot(ga[block], owc[pl.ds(pl.multiple_of(block * 256, 256), 256), cols])
            att[:, cols] = part if first else att[:, cols] + part
            return carry

        lax.fori_loop(0, OC // 256, tile, 0)

    mark("proj0")
    project(tp, True)
    mark("gpart")
    gathered.got(4, partner, None)
    project(partner)
    mark("gside")
    gathered.from_side()
    mark("proj2")
    project(2 * ym + core)
    project(2 * yp + core)
    mark("lev1b_0")
    level1b(0)
    mark("gpart2")
    gathered.got(5, 2 * ym + other, None)
    project(2 * ym + other)
    gathered.got(6, 2 * yp + other, None)
    project(2 * yp + other)
    mark("gfar")
    gathered.from_far()
    project(2 * y2 + core)
    gathered.got(7, 2 * y2 + other, 0)
    gathered.got(8, 2 * y2 + other, 1)
    project(2 * y2 + other)

    TILE = 128

    def middle(i, carry):
        rows = pl.ds(pl.multiple_of(i * TILE, TILE), TILE)
        xa[tp, rows, :] = (res_v[rows, :].astype(F32) + att[rows, :]).astype(BF16)
        return carry

    mark("middle")
    lax.fori_loop(0, TOK // TILE, middle, 0)

    spread = Gather(xa, x_send, x_recv)
    spread.own()
    def scale(chip, c, first=False):
        block = 2 * chip + c
        gain = ng_v[:, pl.ds(pl.multiple_of(block * OC, OC), OC)]
        cols = pl.ds(pl.multiple_of(c * OC, OC), OC)

        def body(i, carry):
            rows = pl.ds(pl.multiple_of(i * TILE, TILE), TILE)
            v = xa[block, rows, :].astype(F32)
            sq = v * v
            sq = (sq[:, 0:128] + sq[:, 128:256]) + (sq[:, 256:384] + sq[:, 384:512])
            ss[rows, :] = sq if first else ss[rows, :] + sq
            xg[rows, cols] = (v * gain).astype(BF16)
            return carry

        lax.fori_loop(0, TOK // TILE, body, 0)

    def lift(chip, first=False):
        def tile(n, carry):
            cols = pl.ds(pl.multiple_of(n * 256, 256), 256)
            part = dot(xg[...], wu[pl.ds(pl.multiple_of(chip * 2 * OC, 2 * OC), 2 * OC), cols])
            acc[:, cols] = part if first else acc[:, cols] + part
            return carry

        lax.fori_loop(0, FFL // 256, tile, 0)

    mark("lev2_0")
    level2(0)
    mark("scale0")
    scale(y, core, True)
    spread.got(4, partner, None)
    scale(y, other)
    mark("lev3_0")
    level3(0)
    level0a(1)
    level0b(1, 0)
    level0b(1, 1)
    mark("xside")
    spread.from_side()
    mark("lev4_0")
    level4(0)
    mark("lift0")
    lift(y, True)
    mark("lift1")
    scale(ym, core)
    spread.got(5, 2 * ym + other, None)
    scale(ym, other)
    lift(ym)
    mark("lev1_1")
    level1a(1)
    level1b(1)
    mark("lift2")
    scale(yp, core)
    spread.got(6, 2 * yp + other, None)
    scale(yp, other)
    lift(yp)
    mark("xfar")
    spread.from_far()
    mark("lift3")
    scale(y2, core)
    spread.got(7, 2 * y2 + other, 0)
    spread.got(8, 2 * y2 + other, 1)
    scale(y2, other)
    lift(y2)

    def activate(i, carry):
        rows = pl.ds(pl.multiple_of(i * TILE, TILE), TILE)
        total = jnp.sum(ss[rows, :], axis=-1, keepdims=True)
        v = jnp.maximum(acc[rows, :] * lax.rsqrt(total / D + EPS), 0.0)
        hid[rows, :] = (v * v).astype(BF16)
        return carry

    mark("act")
    lax.fori_loop(0, TOK // TILE, activate, 0)


    PAIRS = ((1, 0), (0, 0), (1, 1), (1, -1), (1, 2), (0, 1), (0, -1), (0, 2))

    class Step:
        def __init__(self, n):
            self.n = n
            self.dx, dz = PAIRS[n]
            zs = ring(z, dz)
            column = lax.rem(x + self.dx, 2)
            self.slot = self.dx * 4 + zs
            self.first = zs * 4 + column
            self.delta = lax.rem(zs + 4 - y, 4)
            self.odd = lax.rem(self.delta, 2) == 1
            self.far = self.delta == 2
            self.k = lax.div(self.delta, 2)
            self.to = 2 * lax.rem(y + self.delta, 4) + core

        def chip(self):
            return remote(
                pp.at[0, self.slot], d2r.at[self.slot], c_send.at[self.n], c_recv.at[self.n], (sp, partner)
            )

        def half(self, k):
            return pl.ds(pl.multiple_of(k * HALF, HALF), HALF)

        def out_far(self, k):
            return remote(
                pp.at[1, self.slot, self.half(k)], ra.at[self.slot], r_send.at[self.n, k],
                r_recv.at[self.n], (sp, 2 * (yp, ym)[k] + core),
            )

        def out_near(self, k):
            return remote(
                pp.at[1, self.slot, self.half(k)], ee.at[self.k, self.dx, self.half(k)],
                e_send.at[self.n, k], e_recv.at[self.k, self.dx, k], (sp, self.to),
            )

        def compute(self):
            mark("comp%d" % self.n)
            def part(i, carry):
                first = (self.first + 2 * (other + i * (core - other))) * SHARD
                rows = wd[pl.ds(pl.multiple_of(first, SHARD), SHARD), :]
                pp[i, self.slot] = dot(hid[...], rows, LAST).astype(BF16)

                @pl.when(i == 0)
                def _():
                    self.chip().start()

                return carry

            lax.fori_loop(0, 2, part, 0)
            started.append(self.chip())

        def chip_sum(self):
            mark("cs%d" % self.n)
            self.chip().wait_recv()

            def add(i, carry):
                rows = pl.ds(pl.multiple_of(i * TILE, TILE), TILE)
                total = pp[1, self.slot, rows, :].astype(F32) + d2r[self.slot, rows, :].astype(F32)
                pp[1, self.slot, rows, :] = total.astype(BF16)
                return carry

            lax.fori_loop(0, TOK // TILE, add, 0)

            @pl.when(self.far)
            def _():
                self.out_far(0).start()
                self.out_far(1).start()

            @pl.when(self.odd)
            def _():
                self.out_near(1 - self.k).start()

        def join(self):
            mark("jn%d" % self.n)
            @pl.when(self.odd)
            def _():
                remote(
                    ra.at[self.slot], ra.at[self.slot], r_send.at[self.n, 0], r_recv.at[self.n],
                    (sp, self.to),
                ).wait_recv()

                def add(i, carry):
                    rows = pl.ds(pl.multiple_of(self.k * HALF + i * TILE, TILE), TILE)
                    got = ra[self.slot, pl.ds(pl.multiple_of(i * TILE, TILE), TILE), :]
                    total = pp[1, self.slot, rows, :].astype(F32) + got.astype(F32)
                    pp[1, self.slot, rows, :] = total.astype(BF16)
                    return carry

                lax.fori_loop(0, HALF // TILE, add, 0)
                self.out_near(self.k).start()

        def drain(self):
            @pl.when(self.far)
            def _():
                self.out_far(0).wait_send()
                self.out_far(1).wait_send()

            @pl.when(self.odd)
            def _():
                self.out_near(1 - self.k).wait_send()
                self.out_near(self.k).wait_send()

    steps = [Step(n) for n in range(8)]
    steps[0].compute()
    mark("lev2_1")
    level2(1)
    level4(1, (0,))
    steps[1].compute()
    steps[0].chip_sum()
    steps[2].compute()
    steps[1].chip_sum()
    steps[3].compute()
    steps[2].chip_sum()
    steps[0].join()
    mark("lev3_1")
    level3(1)
    level4(1, (1, 2))
    steps[4].compute()
    steps[3].chip_sum()
    steps[1].join()
    steps[5].compute()
    steps[4].chip_sum()
    steps[2].join()
    steps[6].compute()
    steps[5].chip_sum()
    steps[3].join()
    mark("lev4_1")
    level4(1, (3,))
    steps[7].compute()
    steps[6].chip_sum()
    mark("d8")
    steps[7].chip_sum()
    for n in range(4, 8):
        mark("j%d" % n)
        steps[n].join()
    mark("ewait")

    for dx in range(2):
        slot = dx * 4 + y
        for k in range(2):
            for half in range(2):
                rows = pl.ds(half * HALF, HALF)
                remote(
                    ee.at[k, dx, rows], ee.at[k, dx, rows], e_send.at[0, 0], e_recv.at[k, dx, half],
                    (sp, partner),
                ).wait_recv()
        cols = pl.ds(pl.multiple_of(lax.rem(x + dx, 2) * SHARD, SHARD), SHARD)

        def finish(i, carry):
            rows = pl.ds(pl.multiple_of(i * TILE, TILE), TILE)
            total = pp[1, slot, rows, :].astype(F32)
            total = total + (ee[0, dx, rows, :].astype(F32) + ee[1, dx, rows, :].astype(F32))
            res_v[rows, cols] = (xa[tp, rows, cols].astype(F32) + total).astype(BF16)
            return carry

        lax.fori_loop(0, TOK // TILE, finish, 0)
    mark("final")
    final = pltpu.make_async_copy(res_v, out, in_sem.at[0])
    final.start()
    for copy in started:
        copy.wait_send()
    for step in steps:
        step.drain()
    final.wait()
    mark(None)


def per_device(
    residual, values, forget_onward, forget_reverse, surge_log_decay, gate_limit_complement,
    readout_query, output_gate, head_norm_gain, output_weight, mixer_norm_gain, up_weight,
    down_weight,
):
    any_spec = pl.BlockSpec(memory_space=pl.ANY)
    vmem, dma = pltpu.VMEM, pltpu.SemaphoreType.DMA
    scratch = [
        vmem((TOK, OC), BF16), vmem((TOK, CH), BF16), vmem((TOK, CH), BF16), vmem((TOK, CH), BF16),
        vmem((8, TOK), F32), vmem((TOK, 8), F32), vmem((2, CH), F32), vmem((TOK, CH), BF16), vmem((TOK, CH), BF16),
        vmem((1, HD), F32), vmem((1, D), F32),
        vmem((D, FFL), BF16), vmem((D, FFL), BF16), vmem((2048, OC), BF16),
        vmem((8, TOK, CH), BF16), vmem((8, TOK, OC), BF16),
        vmem((2, TOK, CH), BF16), vmem((2, TOK, CH), BF16), vmem((2, NB, CH, HD), BF16),
        vmem((2, NB, 8, CH), F32), vmem((2, NB, 8, CH), F32),
        vmem((2, CH, HD), F32), vmem((2, 8, CH), F32),
        vmem((4, 2, ST_ROWS, HD), BF16), vmem((4, 2, ST_ROWS, HD), BF16), vmem((2, CH, HD), F32),
        vmem((TOK, CH), F32), vmem((TOK, OC), F32),
        vmem((TOK, 2 * OC), BF16), vmem((TOK, HD), F32), vmem((TOK, FFL), F32), vmem((TOK, FFL), BF16),
        vmem((2, 8, TOK, SHARD), BF16), vmem((8, TOK, SHARD), BF16),
        vmem((8, TOK // 2, SHARD), BF16), vmem((2, 2, TOK, SHARD), BF16),
        dma((13,)), dma((2, 2, 20)), dma((2, 2, 20)), dma((7,)), dma((7,)), dma((6,)), dma((6,)),
        dma((9,)), dma((9,)), dma((9,)), dma((9,)), dma((8,)), dma((8,)), dma((8, 2)), dma((8,)),
        dma((8, 2)), dma((2, 2, 2)),
    ]
    return pl.pallas_call(
        kernel,
        out_shape=jax.ShapeDtypeStruct((TOK, OC), BF16),
        in_specs=[any_spec] * 13,
        out_specs=any_spec,
        scratch_shapes=scratch,
        compiler_params=pltpu.CompilerParams(
            collective_id=0, has_side_effects=True, vmem_limit_bytes=66_000_000
        ),
        name="layer",
    )(
        residual, values, forget_onward, forget_reverse, surge_log_decay.T, gate_limit_complement,
        readout_query, output_gate, head_norm_gain.reshape(1, HD), output_weight,
        mixer_norm_gain.reshape(1, D), up_weight, down_weight,
    )


def solution(mesh):
    both = P("sp", "tp")
    placed = (
        both, both, both, both, both, P(None, "tp"), both, both, P(), P("tp", None), P(), both, both,
    )
    return jax.shard_map(
        per_device, mesh=mesh, in_specs=placed, out_specs=both, check_vma=False
    )
```

```python
import functools

import jax
import jax.numpy as jnp
from jax import lax
from jax.experimental import pallas as pl
from jax.experimental.pallas import tpu as pltpu
from jax.sharding import PartitionSpec as P

D = 4096
HD = 128
HEADS = 2
CH = HEADS * HD
TOK = 768
BLK = 64
UNROLL = 3
NB = TOK // BLK
OC = 512
FFL = 1024
SHARD = 256
QUARTER = 64
EPS = 1e-06
MESH = pl.DeviceIdType.MESH
F32 = jnp.float32
BF16 = jnp.bfloat16
ST_ROWS = 272


def dot(a, b, dims=(((1,), (0,)), ((), ()))):
    return lax.dot_general(a, b, dims, preferred_element_type=F32)


LAST = (((1,), (1,)), ((), ()))
FIRST = (((0,), (0,)), ((), ()))


def sigmoid(x):
    return 1.0 / (1.0 + jnp.exp(-x))


def kernel(
    residual, values, f_on, f_rev, surge, glc, query, gate, head_gain, out_w,
    norm_gain, up_w, down_w,
    out,
    res_v, val_v, fon_v, frev_v, sur_t, sur_v, glc_v, que_v, gat_v, hg_v, ng_v,
    wu, wd, owc, ga, xa,
    qd, kr, sx, em, elx, run_state, run_log, row_in, col_in, sin, o_v, att,
    xg, ss, acc, hid,
    pp, d2r, ra, ee, relay,
    in_sem, w_send, w_recv, ow_send, ow_recv, st_send, st_recv,
    g_send, g_recv, x_send, x_recv, c_send, c_recv, r_send, r_recv, e_send, e_recv,
):
    sp, tp = lax.axis_index("sp"), lax.axis_index("tp")
    x, z = lax.rem(sp, 4), lax.div(sp, 4)
    core, y = lax.rem(tp, 2), lax.div(tp, 2)
    other = 1 - core

    cur = [None]

    def mark(name):
        if cur[0] is not None:
            cur[0].__exit__(None, None, None)
        cur[0] = jax.named_scope(name) if name else None
        if name:
            cur[0].__enter__()

    mark("start")

    def ring(v, k):
        return lax.rem(v + (k % 4), 4)

    yp, ym, y2 = ring(y, 1), ring(y, 3), ring(y, 2)
    partner = 2 * y + other

    barrier = pltpu.get_barrier_semaphore()
    for o in range(1, 16):
        pl.semaphore_signal(barrier, inc=1, device_id=(lax.rem(sp + o, 16), tp), device_id_type=MESH)
    for o in range(1, 8):
        pl.semaphore_signal(barrier, inc=1, device_id=(sp, lax.rem(tp + o, 8)), device_id_type=MESH)

    own_rows = pl.ds(pl.multiple_of(sp * SHARD, SHARD), SHARD)
    ow_rows = pl.ds(pl.multiple_of(tp * 256, 256), 256)
    own_cols = pl.ds(pl.multiple_of(tp * OC, OC), OC)
    loads = [
        (f_on, fon_v), (f_rev, frev_v), (surge, sur_t.at[pl.ds(0, HEADS)]), (glc, glc_v), (query, que_v),
        (values, val_v), (gate, gat_v), (head_gain, hg_v), (residual, res_v), (norm_gain, ng_v),
        (up_w, wu.at[own_rows]), (down_w, wd.at[own_rows]),
        (out_w.at[:, own_cols], owc.at[ow_rows]),
    ]
    loads = [pltpu.make_async_copy(a, b, in_sem.at[i]) for i, (a, b) in enumerate(loads)]
    for copy in loads:
        copy.start()

    pl.semaphore_wait(barrier, 22)

    def remote(src, dst, ss_, rs_, dev):
        return pltpu.make_async_remote_copy(
            src_ref=src, dst_ref=dst, send_sem=ss_, recv_sem=rs_, device_id=dev, device_id_type=MESH
        )

    started = []

    def go(copy):
        copy.start()
        started.append(copy)

    weights = ((up_w, wu), (down_w, wd))

    def sp_at(half, i, j):
        return ring(z, j) * 4 + ring(x, i) if half == 0 else ring(z, i) * 4 + ring(x, j)

    def piece(t, half, i, j, part):
        start, size = (0, 2 * QUARTER) if part is None else (part * QUARTER, QUARTER)
        first = sp_at(half, i, j) * SHARD + half * 2 * QUARTER + start
        return weights[t][1].at[pl.ds(pl.multiple_of(first, QUARTER), size)]

    FWD = (0, -1, 1, 2)

    def w_copy(t, half, slot, i, j, part, to, src=None):
        ref = piece(t, half, i, j, part)
        return remote(
            ref if src is None else src, ref, w_send.at[t, half, slot], w_recv.at[t, half, slot],
            (sp_at(half, *to), tp),
        )

    def w_go(*args, **kw):
        copy = w_copy(*args, **kw)
        copy.start()
        started.append(copy)

    def w_got(t, half, slot, i, j, part):
        w_copy(t, half, slot, i, j, part, (1, 0)).wait_recv()

    def w_second(t, half, n, src=None):
        i = FWD[n]
        w_go(t, half, 4 + 4 * n, i, 0, None, (0, 1), src=src)
        w_go(t, half, 5 + 4 * n, i, 0, None, (0, -1), src=src)

    def w_second_forward(t, half, n):
        i = FWD[n]
        w_got(t, half, 4 + 4 * n, i, -1, None)
        w_go(t, half, 6 + 4 * n, i, -1, 0, (0, 1))
        w_got(t, half, 5 + 4 * n, i, 1, None)
        w_go(t, half, 7 + 4 * n, i, 1, 1, (0, -1))

    def level0a(t):
        for half in range(2):
            src = weights[t][0].at[pl.ds(half * 2 * QUARTER, 2 * QUARTER)]
            w_go(t, half, 0, 0, 0, None, (1, 0), src=src)
            w_go(t, half, 1, 0, 0, None, (-1, 0), src=src)

    def level0b(t, half):
        src = weights[t][0].at[pl.ds(half * 2 * QUARTER, 2 * QUARTER)]
        w_second(t, half, 0, src=src)

    def level1a(t):
        for half in range(2):
            w_got(t, half, 0, -1, 0, None)
            w_go(t, half, 2, -1, 0, 0, (1, 0))
            w_got(t, half, 1, 1, 0, None)
            w_go(t, half, 3, 1, 0, 1, (-1, 0))
        for half in range(2):
            w_second(t, half, 1)
            w_second(t, half, 2)

    def level1b(t):
        for half in range(2):
            w_second_forward(t, half, 0)

    def level2a(t, half):
        w_got(t, half, 2, 2, 0, 0)
        w_got(t, half, 3, 2, 0, 1)
        w_second(t, half, 3)

    def level2b(t, half):
        w_second_forward(t, half, 1)
        w_second_forward(t, half, 2)

    def level3(t, half):
        w_second_forward(t, half, 3)

    def level4(t, half, blocks):
        for n in blocks:
            w_got(t, half, 6 + 4 * n, FWD[n], 2, 0)
            w_got(t, half, 7 + 4 * n, FWD[n], 2, 1)

    mark("w0")
    level0a(0)

    def ow_cols(to):
        return pl.ds(pl.multiple_of(to * OC, OC), OC)

    def ow_rows_of(source, k=None):
        first, size = (0, 256) if k is None else (k * 128, 128)
        return pl.ds(pl.multiple_of(source * 256 + first, 128), size)

    near = (yp, ym)

    def ow_leg1(k, c):
        return remote(
            out_w.at[pl.ds(k * 128, 128), ow_cols(2 * y2 + c)], relay.at[k, c],
            ow_send.at[2 * k + c], ow_recv.at[2 * k + c], (sp, 2 * near[k] + core),
        )

    def ow_direct(k, c):
        return remote(
            out_w.at[:, ow_cols(2 * near[k] + c)], owc.at[ow_rows],
            ow_send.at[4 + 2 * k + c], ow_recv.at[4 + 2 * k + core], (sp, 2 * near[k] + c),
        )

    def ow_partner():
        return remote(
            out_w.at[:, ow_cols(partner)], owc.at[ow_rows], ow_send.at[8], ow_recv.at[8], (sp, partner)
        )

    def ow_leg2(k, c):
        return remote(
            relay.at[k, c], owc.at[ow_rows_of(2 * near[1 - k] + core, k)],
            ow_send.at[9 + 2 * k + c], ow_recv.at[9 + 2 * k + core], (sp, 2 * near[k] + c),
        )

    def ow_forward():
        for k in range(2):
            for c in range(2):
                ow_leg1(k, c).wait_recv()
                go(ow_leg2(k, c))

    def ow_wait():
        def landed(rows, sem):
            ref = owc.at[rows]
            remote(ref, ref, ow_send.at[8], ow_recv.at[sem], (sp, partner)).wait_recv()

        landed(ow_rows_of(partner), 8)
        for k in range(2):
            for c in range(2):
                landed(ow_rows_of(2 * near[1 - k] + c), 4 + 2 * k + c)
        for k in range(2):
            for c in range(2):
                landed(ow_rows_of(2 * y2 + c, k), 9 + 2 * k + c)

    for k in range(2):
        for c in range(2):
            go(ow_leg1(k, c))
    for k in range(2):
        for c in range(2):
            go(ow_direct(k, c))
    go(ow_partner())

    mark("loadwait")
    for copy in loads[:7]:
        copy.wait()

    mark("pass1")
    row_id = lax.broadcasted_iota(jnp.int32, (BLK, BLK), 0)
    col_id = lax.broadcasted_iota(jnp.int32, (BLK, BLK), 1)
    lower, upper = row_id >= col_id, row_id <= col_id
    run_state[...] = jnp.zeros_like(run_state)
    run_log[...] = jnp.zeros_like(run_log)
    sur_v[...] = jnp.concatenate([sur_t[0:HEADS, :], jnp.zeros((8 - HEADS, TOK), F32)], axis=0).T
    sums = tuple(
        jnp.concatenate([jnp.where(tri, 1.0, 0.0)] * 3, axis=1).astype(BF16) for tri in (lower, upper)
    )

    def split3(v):
        a = v.astype(BF16)
        rest = v - a.astype(F32)
        b = rest.astype(BF16)
        return jnp.concatenate([a, b, (rest - b.astype(F32)).astype(BF16)], axis=0)

    def pass1_block(d, blk):
        logits = (fon_v, frev_v)[d]
        mid_at, end_at = ((BLK // 2 - 1, BLK - 1), (BLK // 2, 0))[d]
        rows = pl.ds(pl.multiple_of(blk * BLK, BLK), BLK)
        key = glc_v[d : d + 1, :] / (1.0 + jnp.exp(logits[rows, :].astype(F32)))
        sg = sur_v[rows, :]
        sg = jnp.concatenate(
            [jnp.broadcast_to(sg[:, h : h + 1], (BLK, HD)) for h in range(HEADS)], axis=1
        )
        run = dot(sums[d], split3(jnp.log1p(-key) + sg))
        mid, end = run[mid_at : mid_at + 1, :], run[end_at : end_at + 1, :]
        q = que_v[rows, :].astype(F32)
        q = q * sigmoid(q) * (HD ** -0.5)
        qd[d, rows, :] = (q * jnp.exp(run - mid)).astype(BF16)
        k = key * jnp.exp(mid - run)
        kr[d, rows, :] = k.astype(BF16)
        tail = (k * jnp.exp(end - mid)).astype(BF16)
        v = val_v[rows, :]
        new = [
            dot(v[:, h * HD : (h + 1) * HD], tail[:, h * HD : (h + 1) * HD], FIRST)
            for h in range(HEADS)
        ]
        em[d, blk] = jnp.broadcast_to(jnp.exp(mid), (8, CH))
        return end, new

    def pass1(step, carry):
        blocks = [
            (d, step * UNROLL + u if d == 0 else NB - 1 - (step * UNROLL + u))
            for u in range(UNROLL)
            for d in range(2)
        ]
        parts = [pass1_block(d, blk) for d, blk in blocks]
        for (d, blk), (end, new) in zip(blocks, parts):
            gone = run_log[d, 0:1, :]
            elx[d, blk] = jnp.broadcast_to(jnp.exp(gone), (8, CH))
            run_log[d] = jnp.broadcast_to(gone + end, (8, CH))
            decay = jnp.exp(end)
            for h in range(HEADS):
                hs = slice(h * HD, (h + 1) * HD)
                state = run_state[d, hs, :]
                sx[d, blk, hs, :] = state.astype(BF16)
                run_state[d, hs, :] = state * decay[:, hs] + new[h]
        return carry

    lax.fori_loop(0, NB // UNROLL, pass1, 0)

    mark("stsend")
    def store_state(ref, at, d, state, log):
        ref[at, d, 0:CH, :] = state.astype(BF16)
        high = log.astype(BF16).astype(F32)
        rest = log - high
        ref[at, d, CH:ST_ROWS, :] = jnp.concatenate(
            [high[:, :HD], high[:, HD:], rest[:, :HD], rest[:, HD:], jnp.zeros((12, HD), F32)], axis=0
        ).astype(BF16)

    def load_log(ref, at, d):
        tail = ref[at, d, CH:ST_ROWS, :].astype(F32)
        return [tail[h : h + 1, :] + tail[2 + h : 3 + h, :] for h in range(HEADS)]

    for d in range(2):
        store_state(row_in, x, d, run_state[d], run_log[d, 0:1, :])

    def row_copy(o):
        return remote(
            row_in.at[x], row_in.at[x], st_send.at[o - 1], st_recv.at[o - 1],
            (z * 4 + ring(x, o), tp),
        )

    def row_got(o):
        ref = row_in.at[ring(x, -o)]
        remote(ref, ref, st_send.at[o - 1], st_recv.at[o - 1], (z * 4 + ring(x, o), tp)).wait_recv()

    def col_copy(o):
        ref = col_in.at[z, lax.div(z + o, 4)]
        return remote(
            ref, ref, st_send.at[o + 2], st_recv.at[o + 2], (ring(z, o) * 4 + x, tp)
        )

    def col_got(o):
        ref = col_in.at[ring(z, -o), lax.div(z + 4 - o, 4) * -1 + 1]
        remote(ref, ref, st_send.at[o + 2], st_recv.at[o + 2], (ring(z, o) * 4 + x, tp)).wait_recv()

    for o in (1, 3, 2):
        copy = row_copy(o)
        copy.start()
        started.append(copy)
    mark("l0b")
    level0b(0, 0)

    def pass2_block(blk):
        rows = pl.ds(pl.multiple_of(blk * BLK, BLK), BLK)
        v = val_v[rows, :]
        for h in range(HEADS):
            hs = slice(h * HD, (h + 1) * HD)
            fwd = dot(qd[0, rows, hs], kr[0, rows, hs], LAST)
            bwd = dot(qd[1, rows, hs], kr[1, rows, hs], LAST)
            score = jnp.where(lower, fwd, 0.0) + jnp.where(upper, bwd, 0.0)
            o_v[rows, hs] = dot(score.astype(BF16), v[:, hs])

    def by_blocks(body):
        def step(i, carry):
            for u in range(UNROLL):
                body(i * UNROLL + u)
            return carry

        lax.fori_loop(0, NB // UNROLL, step, 0)

    mark("pass2")
    by_blocks(pass2_block)


    mark("owfwd")
    ow_forward()
    mark("roww")
    for o in (1, 3, 2):
        row_got(o)
    mark("rowc")
    for d in range(2):
        state = jnp.zeros((CH, HD), F32)
        log = [jnp.zeros((1, HD), F32)] * HEADS
        for j in range(4) if d == 0 else range(3, -1, -1):
            own = load_log(row_in, j, d)
            state = jnp.concatenate(
                [
                    state[h * HD : (h + 1) * HD] * jnp.exp(own[h])
                    + row_in[j, d, h * HD : (h + 1) * HD, :].astype(F32)
                    for h in range(HEADS)
                ],
                axis=0,
            )
            log = [log[h] + own[h] for h in range(HEADS)]
        store_state(col_in, z, d, state, jnp.concatenate(log, axis=1))
    for o in (1, 3, 2):
        copy = col_copy(o)
        copy.start()
        started.append(copy)
    level0b(0, 1)
    sin[...] = jnp.zeros_like(sin)
    mark("colw")
    for o in (1, 3, 2):
        col_got(o)
    level1a(0)
    mark("combine")

    def chain(ref, at):
        def body(i, carry):
            d = lax.div(i + 4 - at, 4)
            j = (1 - d) * i + d * (3 + at - i)
            own = load_log(ref, j, d)
            for h in range(HEADS):
                hs = slice(h * HD, (h + 1) * HD)
                sin[d, hs, :] = sin[d, hs, :] * jnp.exp(own[h]) + ref[j, d, hs, :].astype(F32)
            return carry

        lax.fori_loop(0, 3, body, 0)

    chain(col_in, z)
    chain(row_in, x)

    for copy in loads[6:10]:
        if copy is not loads[6]:
            copy.wait()

    def pass3_block(blk):
        rows = pl.ds(pl.multiple_of(blk * BLK, BLK), BLK)
        for h in range(HEADS):
            hs = slice(h * HD, (h + 1) * HD)
            mixed = o_v[rows, hs]
            for d in range(2):
                qs = (qd[d, rows, hs].astype(F32) * em[d, blk, 0:1, hs]).astype(BF16)
                state = sx[d, blk, hs, :].astype(F32) + elx[d, blk, 0:1, hs] * sin[d, hs, :]
                mixed = mixed + dot(qs, state.astype(BF16), LAST)
            norm = mixed * lax.rsqrt(jnp.mean(mixed * mixed, axis=-1, keepdims=True) + EPS)
            g = gat_v[rows, hs].astype(F32)
            ga[tp, rows, hs] = (norm * hg_v[0:1, :] * (g * sigmoid(g))).astype(BF16)

    mark("pass3")
    by_blocks(pass3_block)

    HALF = TOK // 2

    class Gather:
        def __init__(self, buf, send_sem, recv_sem):
            self.buf, self.ss, self.rs = buf, send_sem, recv_sem

        def copy(self, k, slot, part, to):
            ref = self.buf.at[slot]
            if part is not None:
                ref = self.buf.at[slot, pl.ds(part * HALF, HALF)]
            return remote(ref, ref, self.ss.at[k], self.rs.at[k], (sp, to))

        def go(self, *args):
            copy = self.copy(*args)
            copy.start()
            started.append(copy)

        def got(self, k, slot, part):
            self.copy(k, slot, part, partner).wait_recv()

        def own(self):
            right, left = 2 * yp + core, 2 * ym + core
            self.go(0, tp, 0, right)
            self.go(3, tp, 1, left)
            self.go(6, tp, None, partner)
            self.go(1, tp, 1, right)
            self.go(2, tp, 0, left)

        def forward(self):
            left, right = 2 * ym + core, 2 * yp + core
            self.got(0, left, 0)
            self.go(4, left, 0, right)
            self.got(3, right, 1)
            self.go(5, right, 1, left)

        def from_side(self):
            left, right = 2 * ym + core, 2 * yp + core
            self.got(1, left, 1)
            self.go(7, left, None, partner)
            self.got(2, right, 0)
            self.go(8, right, None, partner)

        def from_far(self):
            far = 2 * y2 + core
            self.got(4, far, 0)
            self.go(9, far, 0, partner)
            self.got(5, far, 1)
            self.go(10, far, 1, partner)

    gathered = Gather(ga, g_send, g_recv)
    mark("gown")
    gathered.own()

    mark("owwait")
    for copy in loads[10:13]:
        copy.wait()
    ow_wait()

    def project(block, first=False):
        def tile(n, carry):
            cols = pl.ds(pl.multiple_of(n * 256, 256), 256)
            part = dot(ga[block], owc[pl.ds(pl.multiple_of(block * 256, 256), 256), cols])
            att[:, cols] = part if first else att[:, cols] + part
            return carry

        lax.fori_loop(0, OC // 256, tile, 0)

    mark("proj0")
    project(tp, True)
    mark("gpart")
    gathered.got(6, partner, None)
    project(partner)
    mark("lev2a_0")
    level1b(0)
    level2a(0, 0)
    level2a(0, 1)
    mark("gfwd")
    gathered.forward()
    mark("gside")
    gathered.from_side()
    mark("proj2")
    project(2 * ym + core)
    project(2 * yp + core)
    mark("lev2b_0")
    level2b(0, 0)
    level2b(0, 1)
    level0a(1)
    mark("gpart2")
    gathered.got(7, 2 * ym + other, None)
    project(2 * ym + other)
    gathered.got(8, 2 * yp + other, None)
    project(2 * yp + other)
    mark("gfar")
    gathered.from_far()
    project(2 * y2 + core)
    gathered.got(9, 2 * y2 + other, 0)
    gathered.got(10, 2 * y2 + other, 1)
    project(2 * y2 + other)

    TILE = 128

    def middle(i, carry):
        rows = pl.ds(pl.multiple_of(i * TILE, TILE), TILE)
        xa[tp, rows, :] = (res_v[rows, :].astype(F32) + att[rows, :]).astype(BF16)
        return carry

    mark("middle")
    lax.fori_loop(0, TOK // TILE, middle, 0)

    spread = Gather(xa, x_send, x_recv)
    spread.own()
    def scale(chip, c, first=False):
        block = 2 * chip + c
        gain = ng_v[:, pl.ds(pl.multiple_of(block * OC, OC), OC)]
        cols = pl.ds(pl.multiple_of(c * OC, OC), OC)

        def body(i, carry):
            rows = pl.ds(pl.multiple_of(i * TILE, TILE), TILE)
            v = xa[block, rows, :].astype(F32)
            sq = v * v
            sq = (sq[:, 0:128] + sq[:, 128:256]) + (sq[:, 256:384] + sq[:, 384:512])
            ss[rows, :] = sq if first else ss[rows, :] + sq
            xg[rows, cols] = (v * gain).astype(BF16)
            return carry

        lax.fori_loop(0, TOK // TILE, body, 0)

    def lift(chip, first=False):
        def tile(n, carry):
            cols = pl.ds(pl.multiple_of(n * 256, 256), 256)
            part = dot(xg[...], wu[pl.ds(pl.multiple_of(chip * 2 * OC, 2 * OC), 2 * OC), cols])
            acc[:, cols] = part if first else acc[:, cols] + part
            return carry

        lax.fori_loop(0, FFL // 256, tile, 0)

    mark("scale0")
    scale(y, core, True)
    spread.got(6, partner, None)
    scale(y, other)
    mark("lev3_0")
    level3(0, 0)
    level3(0, 1)
    level0b(1, 0)
    level0b(1, 1)
    mark("xfwd")
    spread.forward()
    mark("lev1a_1")
    level1a(1)
    mark("xside")
    spread.from_side()
    mark("lev4_0")
    level4(0, 0, range(4))
    level4(0, 1, range(4))
    mark("lift0")
    lift(y, True)
    mark("lift1")
    scale(ym, core)
    spread.got(7, 2 * ym + other, None)
    scale(ym, other)
    lift(ym)
    mark("lev1_1")
    level1b(1)
    level2a(1, 1)
    mark("lift2")
    scale(yp, core)
    spread.got(8, 2 * yp + other, None)
    scale(yp, other)
    lift(yp)
    mark("xfar")
    spread.from_far()
    mark("lift3")
    scale(y2, core)
    spread.got(9, 2 * y2 + other, 0)
    spread.got(10, 2 * y2 + other, 1)
    scale(y2, other)
    lift(y2)

    def activate(i, carry):
        rows = pl.ds(pl.multiple_of(i * TILE, TILE), TILE)
        total = jnp.sum(ss[rows, :], axis=-1, keepdims=True)
        v = jnp.maximum(acc[rows, :] * lax.rsqrt(total / D + EPS), 0.0)
        hid[rows, :] = (v * v).astype(BF16)
        return carry

    mark("act")
    lax.fori_loop(0, TOK // TILE, activate, 0)


    SHARDS = (
        (1, 0), (0, 0), (1, 1), (1, -1), (1, 2), (0, 1), (0, -1), (0, 2), (2, 2)
    )

    class Step:
        def __init__(self, n):
            self.n = n
            dx, dz = SHARDS[n]
            self.single = n >= 7
            self.dx = dx % 2
            zs = ring(z, dz)
            column = lax.rem(x + dx, 2)
            self.keep = lax.div(ring(x, dx), 2) == core
            self.kept = jnp.where(self.keep, 1, 0)
            self.slot = self.dx * 4 + zs
            self.first = zs * 4 + column
            self.delta = lax.rem(zs + 4 - y, 4)
            self.odd = lax.rem(self.delta, 2) == 1
            self.far = self.delta == 2
            self.k = lax.div(self.delta, 2)
            self.to = 2 * lax.rem(y + self.delta, 4) + core

        def chip(self):
            return remote(
                pp.at[0, self.slot], d2r.at[self.slot], c_send.at[self.n], c_recv.at[self.n], (sp, partner)
            )

        def half(self, k):
            return pl.ds(pl.multiple_of(k * HALF, HALF), HALF)

        def out_far(self, k):
            return remote(
                pp.at[1, self.slot, self.half(k)], ra.at[self.slot], r_send.at[self.n, k],
                r_recv.at[self.n], (sp, 2 * (yp, ym)[k] + core),
            )

        def out_near(self, k):
            return remote(
                pp.at[1, self.slot, self.half(k)], ee.at[self.k, self.dx, self.half(k)],
                e_send.at[self.n, k], e_recv.at[self.k, self.dx, k], (sp, self.to),
            )

        def compute(self):
            mark("comp%d" % self.n)
            def part(i, carry):
                first = (self.first + 2 * (other + i * (core - other))) * SHARD
                rows = wd[pl.ds(pl.multiple_of(first, SHARD), SHARD), :]
                pp[i, self.slot] = dot(hid[...], rows, LAST).astype(BF16)

                @pl.when(i == 0)
                def _():
                    self.chip().start()

                return carry

            if self.single:
                part(self.kept, 0)
            else:
                lax.fori_loop(0, 2, part, 0)

        def when_kept(self, body):
            if self.single:
                pl.when(self.keep)(body)
            else:
                body()

        def chip_sum(self):
            mark("cs%d" % self.n)
            self.when_kept(self.chip_sum_kept)

        def chip_sum_kept(self):
            self.chip().wait_recv()

            def add(i, carry):
                rows = pl.ds(pl.multiple_of(i * TILE, TILE), TILE)
                total = pp[1, self.slot, rows, :].astype(F32) + d2r[self.slot, rows, :].astype(F32)
                pp[1, self.slot, rows, :] = total.astype(BF16)
                return carry

            lax.fori_loop(0, TOK // TILE, add, 0)

            @pl.when(self.far)
            def _():
                self.out_far(0).start()
                self.out_far(1).start()

            @pl.when(self.odd)
            def _():
                self.out_near(1 - self.k).start()

        def join(self):
            mark("jn%d" % self.n)
            self.when_kept(self.join_kept)

        def join_kept(self):
            @pl.when(self.odd)
            def _():
                remote(
                    ra.at[self.slot], ra.at[self.slot], r_send.at[self.n, 0], r_recv.at[self.n],
                    (sp, self.to),
                ).wait_recv()

                def add(i, carry):
                    rows = pl.ds(pl.multiple_of(self.k * HALF + i * TILE, TILE), TILE)
                    got = ra[self.slot, pl.ds(pl.multiple_of(i * TILE, TILE), TILE), :]
                    total = pp[1, self.slot, rows, :].astype(F32) + got.astype(F32)
                    pp[1, self.slot, rows, :] = total.astype(BF16)
                    return carry

                lax.fori_loop(0, HALF // TILE, add, 0)
                self.out_near(self.k).start()

        def drain(self):
            if self.single:
                pl.when(jnp.logical_not(self.keep))(lambda: self.chip().wait_send())
            else:
                self.chip().wait_send()
            self.when_kept(self.drain_kept)

        def drain_kept(self):
            @pl.when(self.far)
            def _():
                self.out_far(0).wait_send()
                self.out_far(1).wait_send()

            @pl.when(self.odd)
            def _():
                self.out_near(1 - self.k).wait_send()
                self.out_near(self.k).wait_send()

    steps = [Step(n) for n in range(9)]
    steps[0].compute()
    mark("lev2_1")
    level2b(1, 0)
    level2a(1, 0)
    level2b(1, 1)
    steps[2].compute()
    steps[0].chip_sum()
    steps[3].compute()
    steps[2].chip_sum()
    mark("w7")
    level4(1, 0, (0,))
    level4(1, 1, (0,))
    steps[7].compute()
    steps[3].chip_sum()
    steps[1].compute()
    steps[7].chip_sum()
    steps[1].chip_sum()
    mark("w4")
    level4(1, 0, (1, 2))
    level3(1, 1)
    steps[4].compute()
    steps[0].join()
    steps[4].chip_sum()
    mark("w30")
    level3(1, 0)
    steps[2].join()
    steps[3].join()
    mark("w5")
    level4(1, 1, (1, 2))
    steps[5].compute()
    steps[7].join()
    steps[6].compute()
    steps[5].chip_sum()
    steps[1].join()
    mark("w8")
    level4(1, 0, (3,))
    level4(1, 1, (3,))
    steps[8].compute()
    steps[6].chip_sum()
    steps[8].chip_sum()
    for n in (4, 5, 6, 8):
        steps[n].join()
    mark("ewait")

    for dx in range(2):
        slot = dx * 4 + y
        for k in range(2):
            for half in range(2):
                rows = pl.ds(half * HALF, HALF)
                remote(
                    ee.at[k, dx, rows], ee.at[k, dx, rows], e_send.at[0, 0], e_recv.at[k, dx, half],
                    (sp, partner),
                ).wait_recv()
        cols = pl.ds(pl.multiple_of(lax.rem(x + dx, 2) * SHARD, SHARD), SHARD)

        def finish(i, carry):
            rows = pl.ds(pl.multiple_of(i * TILE, TILE), TILE)
            total = pp[1, slot, rows, :].astype(F32)
            total = total + (ee[0, dx, rows, :].astype(F32) + ee[1, dx, rows, :].astype(F32))
            res_v[rows, cols] = (xa[tp, rows, cols].astype(F32) + total).astype(BF16)
            return carry

        lax.fori_loop(0, TOK // TILE, finish, 0)
    mark("final")
    final = pltpu.make_async_copy(res_v, out, in_sem.at[0])
    final.start()
    for copy in started:
        copy.wait_send()
    for step in steps:
        step.drain()
    final.wait()
    mark(None)


def per_device(
    residual, values, forget_onward, forget_reverse, surge_log_decay, gate_limit_complement,
    readout_query, output_gate, head_norm_gain, output_weight, mixer_norm_gain, up_weight,
    down_weight,
):
    any_spec = pl.BlockSpec(memory_space=pl.ANY)
    vmem, dma = pltpu.VMEM, pltpu.SemaphoreType.DMA
    scratch = [
        vmem((TOK, OC), BF16), vmem((TOK, CH), BF16), vmem((TOK, CH), BF16), vmem((TOK, CH), BF16),
        vmem((8, TOK), F32), vmem((TOK, 8), F32), vmem((2, CH), F32), vmem((TOK, CH), BF16), vmem((TOK, CH), BF16),
        vmem((1, HD), F32), vmem((1, D), F32),
        vmem((D, FFL), BF16), vmem((D, FFL), BF16), vmem((2048, OC), BF16),
        vmem((8, TOK, CH), BF16), vmem((8, TOK, OC), BF16),
        vmem((2, TOK, CH), BF16), vmem((2, TOK, CH), BF16), vmem((2, NB, CH, HD), BF16),
        vmem((2, NB, 8, CH), F32), vmem((2, NB, 8, CH), F32),
        vmem((2, CH, HD), F32), vmem((2, 8, CH), F32),
        vmem((4, 2, ST_ROWS, HD), BF16), vmem((4, 2, ST_ROWS, HD), BF16), vmem((2, CH, HD), F32),
        vmem((TOK, CH), F32), vmem((TOK, OC), F32),
        vmem((TOK, 2 * OC), BF16), vmem((TOK, HD), F32), vmem((TOK, FFL), F32), vmem((TOK, FFL), BF16),
        vmem((2, 8, TOK, SHARD), BF16), vmem((8, TOK, SHARD), BF16),
        vmem((8, TOK // 2, SHARD), BF16), vmem((2, 2, TOK, SHARD), BF16),
        vmem((2, 2, 128, OC), BF16),
        dma((13,)), dma((2, 2, 20)), dma((2, 2, 20)), dma((13,)), dma((13,)), dma((6,)), dma((6,)),
        dma((11,)), dma((11,)), dma((11,)), dma((11,)), dma((9,)), dma((9,)), dma((9, 2)), dma((9,)),
        dma((9, 2)), dma((2, 2, 2)),
    ]
    return pl.pallas_call(
        kernel,
        out_shape=jax.ShapeDtypeStruct((TOK, OC), BF16),
        in_specs=[any_spec] * 13,
        out_specs=any_spec,
        scratch_shapes=scratch,
        compiler_params=pltpu.CompilerParams(
            collective_id=0, has_side_effects=True, vmem_limit_bytes=66_000_000
        ),
        name="layer",
    )(
        residual, values, forget_onward, forget_reverse, surge_log_decay.T, gate_limit_complement,
        readout_query, output_gate, head_norm_gain.reshape(1, HD), output_weight,
        mixer_norm_gain.reshape(1, D), up_weight, down_weight,
    )


def solution(mesh):
    both = P("sp", "tp")
    placed = (
        both, both, both, both, both, P(None, "tp"), both, both, P(), P("tp", None), P(), both, both,
    )
    return jax.shard_map(
        per_device, mesh=mesh, in_specs=placed, out_specs=both, check_vma=False
    )
```

```python
import functools

import jax
import jax.numpy as jnp
from jax import lax
from jax.experimental import pallas as pl
from jax.experimental.pallas import tpu as pltpu
from jax.sharding import PartitionSpec as P

D = 4096
HD = 128
HEADS = 2
CH = HEADS * HD
TOK = 768
BLK = 64
UNROLL = 3
NB = TOK // BLK
OC = 512
FFL = 1024
SHARD = 256
QUARTER = 64
EPS = 1e-06
MESH = pl.DeviceIdType.MESH
F32 = jnp.float32
BF16 = jnp.bfloat16
ST_ROWS = 272


def dot(a, b, dims=(((1,), (0,)), ((), ()))):
    return lax.dot_general(a, b, dims, preferred_element_type=F32)


LAST = (((1,), (1,)), ((), ()))
FIRST = (((0,), (0,)), ((), ()))


def sigmoid(x):
    return 1.0 / (1.0 + jnp.exp(-x))


def kernel(
    residual, values, f_on, f_rev, surge, glc, query, gate, head_gain, out_w,
    norm_gain, up_w, down_w,
    out,
    res_v, val_v, fon_v, frev_v, sur_t, sur_v, glc_v, que_v, gat_v, hg_v, ng_v,
    wu, wd, owc, ga, xa,
    qd, kr, sx, em, elx, run_state, run_log, row_in, col_in, sin, o_v, att,
    xg, ss, acc, hid,
    pp, d2r, ra, ee, relay, rel,
    in_sem, w_send, w_recv, ow_send, ow_recv, st_send, st_recv,
    g_send, g_recv, x_send, x_recv, c_send, c_recv, r_send, r_recv, e_send, e_recv,
):
    sp, tp = lax.axis_index("sp"), lax.axis_index("tp")
    x, z = lax.rem(sp, 4), lax.div(sp, 4)
    core, y = lax.rem(tp, 2), lax.div(tp, 2)
    other = 1 - core

    cur = [None]

    def mark(name):
        if cur[0] is not None:
            cur[0].__exit__(None, None, None)
        cur[0] = jax.named_scope(name) if name else None
        if name:
            cur[0].__enter__()

    mark("start")

    def ring(v, k):
        return lax.rem(v + (k % 4), 4)

    yp, ym, y2 = ring(y, 1), ring(y, 3), ring(y, 2)
    partner = 2 * y + other

    barrier = pltpu.get_barrier_semaphore()
    for o in range(1, 16):
        pl.semaphore_signal(barrier, inc=1, device_id=(lax.rem(sp + o, 16), tp), device_id_type=MESH)
    for o in range(1, 8):
        pl.semaphore_signal(barrier, inc=1, device_id=(sp, lax.rem(tp + o, 8)), device_id_type=MESH)

    own_rows = pl.ds(pl.multiple_of(sp * SHARD, SHARD), SHARD)
    ow_rows = pl.ds(pl.multiple_of(tp * 256, 256), 256)
    own_cols = pl.ds(pl.multiple_of(tp * OC, OC), OC)
    loads = [
        (f_on, fon_v), (f_rev, frev_v), (surge, sur_t.at[pl.ds(0, HEADS)]), (glc, glc_v), (query, que_v),
        (values, val_v), (gate, gat_v), (head_gain, hg_v), (residual, res_v), (norm_gain, ng_v),
        (up_w, wu.at[own_rows]), (down_w, wd.at[own_rows]),
        (out_w.at[:, own_cols], owc.at[ow_rows]),
    ]
    loads = [pltpu.make_async_copy(a, b, in_sem.at[i]) for i, (a, b) in enumerate(loads)]
    for copy in loads:
        copy.start()

    pl.semaphore_wait(barrier, 22)

    def remote(src, dst, ss_, rs_, dev):
        return pltpu.make_async_remote_copy(
            src_ref=src, dst_ref=dst, send_sem=ss_, recv_sem=rs_, device_id=dev, device_id_type=MESH
        )

    started = []

    def go(copy):
        copy.start()
        started.append(copy)

    weights = ((up_w, wu), (down_w, wd))

    def sp_at(half, i, j):
        return ring(z, j) * 4 + ring(x, i) if half == 0 else ring(z, i) * 4 + ring(x, j)

    def piece(t, half, i, j, part):
        start, size = (0, 2 * QUARTER) if part is None else (part * QUARTER, QUARTER)
        first = sp_at(half, i, j) * SHARD + half * 2 * QUARTER + start
        return weights[t][1].at[pl.ds(pl.multiple_of(first, QUARTER), size)]

    FWD = (0, -1, 1, 2)

    def w_copy(t, half, slot, i, j, part, to, src=None):
        ref = piece(t, half, i, j, part)
        return remote(
            ref if src is None else src, ref, w_send.at[t, half, slot], w_recv.at[t, half, slot],
            (sp_at(half, *to), tp),
        )

    def w_go(*args, **kw):
        copy = w_copy(*args, **kw)
        copy.start()
        started.append(copy)

    def w_got(t, half, slot, i, j, part):
        w_copy(t, half, slot, i, j, part, (1, 0)).wait_recv()

    def w_second(t, half, n, src=None):
        i = FWD[n]
        w_go(t, half, 4 + 4 * n, i, 0, None, (0, 1), src=src)
        w_go(t, half, 5 + 4 * n, i, 0, None, (0, -1), src=src)

    def w_second_forward(t, half, n):
        i = FWD[n]
        w_got(t, half, 4 + 4 * n, i, -1, None)
        w_go(t, half, 6 + 4 * n, i, -1, 0, (0, 1))
        w_got(t, half, 5 + 4 * n, i, 1, None)
        w_go(t, half, 7 + 4 * n, i, 1, 1, (0, -1))

    def level0a(t):
        for half in range(2):
            src = weights[t][0].at[pl.ds(half * 2 * QUARTER, 2 * QUARTER)]
            w_go(t, half, 0, 0, 0, None, (1, 0), src=src)
            w_go(t, half, 1, 0, 0, None, (-1, 0), src=src)

    def level0b(t, half):
        src = weights[t][0].at[pl.ds(half * 2 * QUARTER, 2 * QUARTER)]
        w_second(t, half, 0, src=src)

    def level1a(t):
        for half in range(2):
            w_got(t, half, 0, -1, 0, None)
            w_go(t, half, 2, -1, 0, 0, (1, 0))
            w_got(t, half, 1, 1, 0, None)
            w_go(t, half, 3, 1, 0, 1, (-1, 0))
        for half in range(2):
            w_second(t, half, 1)
            w_second(t, half, 2)

    def level1b(t):
        for half in range(2):
            w_second_forward(t, half, 0)

    def level2a(t, half):
        w_got(t, half, 2, 2, 0, 0)
        w_got(t, half, 3, 2, 0, 1)
        w_second(t, half, 3)

    def level2b(t, half):
        w_second_forward(t, half, 1)
        w_second_forward(t, half, 2)

    def level3(t, half):
        w_second_forward(t, half, 3)

    def level4(t, half, blocks):
        for n in blocks:
            w_got(t, half, 6 + 4 * n, FWD[n], 2, 0)
            w_got(t, half, 7 + 4 * n, FWD[n], 2, 1)

    mark("w0")
    level0a(0)

    def ow_cols(to):
        return pl.ds(pl.multiple_of(to * OC, OC), OC)

    def ow_rows_of(source, k=None):
        first, size = (0, 256) if k is None else (k * 128, 128)
        return pl.ds(pl.multiple_of(source * 256 + first, 128), size)

    near = (yp, ym)

    def ow_leg1(k, c):
        return remote(
            out_w.at[pl.ds(k * 128, 128), ow_cols(2 * y2 + c)], relay.at[k, c],
            ow_send.at[2 * k + c], ow_recv.at[2 * k + c], (sp, 2 * near[k] + core),
        )

    def ow_direct(k, c):
        return remote(
            out_w.at[:, ow_cols(2 * near[k] + c)], owc.at[ow_rows],
            ow_send.at[4 + 2 * k + c], ow_recv.at[4 + 2 * k + core], (sp, 2 * near[k] + c),
        )

    def ow_partner():
        return remote(
            out_w.at[:, ow_cols(partner)], owc.at[ow_rows], ow_send.at[8], ow_recv.at[8], (sp, partner)
        )

    def ow_leg2(k, c):
        return remote(
            relay.at[k, c], owc.at[ow_rows_of(2 * near[1 - k] + core, k)],
            ow_send.at[9 + 2 * k + c], ow_recv.at[9 + 2 * k + core], (sp, 2 * near[k] + c),
        )

    def ow_forward():
        for k in range(2):
            for c in range(2):
                ow_leg1(k, c).wait_recv()
                go(ow_leg2(k, c))

    def ow_wait():
        def landed(rows, sem):
            ref = owc.at[rows]
            remote(ref, ref, ow_send.at[8], ow_recv.at[sem], (sp, partner)).wait_recv()

        landed(ow_rows_of(partner), 8)
        for k in range(2):
            for c in range(2):
                landed(ow_rows_of(2 * near[1 - k] + c), 4 + 2 * k + c)
        for k in range(2):
            for c in range(2):
                landed(ow_rows_of(2 * y2 + c, k), 9 + 2 * k + c)

    for k in range(2):
        for c in range(2):
            go(ow_leg1(k, c))
    for k in range(2):
        for c in range(2):
            go(ow_direct(k, c))
    go(ow_partner())

    mark("loadwait")
    for copy in loads[:7]:
        copy.wait()

    mark("pass1")
    row_id = lax.broadcasted_iota(jnp.int32, (BLK, BLK), 0)
    col_id = lax.broadcasted_iota(jnp.int32, (BLK, BLK), 1)
    lower, upper = row_id >= col_id, row_id <= col_id
    run_state[...] = jnp.zeros_like(run_state)
    run_log[...] = jnp.zeros_like(run_log)
    sur_v[...] = jnp.concatenate([sur_t[0:HEADS, :], jnp.zeros((8 - HEADS, TOK), F32)], axis=0).T
    sums = tuple(
        jnp.concatenate([jnp.where(tri, 1.0, 0.0)] * 3, axis=1).astype(BF16) for tri in (lower, upper)
    )

    def split3(v):
        a = v.astype(BF16)
        rest = v - a.astype(F32)
        b = rest.astype(BF16)
        return jnp.concatenate([a, b, (rest - b.astype(F32)).astype(BF16)], axis=0)

    def pass1_block(d, blk):
        logits = (fon_v, frev_v)[d]
        mid_at, end_at = ((BLK // 2 - 1, BLK - 1), (BLK // 2, 0))[d]
        rows = pl.ds(pl.multiple_of(blk * BLK, BLK), BLK)
        key = glc_v[d : d + 1, :] / (1.0 + jnp.exp(logits[rows, :].astype(F32)))
        sg = sur_v[rows, :]
        sg = jnp.concatenate(
            [jnp.broadcast_to(sg[:, h : h + 1], (BLK, HD)) for h in range(HEADS)], axis=1
        )
        run = dot(sums[d], split3(jnp.log1p(-key) + sg))
        mid, end = run[mid_at : mid_at + 1, :], run[end_at : end_at + 1, :]
        away = mid - run
        rel[d, rows, :] = away
        k = key * jnp.exp(away)
        kr[d, rows, :] = k.astype(BF16)
        tail = (k * jnp.exp(end - mid)).astype(BF16)
        v = val_v[rows, :]
        new = [
            dot(v[:, h * HD : (h + 1) * HD], tail[:, h * HD : (h + 1) * HD], FIRST)
            for h in range(HEADS)
        ]
        em[d, blk] = jnp.broadcast_to(jnp.exp(mid), (8, CH))
        return end, new

    def pass1(step, carry):
        blocks = [
            (d, step * UNROLL + u if d == 0 else NB - 1 - (step * UNROLL + u))
            for u in range(UNROLL)
            for d in range(2)
        ]
        parts = [pass1_block(d, blk) for d, blk in blocks]
        for (d, blk), (end, new) in zip(blocks, parts):
            gone = run_log[d, 0:1, :]
            elx[d, blk] = jnp.broadcast_to(jnp.exp(gone), (8, CH))
            run_log[d] = jnp.broadcast_to(gone + end, (8, CH))
            decay = jnp.exp(end)
            for h in range(HEADS):
                hs = slice(h * HD, (h + 1) * HD)
                state = run_state[d, hs, :]
                sx[d, blk, hs, :] = state.astype(BF16)
                run_state[d, hs, :] = state * decay[:, hs] + new[h]
        return carry

    lax.fori_loop(0, NB // UNROLL, pass1, 0)

    mark("stsend")
    def store_state(ref, at, d, state, log):
        ref[at, d, 0:CH, :] = state.astype(BF16)
        high = log.astype(BF16).astype(F32)
        rest = log - high
        ref[at, d, CH:ST_ROWS, :] = jnp.concatenate(
            [high[:, :HD], high[:, HD:], rest[:, :HD], rest[:, HD:], jnp.zeros((12, HD), F32)], axis=0
        ).astype(BF16)

    def load_log(ref, at, d):
        tail = ref[at, d, CH:ST_ROWS, :].astype(F32)
        return [tail[h : h + 1, :] + tail[2 + h : 3 + h, :] for h in range(HEADS)]

    for d in range(2):
        store_state(row_in, x, d, run_state[d], run_log[d, 0:1, :])

    def row_copy(o):
        return remote(
            row_in.at[x], row_in.at[x], st_send.at[o - 1], st_recv.at[o - 1],
            (z * 4 + ring(x, o), tp),
        )

    def row_got(o):
        ref = row_in.at[ring(x, -o)]
        remote(ref, ref, st_send.at[o - 1], st_recv.at[o - 1], (z * 4 + ring(x, o), tp)).wait_recv()

    def col_copy(o):
        ref = col_in.at[z, lax.div(z + o, 4)]
        return remote(
            ref, ref, st_send.at[o + 2], st_recv.at[o + 2], (ring(z, o) * 4 + x, tp)
        )

    def col_got(o):
        ref = col_in.at[ring(z, -o), lax.div(z + 4 - o, 4) * -1 + 1]
        remote(ref, ref, st_send.at[o + 2], st_recv.at[o + 2], (ring(z, o) * 4 + x, tp)).wait_recv()

    for o in (1, 3, 2):
        copy = row_copy(o)
        copy.start()
        started.append(copy)
    mark("l0b")
    level0b(0, 0)

    def pass2_block(blk):
        rows = pl.ds(pl.multiple_of(blk * BLK, BLK), BLK)
        v = val_v[rows, :]
        q = que_v[rows, :].astype(F32)
        q = q * sigmoid(q) * (HD ** -0.5)
        for d in range(2):
            qd[d, rows, :] = (q * jnp.exp(-rel[d, rows, :])).astype(BF16)
        for h in range(HEADS):
            hs = slice(h * HD, (h + 1) * HD)
            fwd = dot(qd[0, rows, hs], kr[0, rows, hs], LAST)
            bwd = dot(qd[1, rows, hs], kr[1, rows, hs], LAST)
            score = jnp.where(lower, fwd, 0.0) + jnp.where(upper, bwd, 0.0)
            o_v[rows, hs] = dot(score.astype(BF16), v[:, hs])

    def by_blocks(body):
        def step(i, carry):
            for u in range(UNROLL):
                body(i * UNROLL + u)
            return carry

        lax.fori_loop(0, NB // UNROLL, step, 0)

    mark("pass2")
    by_blocks(pass2_block)


    mark("owfwd")
    ow_forward()
    mark("roww")
    for o in (1, 3, 2):
        row_got(o)
    mark("rowc")
    for d in range(2):
        state = jnp.zeros((CH, HD), F32)
        log = [jnp.zeros((1, HD), F32)] * HEADS
        for j in range(4) if d == 0 else range(3, -1, -1):
            own = load_log(row_in, j, d)
            state = jnp.concatenate(
                [
                    state[h * HD : (h + 1) * HD] * jnp.exp(own[h])
                    + row_in[j, d, h * HD : (h + 1) * HD, :].astype(F32)
                    for h in range(HEADS)
                ],
                axis=0,
            )
            log = [log[h] + own[h] for h in range(HEADS)]
        store_state(col_in, z, d, state, jnp.concatenate(log, axis=1))
    for o in (1, 3, 2):
        copy = col_copy(o)
        copy.start()
        started.append(copy)
    level0b(0, 1)
    sin[...] = jnp.zeros_like(sin)
    mark("colw")
    for o in (1, 3, 2):
        col_got(o)
    level1a(0)
    mark("combine")

    def chain(ref, at):
        def body(i, carry):
            d = lax.div(i + 4 - at, 4)
            j = (1 - d) * i + d * (3 + at - i)
            own = load_log(ref, j, d)
            for h in range(HEADS):
                hs = slice(h * HD, (h + 1) * HD)
                sin[d, hs, :] = sin[d, hs, :] * jnp.exp(own[h]) + ref[j, d, hs, :].astype(F32)
            return carry

        lax.fori_loop(0, 3, body, 0)

    chain(col_in, z)
    chain(row_in, x)

    for copy in loads[6:10]:
        if copy is not loads[6]:
            copy.wait()

    def pass3_block(blk):
        rows = pl.ds(pl.multiple_of(blk * BLK, BLK), BLK)
        for h in range(HEADS):
            hs = slice(h * HD, (h + 1) * HD)
            mixed = o_v[rows, hs]
            for d in range(2):
                qs = (qd[d, rows, hs].astype(F32) * em[d, blk, 0:1, hs]).astype(BF16)
                state = sx[d, blk, hs, :].astype(F32) + elx[d, blk, 0:1, hs] * sin[d, hs, :]
                mixed = mixed + dot(qs, state.astype(BF16), LAST)
            norm = mixed * lax.rsqrt(jnp.mean(mixed * mixed, axis=-1, keepdims=True) + EPS)
            g = gat_v[rows, hs].astype(F32)
            ga[tp, rows, hs] = (norm * hg_v[0:1, :] * (g * sigmoid(g))).astype(BF16)

    mark("pass3")
    by_blocks(pass3_block)

    HALF = TOK // 2

    class Gather:
        def __init__(self, buf, send_sem, recv_sem):
            self.buf, self.ss, self.rs = buf, send_sem, recv_sem

        def copy(self, k, slot, part, to):
            ref = self.buf.at[slot]
            if part is not None:
                ref = self.buf.at[slot, pl.ds(part * HALF, HALF)]
            return remote(ref, ref, self.ss.at[k], self.rs.at[k], (sp, to))

        def go(self, *args):
            copy = self.copy(*args)
            copy.start()
            started.append(copy)

        def got(self, k, slot, part):
            self.copy(k, slot, part, partner).wait_recv()

        def own(self):
            right, left = 2 * yp + core, 2 * ym + core
            self.go(0, tp, 0, right)
            self.go(3, tp, 1, left)
            self.go(6, tp, None, partner)
            self.go(1, tp, 1, right)
            self.go(2, tp, 0, left)

        def forward(self):
            left, right = 2 * ym + core, 2 * yp + core
            self.got(0, left, 0)
            self.go(4, left, 0, right)
            self.go(7, left, 0, partner)
            self.got(3, right, 1)
            self.go(5, right, 1, left)
            self.go(8, right, 1, partner)

        def from_side(self):
            left, right = 2 * ym + core, 2 * yp + core
            self.got(1, left, 1)
            self.go(9, left, 1, partner)
            self.got(2, right, 0)
            self.go(10, right, 0, partner)

        def from_far(self):
            far = 2 * y2 + core
            self.got(4, far, 0)
            self.go(11, far, 0, partner)
            self.got(5, far, 1)
            self.go(12, far, 1, partner)

        def other_core(self, chip):
            block = 2 * chip + other
            for k, part in {id(ym): ((7, 0), (9, 1)), id(yp): ((8, 1), (10, 0)), id(y2): ((11, 0), (12, 1))}[
                id(chip)
            ]:
                self.got(k, block, part)

    gathered = Gather(ga, g_send, g_recv)
    mark("gown")
    gathered.own()

    mark("owwait")
    for copy in loads[10:13]:
        copy.wait()
    ow_wait()

    def project(block, first=False):
        def tile(n, carry):
            cols = pl.ds(pl.multiple_of(n * 256, 256), 256)
            part = dot(ga[block], owc[pl.ds(pl.multiple_of(block * 256, 256), 256), cols])
            att[:, cols] = part if first else att[:, cols] + part
            return carry

        lax.fori_loop(0, OC // 256, tile, 0)

    mark("proj0")
    project(tp, True)
    mark("gpart")
    gathered.got(6, partner, None)
    project(partner)
    mark("lev2a_0")
    level1b(0)
    level2a(0, 0)
    level2a(0, 1)
    mark("gfwd")
    gathered.forward()
    mark("gside")
    gathered.from_side()
    mark("proj2")
    project(2 * ym + core)
    project(2 * yp + core)
    mark("lev2b_0")
    level2b(0, 0)
    level2b(0, 1)
    level0a(1)
    mark("gpart2")
    gathered.other_core(ym)
    project(2 * ym + other)
    gathered.other_core(yp)
    project(2 * yp + other)
    mark("gfar")
    gathered.from_far()
    project(2 * y2 + core)
    gathered.other_core(y2)
    project(2 * y2 + other)

    TILE = 128

    def middle(i, carry):
        rows = pl.ds(pl.multiple_of(i * TILE, TILE), TILE)
        xa[tp, rows, :] = (res_v[rows, :].astype(F32) + att[rows, :]).astype(BF16)
        return carry

    mark("middle")
    lax.fori_loop(0, TOK // TILE, middle, 0)

    spread = Gather(xa, x_send, x_recv)
    spread.own()
    def scale(chip, c, first=False):
        block = 2 * chip + c
        gain = ng_v[:, pl.ds(pl.multiple_of(block * OC, OC), OC)]
        cols = pl.ds(pl.multiple_of(c * OC, OC), OC)

        def body(i, carry):
            rows = pl.ds(pl.multiple_of(i * TILE, TILE), TILE)
            v = xa[block, rows, :].astype(F32)
            sq = v * v
            sq = (sq[:, 0:128] + sq[:, 128:256]) + (sq[:, 256:384] + sq[:, 384:512])
            ss[rows, :] = sq if first else ss[rows, :] + sq
            xg[rows, cols] = (v * gain).astype(BF16)
            return carry

        lax.fori_loop(0, TOK // TILE, body, 0)

    def lift(chip, first=False):
        def tile(n, carry):
            cols = pl.ds(pl.multiple_of(n * 256, 256), 256)
            part = dot(xg[...], wu[pl.ds(pl.multiple_of(chip * 2 * OC, 2 * OC), 2 * OC), cols])
            acc[:, cols] = part if first else acc[:, cols] + part
            return carry

        lax.fori_loop(0, FFL // 256, tile, 0)

    def lift_one(chip, c):
        def tile(n, carry):
            cols = pl.ds(pl.multiple_of(n * 256, 256), 256)
            rows = pl.ds(pl.multiple_of((chip * 2 + c) * OC, OC), OC)
            part = dot(xg[:, pl.ds(pl.multiple_of(c * OC, OC), OC)], wu[rows, cols])
            acc[:, cols] = acc[:, cols] + part
            return carry

        lax.fori_loop(0, FFL // 256, tile, 0)

    mark("scale0")
    scale(y, core, True)
    spread.got(6, partner, None)
    scale(y, other)
    mark("lev3_0")
    level3(0, 0)
    level3(0, 1)
    level0b(1, 0)
    level0b(1, 1)
    mark("xfwd")
    spread.forward()
    mark("lev1a_1")
    level1a(1)
    mark("lev4_0")
    level4(0, 0, range(4))
    level4(0, 1, range(4))
    mark("lift0")
    lift(y, True)
    mark("xside")
    spread.from_side()
    mark("lift1")
    scale(ym, core)
    lift_one(ym, core)
    spread.other_core(ym)
    scale(ym, other)
    lift_one(ym, other)
    mark("lev1_1")
    level1b(1)
    mark("lift2")
    scale(yp, core)
    spread.other_core(yp)
    scale(yp, other)
    lift(yp)
    mark("lev2a_1")
    level2a(1, 1)
    mark("xfar")
    spread.from_far()
    mark("lift3")
    scale(y2, core)
    lift_one(y2, core)
    spread.other_core(y2)
    scale(y2, other)
    lift_one(y2, other)

    def activate(i, carry):
        rows = pl.ds(pl.multiple_of(i * TILE, TILE), TILE)
        total = jnp.sum(ss[rows, :], axis=-1, keepdims=True)
        v = jnp.maximum(acc[rows, :] * lax.rsqrt(total / D + EPS), 0.0)
        hid[rows, :] = (v * v).astype(BF16)
        return carry

    mark("act")
    lax.fori_loop(0, TOK // TILE, activate, 0)


    SHARDS = (
        (1, 0), (0, 0), (1, 1), (1, -1), (1, 2), (0, 1), (0, -1), (0, 2), (2, 2)
    )

    class Step:
        def __init__(self, n):
            self.n = n
            dx, dz = SHARDS[n]
            self.single = n >= 7
            self.dx = dx % 2
            zs = ring(z, dz)
            column = lax.rem(x + dx, 2)
            self.keep = lax.div(ring(x, dx), 2) == core
            self.kept = jnp.where(self.keep, 1, 0)
            self.slot = self.dx * 4 + zs
            self.first = zs * 4 + column
            self.delta = lax.rem(zs + 4 - y, 4)
            self.odd = lax.rem(self.delta, 2) == 1
            self.far = self.delta == 2
            self.k = lax.div(self.delta, 2)
            self.to = 2 * lax.rem(y + self.delta, 4) + core

        def chip(self):
            return remote(
                pp.at[0, self.slot], d2r.at[self.slot], c_send.at[self.n], c_recv.at[self.n], (sp, partner)
            )

        def half(self, k):
            return pl.ds(pl.multiple_of(k * HALF, HALF), HALF)

        def out_far(self, k):
            return remote(
                pp.at[1, self.slot, self.half(k)], ra.at[self.slot], r_send.at[self.n, k],
                r_recv.at[self.n], (sp, 2 * (yp, ym)[k] + core),
            )

        def out_near(self, k):
            return remote(
                pp.at[1, self.slot, self.half(k)], ee.at[self.k, self.dx, self.half(k)],
                e_send.at[self.n, k], e_recv.at[self.k, self.dx, k], (sp, self.to),
            )

        def compute(self):
            mark("comp%d" % self.n)
            def part(i, carry):
                first = (self.first + 2 * (other + i * (core - other))) * SHARD
                rows = wd[pl.ds(pl.multiple_of(first, SHARD), SHARD), :]
                pp[i, self.slot] = dot(hid[...], rows, LAST).astype(BF16)

                @pl.when(i == 0)
                def _():
                    self.chip().start()

                return carry

            if self.single:
                part(self.kept, 0)
            else:
                lax.fori_loop(0, 2, part, 0)

        def when_kept(self, body):
            if self.single:
                pl.when(self.keep)(body)
            else:
                body()

        def chip_sum(self):
            mark("cs%d" % self.n)
            self.when_kept(self.chip_sum_kept)

        def chip_sum_kept(self):
            self.chip().wait_recv()

            def add(i, carry):
                rows = pl.ds(pl.multiple_of(i * TILE, TILE), TILE)
                total = pp[1, self.slot, rows, :].astype(F32) + d2r[self.slot, rows, :].astype(F32)
                pp[1, self.slot, rows, :] = total.astype(BF16)
                return carry

            lax.fori_loop(0, TOK // TILE, add, 0)

            @pl.when(self.far)
            def _():
                self.out_far(0).start()
                self.out_far(1).start()

            @pl.when(self.odd)
            def _():
                self.out_near(1 - self.k).start()

        def join(self):
            mark("jn%d" % self.n)
            self.when_kept(self.join_kept)

        def join_kept(self):
            @pl.when(self.odd)
            def _():
                remote(
                    ra.at[self.slot], ra.at[self.slot], r_send.at[self.n, 0], r_recv.at[self.n],
                    (sp, self.to),
                ).wait_recv()

                def add(i, carry):
                    rows = pl.ds(pl.multiple_of(self.k * HALF + i * TILE, TILE), TILE)
                    got = ra[self.slot, pl.ds(pl.multiple_of(i * TILE, TILE), TILE), :]
                    total = pp[1, self.slot, rows, :].astype(F32) + got.astype(F32)
                    pp[1, self.slot, rows, :] = total.astype(BF16)
                    return carry

                lax.fori_loop(0, HALF // TILE, add, 0)
                self.out_near(self.k).start()

        def drain(self):
            if self.single:
                pl.when(jnp.logical_not(self.keep))(lambda: self.chip().wait_send())
            else:
                self.chip().wait_send()
            self.when_kept(self.drain_kept)

        def drain_kept(self):
            @pl.when(self.far)
            def _():
                self.out_far(0).wait_send()
                self.out_far(1).wait_send()

            @pl.when(self.odd)
            def _():
                self.out_near(1 - self.k).wait_send()
                self.out_near(self.k).wait_send()

    steps = [Step(n) for n in range(9)]
    steps[0].compute()
    steps[0].chip_sum()
    mark("lev2_1")
    level2b(1, 0)
    level2a(1, 0)
    level2b(1, 1)
    steps[2].compute()
    steps[3].compute()
    steps[2].chip_sum()
    mark("w7")
    level4(1, 0, (0,))
    level4(1, 1, (0,))
    steps[7].compute()
    steps[3].chip_sum()
    steps[1].compute()
    steps[7].chip_sum()
    steps[1].chip_sum()
    mark("w4")
    level4(1, 0, (1, 2))
    level3(1, 1)
    steps[4].compute()
    steps[0].join()
    steps[4].chip_sum()
    mark("w30")
    level3(1, 0)
    steps[2].join()
    steps[3].join()
    mark("w5")
    level4(1, 1, (1, 2))
    steps[5].compute()
    steps[7].join()
    steps[6].compute()
    steps[5].chip_sum()
    mark("w8")
    level4(1, 0, (3,))
    level4(1, 1, (3,))
    steps[8].compute()
    steps[6].chip_sum()
    steps[1].join()
    steps[4].join()
    steps[8].chip_sum()
    for n in (5, 6, 8):
        steps[n].join()
    mark("ewait")

    for dx in range(2):
        slot = dx * 4 + y
        for k in range(2):
            for half in range(2):
                rows = pl.ds(half * HALF, HALF)
                remote(
                    ee.at[k, dx, rows], ee.at[k, dx, rows], e_send.at[0, 0], e_recv.at[k, dx, half],
                    (sp, partner),
                ).wait_recv()
        cols = pl.ds(pl.multiple_of(lax.rem(x + dx, 2) * SHARD, SHARD), SHARD)

        def finish(i, carry):
            rows = pl.ds(pl.multiple_of(i * TILE, TILE), TILE)
            total = pp[1, slot, rows, :].astype(F32)
            total = total + (ee[0, dx, rows, :].astype(F32) + ee[1, dx, rows, :].astype(F32))
            out[rows, cols] = (xa[tp, rows, cols].astype(F32) + total).astype(BF16)
            return carry

        lax.fori_loop(0, TOK // TILE, finish, 0)
    mark("final")
    for copy in started:
        copy.wait_send()
    for step in steps:
        step.drain()
    mark(None)


def per_device(
    residual, values, forget_onward, forget_reverse, surge_log_decay, gate_limit_complement,
    readout_query, output_gate, head_norm_gain, output_weight, mixer_norm_gain, up_weight,
    down_weight,
):
    any_spec = pl.BlockSpec(memory_space=pl.ANY)
    vmem, dma = pltpu.VMEM, pltpu.SemaphoreType.DMA
    scratch = [
        vmem((TOK, OC), BF16), vmem((TOK, CH), BF16), vmem((TOK, CH), BF16), vmem((TOK, CH), BF16),
        vmem((8, TOK), F32), vmem((TOK, 8), F32), vmem((2, CH), F32), vmem((TOK, CH), BF16), vmem((TOK, CH), BF16),
        vmem((1, HD), F32), vmem((1, D), F32),
        vmem((D, FFL), BF16), vmem((D, FFL), BF16), vmem((2048, OC), BF16),
        vmem((8, TOK, CH), BF16), vmem((8, TOK, OC), BF16),
        vmem((2, TOK, CH), BF16), vmem((2, TOK, CH), BF16), vmem((2, NB, CH, HD), BF16),
        vmem((2, NB, 8, CH), F32), vmem((2, NB, 8, CH), F32),
        vmem((2, CH, HD), F32), vmem((2, 8, CH), F32),
        vmem((4, 2, ST_ROWS, HD), BF16), vmem((4, 2, ST_ROWS, HD), BF16), vmem((2, CH, HD), F32),
        vmem((TOK, CH), F32), vmem((TOK, OC), F32),
        vmem((TOK, 2 * OC), BF16), vmem((TOK, HD), F32), vmem((TOK, FFL), F32), vmem((TOK, FFL), BF16),
        vmem((2, 8, TOK, SHARD), BF16), vmem((8, TOK, SHARD), BF16),
        vmem((8, TOK // 2, SHARD), BF16), vmem((2, 2, TOK, SHARD), BF16),
        vmem((2, 2, 128, OC), BF16), vmem((2, TOK, CH), F32),
        dma((13,)), dma((2, 2, 20)), dma((2, 2, 20)), dma((13,)), dma((13,)), dma((6,)), dma((6,)),
        dma((13,)), dma((13,)), dma((13,)), dma((13,)), dma((9,)), dma((9,)), dma((9, 2)), dma((9,)),
        dma((9, 2)), dma((2, 2, 2)),
    ]
    return pl.pallas_call(
        kernel,
        out_shape=pltpu.VMEM((TOK, OC), BF16),
        in_specs=[any_spec] * 13,
        out_specs=pl.BlockSpec(memory_space=pltpu.VMEM),
        scratch_shapes=scratch,
        compiler_params=pltpu.CompilerParams(
            collective_id=0, has_side_effects=True, vmem_limit_bytes=66_000_000
        ),
        name="layer",
    )(
        residual, values, forget_onward, forget_reverse, surge_log_decay.T, gate_limit_complement,
        readout_query, output_gate, head_norm_gain.reshape(1, HD), output_weight,
        mixer_norm_gain.reshape(1, D), up_weight, down_weight,
    )


def solution(mesh):
    both = P("sp", "tp")
    placed = (
        both, both, both, both, both, P(None, "tp"), both, both, P(), P("tp", None), P(), both, both,
    )
    return jax.shard_map(
        per_device, mesh=mesh, in_specs=placed, out_specs=both, check_vma=False
    )
```

```python
import functools

import jax
import jax.numpy as jnp
from jax import lax
from jax.experimental import pallas as pl
from jax.experimental.pallas import tpu as pltpu
from jax.sharding import PartitionSpec as P

D = 4096
HD = 128
HEADS = 2
CH = HEADS * HD
TOK = 768
BLK = 64
UNROLL = 3
NB = TOK // BLK
OC = 512
FFL = 1024
SHARD = 256
QUARTER = 64
EPS = 1e-06
MESH = pl.DeviceIdType.MESH
F32 = jnp.float32
BF16 = jnp.bfloat16
ST_ROWS = 272


def dot(a, b, dims=(((1,), (0,)), ((), ()))):
    return lax.dot_general(a, b, dims, preferred_element_type=F32)


LAST = (((1,), (1,)), ((), ()))
FIRST = (((0,), (0,)), ((), ()))


def sigmoid(x):
    return 1.0 / (1.0 + jnp.exp(-x))


def kernel(
    residual, values, f_on, f_rev, surge, glc, query, gate, head_gain, out_w,
    norm_gain, up_w, down_w,
    out,
    res_v, val_v, fon_v, frev_v, sur_t, sur_v, glc_v, que_v, gat_v, hg_v, ng_v,
    wu, wd, owc, ga, xa,
    qd, kr, sx, em, elx, run_state, run_log, row_in, col_in, sin, o_v, att,
    xg, ss, acc, hid,
    pp, d2r, ra, ee, relay, rel,
    in_sem, w_send, w_recv, ow_send, ow_recv, st_send, st_recv,
    g_send, g_recv, x_send, x_recv, c_send, c_recv, r_send, r_recv, e_send, e_recv,
):
    sp, tp = lax.axis_index("sp"), lax.axis_index("tp")
    x, z = lax.rem(sp, 4), lax.div(sp, 4)
    core, y = lax.rem(tp, 2), lax.div(tp, 2)
    other = 1 - core

    cur = [None]

    def mark(name):
        if cur[0] is not None:
            cur[0].__exit__(None, None, None)
        cur[0] = jax.named_scope(name) if name else None
        if name:
            cur[0].__enter__()

    mark("start")

    def ring(v, k):
        return lax.rem(v + (k % 4), 4)

    yp, ym, y2 = ring(y, 1), ring(y, 3), ring(y, 2)
    partner = 2 * y + other

    barrier = pltpu.get_barrier_semaphore()
    peers = [(z * 4 + ring(x, o), tp) for o in (1, 3, 2)]
    peers += [(ring(z, o) * 4 + x, tp) for o in (1, 3, 2)]
    peers += [(sp, 2 * near + c) for near in (yp, ym) for c in range(2)] + [(sp, partner)]
    for peer in peers:
        pl.semaphore_signal(barrier, inc=1, device_id=peer, device_id_type=MESH)

    own_rows = pl.ds(pl.multiple_of(sp * SHARD, SHARD), SHARD)
    ow_rows = pl.ds(pl.multiple_of(tp * 256, 256), 256)
    own_cols = pl.ds(pl.multiple_of(tp * OC, OC), OC)
    loads = [
        (f_on, fon_v), (f_rev, frev_v), (surge, sur_t.at[pl.ds(0, HEADS)]), (glc, glc_v), (query, que_v),
        (values, val_v), (gate, gat_v), (head_gain, hg_v), (residual, res_v), (norm_gain, ng_v),
        (up_w, wu.at[own_rows]), (down_w, wd.at[own_rows]),
        (out_w.at[:, own_cols], owc.at[ow_rows]),
    ]
    loads = [pltpu.make_async_copy(a, b, in_sem.at[i]) for i, (a, b) in enumerate(loads)]
    for copy in loads:
        copy.start()

    pl.semaphore_wait(barrier, len(peers))

    def remote(src, dst, ss_, rs_, dev):
        return pltpu.make_async_remote_copy(
            src_ref=src, dst_ref=dst, send_sem=ss_, recv_sem=rs_, device_id=dev, device_id_type=MESH
        )

    started = []

    def go(copy):
        copy.start()
        started.append(copy)

    weights = ((up_w, wu), (down_w, wd))

    def sp_at(half, i, j):
        return ring(z, j) * 4 + ring(x, i) if half == 0 else ring(z, i) * 4 + ring(x, j)

    def piece(t, half, i, j, part):
        start, size = (0, 2 * QUARTER) if part is None else (part * QUARTER, QUARTER)
        first = sp_at(half, i, j) * SHARD + half * 2 * QUARTER + start
        return weights[t][1].at[pl.ds(pl.multiple_of(first, QUARTER), size)]

    FWD = (0, -1, 1, 2)

    def w_copy(t, half, slot, i, j, part, to, src=None):
        ref = piece(t, half, i, j, part)
        return remote(
            ref if src is None else src, ref, w_send.at[t, half, slot], w_recv.at[t, half, slot],
            (sp_at(half, *to), tp),
        )

    def w_go(*args, **kw):
        copy = w_copy(*args, **kw)
        copy.start()
        started.append(copy)

    def w_got(t, half, slot, i, j, part):
        w_copy(t, half, slot, i, j, part, (1, 0)).wait_recv()

    def w_second(t, half, n, src=None):
        i = FWD[n]
        w_go(t, half, 4 + 4 * n, i, 0, None, (0, 1), src=src)
        w_go(t, half, 5 + 4 * n, i, 0, None, (0, -1), src=src)

    def w_second_forward(t, half, n):
        i = FWD[n]
        w_got(t, half, 4 + 4 * n, i, -1, None)
        w_go(t, half, 6 + 4 * n, i, -1, 0, (0, 1))
        w_got(t, half, 5 + 4 * n, i, 1, None)
        w_go(t, half, 7 + 4 * n, i, 1, 1, (0, -1))

    def level0a(t):
        for half in range(2):
            src = weights[t][0].at[pl.ds(half * 2 * QUARTER, 2 * QUARTER)]
            w_go(t, half, 0, 0, 0, None, (1, 0), src=src)
            w_go(t, half, 1, 0, 0, None, (-1, 0), src=src)

    def level0b(t, half):
        src = weights[t][0].at[pl.ds(half * 2 * QUARTER, 2 * QUARTER)]
        w_second(t, half, 0, src=src)

    def level1a(t):
        for half in range(2):
            w_got(t, half, 0, -1, 0, None)
            w_go(t, half, 2, -1, 0, 0, (1, 0))
            w_got(t, half, 1, 1, 0, None)
            w_go(t, half, 3, 1, 0, 1, (-1, 0))
        for half in range(2):
            w_second(t, half, 1)
            w_second(t, half, 2)

    def level1b(t):
        for half in range(2):
            w_second_forward(t, half, 0)

    def level2a(t, half):
        w_got(t, half, 2, 2, 0, 0)
        w_got(t, half, 3, 2, 0, 1)
        w_second(t, half, 3)

    def level2b(t, half):
        w_second_forward(t, half, 1)
        w_second_forward(t, half, 2)

    def level3(t, half):
        w_second_forward(t, half, 3)

    def level4(t, half, blocks):
        for n in blocks:
            w_got(t, half, 6 + 4 * n, FWD[n], 2, 0)
            w_got(t, half, 7 + 4 * n, FWD[n], 2, 1)

    mark("w0")
    level0a(0)

    def ow_cols(to):
        return pl.ds(pl.multiple_of(to * OC, OC), OC)

    def ow_rows_of(source, k=None):
        first, size = (0, 256) if k is None else (k * 128, 128)
        return pl.ds(pl.multiple_of(source * 256 + first, 128), size)

    near = (yp, ym)

    def ow_leg1(k, c):
        return remote(
            out_w.at[pl.ds(k * 128, 128), ow_cols(2 * y2 + c)], relay.at[k, c],
            ow_send.at[2 * k + c], ow_recv.at[2 * k + c], (sp, 2 * near[k] + core),
        )

    def ow_direct(k, c):
        return remote(
            out_w.at[:, ow_cols(2 * near[k] + c)], owc.at[ow_rows],
            ow_send.at[4 + 2 * k + c], ow_recv.at[4 + 2 * k + core], (sp, 2 * near[k] + c),
        )

    def ow_partner():
        return remote(
            out_w.at[:, ow_cols(partner)], owc.at[ow_rows], ow_send.at[8], ow_recv.at[8], (sp, partner)
        )

    def ow_leg2(k, c):
        return remote(
            relay.at[k, c], owc.at[ow_rows_of(2 * near[1 - k] + core, k)],
            ow_send.at[9 + 2 * k + c], ow_recv.at[9 + 2 * k + core], (sp, 2 * near[k] + c),
        )

    def ow_forward():
        for k in range(2):
            for c in range(2):
                ow_leg1(k, c).wait_recv()
                go(ow_leg2(k, c))

    def ow_wait():
        def landed(rows, sem):
            ref = owc.at[rows]
            remote(ref, ref, ow_send.at[8], ow_recv.at[sem], (sp, partner)).wait_recv()

        landed(ow_rows_of(partner), 8)
        for k in range(2):
            for c in range(2):
                landed(ow_rows_of(2 * near[1 - k] + c), 4 + 2 * k + c)
        for k in range(2):
            for c in range(2):
                landed(ow_rows_of(2 * y2 + c, k), 9 + 2 * k + c)

    for k in range(2):
        for c in range(2):
            go(ow_leg1(k, c))
    for k in range(2):
        for c in range(2):
            go(ow_direct(k, c))
    go(ow_partner())

    mark("loadwait")
    for copy in loads[:7]:
        copy.wait()

    mark("pass1")
    row_id = lax.broadcasted_iota(jnp.int32, (BLK, BLK), 0)
    col_id = lax.broadcasted_iota(jnp.int32, (BLK, BLK), 1)
    lower, upper = row_id >= col_id, row_id <= col_id
    run_state[...] = jnp.zeros_like(run_state)
    run_log[...] = jnp.zeros_like(run_log)
    sur_v[...] = jnp.concatenate([sur_t[0:HEADS, :], jnp.zeros((8 - HEADS, TOK), F32)], axis=0).T
    sums = tuple(
        jnp.concatenate([jnp.where(tri, 1.0, 0.0)] * 3, axis=1).astype(BF16) for tri in (lower, upper)
    )

    def split3(v):
        a = v.astype(BF16)
        rest = v - a.astype(F32)
        b = rest.astype(BF16)
        return jnp.concatenate([a, b, (rest - b.astype(F32)).astype(BF16)], axis=0)

    def pass1_block(d, blk):
        logits = (fon_v, frev_v)[d]
        mid_at, end_at = ((BLK // 2 - 1, BLK - 1), (BLK // 2, 0))[d]
        rows = pl.ds(pl.multiple_of(blk * BLK, BLK), BLK)
        key = glc_v[d : d + 1, :] / (1.0 + jnp.exp(logits[rows, :].astype(F32)))
        sg = sur_v[rows, :]
        sg = jnp.concatenate(
            [jnp.broadcast_to(sg[:, h : h + 1], (BLK, HD)) for h in range(HEADS)], axis=1
        )
        run = dot(sums[d], split3(jnp.log1p(-key) + sg))
        mid, end = run[mid_at : mid_at + 1, :], run[end_at : end_at + 1, :]
        away = mid - run
        rel[d, rows, :] = away
        k = key * jnp.exp(away)
        kr[d, rows, :] = k.astype(BF16)
        tail = (k * jnp.exp(end - mid)).astype(BF16)
        v = val_v[rows, :]
        new = [
            dot(v[:, h * HD : (h + 1) * HD], tail[:, h * HD : (h + 1) * HD], FIRST)
            for h in range(HEADS)
        ]
        em[d, blk] = jnp.broadcast_to(jnp.exp(mid), (8, CH))
        return end, new

    def pass1(step, carry):
        blocks = [
            (d, step * UNROLL + u if d == 0 else NB - 1 - (step * UNROLL + u))
            for u in range(UNROLL)
            for d in range(2)
        ]
        parts = [pass1_block(d, blk) for d, blk in blocks]
        for (d, blk), (end, new) in zip(blocks, parts):
            gone = run_log[d, 0:1, :]
            elx[d, blk] = jnp.broadcast_to(jnp.exp(gone), (8, CH))
            run_log[d] = jnp.broadcast_to(gone + end, (8, CH))
            decay = jnp.exp(end)
            for h in range(HEADS):
                hs = slice(h * HD, (h + 1) * HD)
                state = run_state[d, hs, :]
                sx[d, blk, hs, :] = state.astype(BF16)
                run_state[d, hs, :] = state * decay[:, hs] + new[h]
        return carry

    lax.fori_loop(0, NB // UNROLL, pass1, 0)

    mark("stsend")
    def store_state(ref, at, d, state, log):
        ref[at, d, 0:CH, :] = state.astype(BF16)
        high = log.astype(BF16).astype(F32)
        rest = log - high
        ref[at, d, CH:ST_ROWS, :] = jnp.concatenate(
            [high[:, :HD], high[:, HD:], rest[:, :HD], rest[:, HD:], jnp.zeros((12, HD), F32)], axis=0
        ).astype(BF16)

    def load_log(ref, at, d):
        tail = ref[at, d, CH:ST_ROWS, :].astype(F32)
        return [tail[h : h + 1, :] + tail[2 + h : 3 + h, :] for h in range(HEADS)]

    for d in range(2):
        store_state(row_in, x, d, run_state[d], run_log[d, 0:1, :])

    def row_copy(o):
        return remote(
            row_in.at[x], row_in.at[x], st_send.at[o - 1], st_recv.at[o - 1],
            (z * 4 + ring(x, o), tp),
        )

    def row_got(o):
        ref = row_in.at[ring(x, -o)]
        remote(ref, ref, st_send.at[o - 1], st_recv.at[o - 1], (z * 4 + ring(x, o), tp)).wait_recv()

    def col_copy(o):
        ref = col_in.at[z, lax.div(z + o, 4)]
        return remote(
            ref, ref, st_send.at[o + 2], st_recv.at[o + 2], (ring(z, o) * 4 + x, tp)
        )

    def col_got(o):
        ref = col_in.at[ring(z, -o), lax.div(z + 4 - o, 4) * -1 + 1]
        remote(ref, ref, st_send.at[o + 2], st_recv.at[o + 2], (ring(z, o) * 4 + x, tp)).wait_recv()

    for o in (1, 3, 2):
        copy = row_copy(o)
        copy.start()
        started.append(copy)
    mark("l0b")
    level0b(0, 0)

    def pass2_block(blk):
        rows = pl.ds(pl.multiple_of(blk * BLK, BLK), BLK)
        v = val_v[rows, :]
        q = que_v[rows, :].astype(F32)
        q = q * sigmoid(q) * (HD ** -0.5)
        for d in range(2):
            qd[d, rows, :] = (q * jnp.exp(-rel[d, rows, :])).astype(BF16)
        for h in range(HEADS):
            hs = slice(h * HD, (h + 1) * HD)
            fwd = dot(qd[0, rows, hs], kr[0, rows, hs], LAST)
            bwd = dot(qd[1, rows, hs], kr[1, rows, hs], LAST)
            score = jnp.where(lower, fwd, 0.0) + jnp.where(upper, bwd, 0.0)
            o_v[rows, hs] = dot(score.astype(BF16), v[:, hs])

    def by_blocks(body):
        def step(i, carry):
            for u in range(UNROLL):
                body(i * UNROLL + u)
            return carry

        lax.fori_loop(0, NB // UNROLL, step, 0)

    mark("pass2")
    by_blocks(pass2_block)


    mark("owfwd")
    ow_forward()
    mark("roww")
    for o in (1, 3, 2):
        row_got(o)
    mark("rowc")
    for d in range(2):
        state = jnp.zeros((CH, HD), F32)
        log = [jnp.zeros((1, HD), F32)] * HEADS
        for j in range(4) if d == 0 else range(3, -1, -1):
            own = load_log(row_in, j, d)
            state = jnp.concatenate(
                [
                    state[h * HD : (h + 1) * HD] * jnp.exp(own[h])
                    + row_in[j, d, h * HD : (h + 1) * HD, :].astype(F32)
                    for h in range(HEADS)
                ],
                axis=0,
            )
            log = [log[h] + own[h] for h in range(HEADS)]
        store_state(col_in, z, d, state, jnp.concatenate(log, axis=1))
    for o in (1, 3, 2):
        copy = col_copy(o)
        copy.start()
        started.append(copy)
    level0b(0, 1)
    sin[...] = jnp.zeros_like(sin)
    mark("colw")
    for o in (1, 3, 2):
        col_got(o)
    level1a(0)
    mark("combine")

    def chain(ref, at):
        def body(i, carry):
            d = lax.div(i + 4 - at, 4)
            j = (1 - d) * i + d * (3 + at - i)
            own = load_log(ref, j, d)
            for h in range(HEADS):
                hs = slice(h * HD, (h + 1) * HD)
                sin[d, hs, :] = sin[d, hs, :] * jnp.exp(own[h]) + ref[j, d, hs, :].astype(F32)
            return carry

        lax.fori_loop(0, 3, body, 0)

    chain(col_in, z)
    chain(row_in, x)

    for copy in loads[6:10]:
        if copy is not loads[6]:
            copy.wait()

    def pass3_block(blk):
        rows = pl.ds(pl.multiple_of(blk * BLK, BLK), BLK)
        for h in range(HEADS):
            hs = slice(h * HD, (h + 1) * HD)
            mixed = o_v[rows, hs]
            for d in range(2):
                qs = (qd[d, rows, hs].astype(F32) * em[d, blk, 0:1, hs]).astype(BF16)
                state = sx[d, blk, hs, :].astype(F32) + elx[d, blk, 0:1, hs] * sin[d, hs, :]
                mixed = mixed + dot(qs, state.astype(BF16), LAST)
            norm = mixed * lax.rsqrt(jnp.mean(mixed * mixed, axis=-1, keepdims=True) + EPS)
            g = gat_v[rows, hs].astype(F32)
            ga[tp, rows, hs] = (norm * hg_v[0:1, :] * (g * sigmoid(g))).astype(BF16)

    mark("pass3")
    by_blocks(pass3_block)

    HALF = TOK // 2

    class Gather:
        def __init__(self, buf, send_sem, recv_sem):
            self.buf, self.ss, self.rs = buf, send_sem, recv_sem

        def copy(self, k, slot, part, to):
            ref = self.buf.at[slot]
            if part is not None:
                ref = self.buf.at[slot, pl.ds(part * HALF, HALF)]
            return remote(ref, ref, self.ss.at[k], self.rs.at[k], (sp, to))

        def go(self, *args):
            copy = self.copy(*args)
            copy.start()
            started.append(copy)

        def got(self, k, slot, part):
            self.copy(k, slot, part, partner).wait_recv()

        def own(self):
            right, left = 2 * yp + core, 2 * ym + core
            self.go(0, tp, 0, right)
            self.go(3, tp, 1, left)
            self.go(6, tp, None, partner)
            self.go(1, tp, 1, right)
            self.go(2, tp, 0, left)

        def forward(self):
            left, right = 2 * ym + core, 2 * yp + core
            self.got(0, left, 0)
            self.go(4, left, 0, right)
            self.go(7, left, 0, partner)
            self.got(3, right, 1)
            self.go(5, right, 1, left)
            self.go(8, right, 1, partner)

        def from_side(self):
            left, right = 2 * ym + core, 2 * yp + core
            self.got(1, left, 1)
            self.go(9, left, 1, partner)
            self.got(2, right, 0)
            self.go(10, right, 0, partner)

        def from_far(self):
            far = 2 * y2 + core
            self.got(4, far, 0)
            self.go(11, far, 0, partner)
            self.got(5, far, 1)
            self.go(12, far, 1, partner)

        def other_core(self, chip):
            block = 2 * chip + other
            for k, part in {id(ym): ((7, 0), (9, 1)), id(yp): ((8, 1), (10, 0)), id(y2): ((11, 0), (12, 1))}[
                id(chip)
            ]:
                self.got(k, block, part)

    gathered = Gather(ga, g_send, g_recv)
    mark("gown")
    gathered.own()

    mark("owwait")
    for copy in loads[10:13]:
        copy.wait()
    ow_wait()

    def project(block, first=False):
        def tile(n, carry):
            cols = pl.ds(pl.multiple_of(n * 256, 256), 256)
            part = dot(ga[block], owc[pl.ds(pl.multiple_of(block * 256, 256), 256), cols])
            att[:, cols] = part if first else att[:, cols] + part
            return carry

        lax.fori_loop(0, OC // 256, tile, 0)

    mark("proj0")
    project(tp, True)
    mark("gpart")
    gathered.got(6, partner, None)
    project(partner)
    mark("lev2a_0")
    level1b(0)
    level2a(0, 0)
    level2a(0, 1)
    mark("gfwd")
    gathered.forward()
    mark("gside")
    gathered.from_side()
    mark("proj2")
    project(2 * ym + core)
    project(2 * yp + core)
    mark("lev2b_0")
    level2b(0, 0)
    level2b(0, 1)
    level0a(1)
    mark("gpart2")
    gathered.other_core(ym)
    project(2 * ym + other)
    gathered.other_core(yp)
    project(2 * yp + other)
    mark("gfar")
    gathered.from_far()
    project(2 * y2 + core)
    gathered.other_core(y2)
    project(2 * y2 + other)

    TILE = 128

    def middle(i, carry):
        rows = pl.ds(pl.multiple_of(i * TILE, TILE), TILE)
        xa[tp, rows, :] = (res_v[rows, :].astype(F32) + att[rows, :]).astype(BF16)
        return carry

    mark("middle")
    lax.fori_loop(0, TOK // TILE, middle, 0)

    spread = Gather(xa, x_send, x_recv)
    spread.own()
    def scale(chip, c, first=False):
        block = 2 * chip + c
        gain = ng_v[:, pl.ds(pl.multiple_of(block * OC, OC), OC)]
        cols = pl.ds(pl.multiple_of(c * OC, OC), OC)

        def body(i, carry):
            rows = pl.ds(pl.multiple_of(i * TILE, TILE), TILE)
            v = xa[block, rows, :].astype(F32)
            sq = v * v
            sq = (sq[:, 0:128] + sq[:, 128:256]) + (sq[:, 256:384] + sq[:, 384:512])
            ss[rows, :] = sq if first else ss[rows, :] + sq
            xg[rows, cols] = (v * gain).astype(BF16)
            return carry

        lax.fori_loop(0, TOK // TILE, body, 0)

    def lift(chip, first=False):
        def tile(n, carry):
            cols = pl.ds(pl.multiple_of(n * 256, 256), 256)
            part = dot(xg[...], wu[pl.ds(pl.multiple_of(chip * 2 * OC, 2 * OC), 2 * OC), cols])
            acc[:, cols] = part if first else acc[:, cols] + part
            return carry

        lax.fori_loop(0, FFL // 256, tile, 0)

    def lift_one(chip, c):
        def tile(n, carry):
            cols = pl.ds(pl.multiple_of(n * 256, 256), 256)
            rows = pl.ds(pl.multiple_of((chip * 2 + c) * OC, OC), OC)
            part = dot(xg[:, pl.ds(pl.multiple_of(c * OC, OC), OC)], wu[rows, cols])
            acc[:, cols] = acc[:, cols] + part
            return carry

        lax.fori_loop(0, FFL // 256, tile, 0)

    mark("scale0")
    scale(y, core, True)
    spread.got(6, partner, None)
    scale(y, other)
    mark("lev3_0")
    level3(0, 0)
    level3(0, 1)
    level0b(1, 0)
    level0b(1, 1)
    mark("xfwd")
    spread.forward()
    mark("lev1a_1")
    level1a(1)
    mark("lev4_0")
    level4(0, 0, range(4))
    level4(0, 1, range(4))
    mark("lift0")
    lift(y, True)
    mark("xside")
    spread.from_side()
    mark("lift1")
    scale(ym, core)
    lift_one(ym, core)
    spread.other_core(ym)
    scale(ym, other)
    lift_one(ym, other)
    mark("lev1_1")
    level1b(1)
    mark("lift2")
    scale(yp, core)
    spread.other_core(yp)
    scale(yp, other)
    lift(yp)
    mark("lev2a_1")
    level2a(1, 1)
    mark("xfar")
    spread.from_far()
    mark("lift3")
    scale(y2, core)
    lift_one(y2, core)
    spread.other_core(y2)
    scale(y2, other)
    lift_one(y2, other)

    def activate(i, carry):
        rows = pl.ds(pl.multiple_of(i * TILE, TILE), TILE)
        total = jnp.sum(ss[rows, :], axis=-1, keepdims=True)
        v = jnp.maximum(acc[rows, :] * lax.rsqrt(total / D + EPS), 0.0)
        hid[rows, :] = (v * v).astype(BF16)
        return carry

    mark("act")
    lax.fori_loop(0, TOK // TILE, activate, 0)


    SHARDS = (
        (1, 0), (0, 0), (1, 1), (1, -1), (1, 2),
        (0, 1), (0, -1), (0, 2), (2, 2), (2, 1), (2, -1),
    )

    class Step:
        def __init__(self, n):
            self.n = n
            dx, dz = SHARDS[n]
            self.single = n >= 5
            self.dx = dx % 2
            zs = ring(z, dz)
            column = lax.rem(x + dx, 2)
            self.keep = lax.div(ring(x, dx), 2) == core
            self.kept = jnp.where(self.keep, 1, 0)
            self.slot = self.dx * 4 + zs
            self.first = zs * 4 + column
            self.delta = lax.rem(zs + 4 - y, 4)
            self.odd = lax.rem(self.delta, 2) == 1
            self.far = self.delta == 2
            self.k = lax.div(self.delta, 2)
            self.to = 2 * lax.rem(y + self.delta, 4) + core

        def chip(self):
            return remote(
                pp.at[0, self.slot], d2r.at[self.slot], c_send.at[self.n], c_recv.at[self.n], (sp, partner)
            )

        def half(self, k):
            return pl.ds(pl.multiple_of(k * HALF, HALF), HALF)

        def out_far(self, k):
            return remote(
                pp.at[1, self.slot, self.half(k)], ra.at[self.slot], r_send.at[self.n, k],
                r_recv.at[self.n], (sp, 2 * (yp, ym)[k] + core),
            )

        def out_near(self, k):
            return remote(
                pp.at[1, self.slot, self.half(k)], ee.at[self.k, self.dx, self.half(k)],
                e_send.at[self.n, k], e_recv.at[self.k, self.dx, k], (sp, self.to),
            )

        def compute(self, *others):
            mark("comp%d" % self.n)

            def part(j, carry):
                i, first, slot = j, self.first, self.slot
                if others:
                    i = self.kept
                    first = first + j * (others[0].first - first)
                    slot = slot + j * (others[0].slot - slot)
                elif self.single:
                    i = self.kept
                first = (first + 2 * (other + i * (core - other))) * SHARD
                rows = wd[pl.ds(pl.multiple_of(first, SHARD), SHARD), :]
                pp[i, slot] = dot(hid[...], rows, LAST).astype(BF16)
                if others:
                    for g, step in enumerate((self, *others)):
                        pl.when(jnp.logical_and(i == 0, j == g))(lambda step=step: step.chip().start())
                else:
                    pl.when(i == 0)(lambda: self.chip().start())
                return carry

            if self.single and not others:
                part(0, 0)
            else:
                lax.fori_loop(0, 2, part, 0)

        def when_kept(self, body):
            if self.single:
                pl.when(self.keep)(body)
            else:
                body()

        def chip_sum(self):
            mark("cs%d" % self.n)
            self.when_kept(self.chip_sum_kept)

        def chip_sum_kept(self):
            self.chip().wait_recv()

            def add(i, carry):
                rows = pl.ds(pl.multiple_of(i * TILE, TILE), TILE)
                total = pp[1, self.slot, rows, :].astype(F32) + d2r[self.slot, rows, :].astype(F32)
                pp[1, self.slot, rows, :] = total.astype(BF16)
                return carry

            lax.fori_loop(0, TOK // TILE, add, 0)

            @pl.when(self.far)
            def _():
                self.out_far(0).start()
                self.out_far(1).start()

            @pl.when(self.odd)
            def _():
                self.out_near(1 - self.k).start()

        def join(self):
            mark("jn%d" % self.n)
            self.when_kept(self.join_kept)

        def join_kept(self):
            @pl.when(self.odd)
            def _():
                remote(
                    ra.at[self.slot], ra.at[self.slot], r_send.at[self.n, 0], r_recv.at[self.n],
                    (sp, self.to),
                ).wait_recv()

                def add(i, carry):
                    rows = pl.ds(pl.multiple_of(self.k * HALF + i * TILE, TILE), TILE)
                    got = ra[self.slot, pl.ds(pl.multiple_of(i * TILE, TILE), TILE), :]
                    total = pp[1, self.slot, rows, :].astype(F32) + got.astype(F32)
                    pp[1, self.slot, rows, :] = total.astype(BF16)
                    return carry

                lax.fori_loop(0, HALF // TILE, add, 0)
                self.out_near(self.k).start()

        def drain(self):
            if self.single:
                pl.when(jnp.logical_not(self.keep))(lambda: self.chip().wait_send())
            else:
                self.chip().wait_send()
            self.when_kept(self.drain_kept)

        def drain_kept(self):
            @pl.when(self.far)
            def _():
                self.out_far(0).wait_send()
                self.out_far(1).wait_send()

            @pl.when(self.odd)
            def _():
                self.out_near(1 - self.k).wait_send()
                self.out_near(self.k).wait_send()

    steps = [Step(n) for n in range(11)]
    steps[0].compute()
    steps[5].compute(steps[6])
    steps[0].chip_sum()
    steps[5].chip_sum()
    mark("lev2_1")
    level2b(1, 0)
    level2a(1, 0)
    level2b(1, 1)
    steps[2].compute()
    steps[6].chip_sum()
    steps[3].compute()
    steps[2].chip_sum()
    mark("w7")
    level4(1, 0, (0,))
    level4(1, 1, (0,))
    steps[7].compute()
    steps[3].chip_sum()
    steps[1].compute()
    steps[7].chip_sum()
    steps[1].chip_sum()
    mark("w4")
    level4(1, 0, (1, 2))
    level3(1, 1)
    steps[4].compute()
    steps[0].join()
    steps[4].chip_sum()
    mark("w30")
    level3(1, 0)
    steps[2].join()
    steps[5].join()
    steps[6].join()
    steps[3].join()
    mark("w5")
    level4(1, 1, (1, 2))
    steps[9].compute(steps[10])
    steps[7].join()
    steps[9].chip_sum()
    steps[10].chip_sum()
    steps[4].join()
    mark("w8")
    level4(1, 0, (3,))
    level4(1, 1, (3,))
    steps[8].compute()
    steps[8].chip_sum()
    steps[1].join()
    for n in (9, 10, 8):
        steps[n].join()
    mark("ewait")

    for dx in range(2):
        slot = dx * 4 + y
        for k in range(2):
            for half in range(2):
                rows = pl.ds(half * HALF, HALF)
                remote(
                    ee.at[k, dx, rows], ee.at[k, dx, rows], e_send.at[0, 0], e_recv.at[k, dx, half],
                    (sp, partner),
                ).wait_recv()
        cols = pl.ds(pl.multiple_of(lax.rem(x + dx, 2) * SHARD, SHARD), SHARD)

        def finish(i, carry):
            rows = pl.ds(pl.multiple_of(i * TILE, TILE), TILE)
            total = pp[1, slot, rows, :].astype(F32)
            total = total + (ee[0, dx, rows, :].astype(F32) + ee[1, dx, rows, :].astype(F32))
            out[rows, cols] = (xa[tp, rows, cols].astype(F32) + total).astype(BF16)
            return carry

        lax.fori_loop(0, TOK // TILE, finish, 0)
    mark("final")
    for copy in started:
        copy.wait_send()
    for step in steps:
        step.drain()
    mark(None)


def per_device(
    residual, values, forget_onward, forget_reverse, surge_log_decay, gate_limit_complement,
    readout_query, output_gate, head_norm_gain, output_weight, mixer_norm_gain, up_weight,
    down_weight,
):
    any_spec = pl.BlockSpec(memory_space=pl.ANY)
    vmem, dma = pltpu.VMEM, pltpu.SemaphoreType.DMA
    scratch = [
        vmem((TOK, OC), BF16), vmem((TOK, CH), BF16), vmem((TOK, CH), BF16), vmem((TOK, CH), BF16),
        vmem((8, TOK), F32), vmem((TOK, 8), F32), vmem((2, CH), F32), vmem((TOK, CH), BF16), vmem((TOK, CH), BF16),
        vmem((1, HD), F32), vmem((1, D), F32),
        vmem((D, FFL), BF16), vmem((D, FFL), BF16), vmem((2048, OC), BF16),
        vmem((8, TOK, CH), BF16), vmem((8, TOK, OC), BF16),
        vmem((2, TOK, CH), BF16), vmem((2, TOK, CH), BF16), vmem((2, NB, CH, HD), BF16),
        vmem((2, NB, 8, CH), F32), vmem((2, NB, 8, CH), F32),
        vmem((2, CH, HD), F32), vmem((2, 8, CH), F32),
        vmem((4, 2, ST_ROWS, HD), BF16), vmem((4, 2, ST_ROWS, HD), BF16), vmem((2, CH, HD), F32),
        vmem((TOK, CH), F32), vmem((TOK, OC), F32),
        vmem((TOK, 2 * OC), BF16), vmem((TOK, HD), F32), vmem((TOK, FFL), F32), vmem((TOK, FFL), BF16),
        vmem((2, 8, TOK, SHARD), BF16), vmem((8, TOK, SHARD), BF16),
        vmem((8, TOK // 2, SHARD), BF16), vmem((2, 2, TOK, SHARD), BF16),
        vmem((2, 2, 128, OC), BF16), vmem((2, TOK, CH), F32),
        dma((13,)), dma((2, 2, 20)), dma((2, 2, 20)), dma((13,)), dma((13,)), dma((6,)), dma((6,)),
        dma((13,)), dma((13,)), dma((13,)), dma((13,)), dma((11,)), dma((11,)), dma((11, 2)), dma((11,)),
        dma((11, 2)), dma((2, 2, 2)),
    ]
    return pl.pallas_call(
        kernel,
        out_shape=pltpu.VMEM((TOK, OC), BF16),
        in_specs=[any_spec] * 13,
        out_specs=pl.BlockSpec(memory_space=pltpu.VMEM),
        scratch_shapes=scratch,
        compiler_params=pltpu.CompilerParams(
            collective_id=0, has_side_effects=True, vmem_limit_bytes=66_000_000
        ),
        name="layer",
    )(
        residual, values, forget_onward, forget_reverse, surge_log_decay.T, gate_limit_complement,
        readout_query, output_gate, head_norm_gain.reshape(1, HD), output_weight,
        mixer_norm_gain.reshape(1, D), up_weight, down_weight,
    )


def solution(mesh):
    both = P("sp", "tp")
    placed = (
        both, both, both, both, both, P(None, "tp"), both, both, P(), P("tp", None), P(), both, both,
    )
    return jax.shard_map(
        per_device, mesh=mesh, in_specs=placed, out_specs=both, check_vma=False
    )
```

```python
import functools

import jax
import jax.numpy as jnp
from jax import lax
from jax.experimental import pallas as pl
from jax.experimental.pallas import tpu as pltpu
from jax.sharding import PartitionSpec as P

D = 4096
HD = 128
HEADS = 2
CH = HEADS * HD
TOK = 768
BLK = 64
UNROLL = 3
NB = TOK // BLK
OC = 512
FFL = 1024
SHARD = 256
QUARTER = 64
EPS = 1e-06
MESH = pl.DeviceIdType.MESH
F32 = jnp.float32
BF16 = jnp.bfloat16
ST_ROWS = 272


def dot(a, b, dims=(((1,), (0,)), ((), ()))):
    return lax.dot_general(a, b, dims, preferred_element_type=F32)


LAST = (((1,), (1,)), ((), ()))
FIRST = (((0,), (0,)), ((), ()))


def sigmoid(x):
    return 1.0 / (1.0 + jnp.exp(-x))


def kernel(
    residual, values, f_on, f_rev, surge, glc, query, gate, head_gain, out_w,
    norm_gain, up_w, down_w,
    out,
    res_v, val_v, fon_v, frev_v, sur_t, sur_v, glc_v, que_v, gat_v, hg_v, ng_v,
    wu, wd, owc, ga, xa,
    qd, kr, sx, em, elx, run_state, run_log, row_in, col_in, sin, o_v, att,
    xg, ss, acc, hid,
    pp, d2r, ra, ee, relay, rel,
    in_sem, w_send, w_recv, ow_send, ow_recv, st_send, st_recv,
    g_send, g_recv, x_send, x_recv, c_send, c_recv, r_send, r_recv, e_send, e_recv,
):
    sp, tp = lax.axis_index("sp"), lax.axis_index("tp")
    x, z = lax.rem(sp, 4), lax.div(sp, 4)
    core, y = lax.rem(tp, 2), lax.div(tp, 2)
    other = 1 - core

    cur = [None]

    def mark(name):
        if cur[0] is not None:
            cur[0].__exit__(None, None, None)
        cur[0] = jax.named_scope(name) if name else None
        if name:
            cur[0].__enter__()

    mark("start")

    def ring(v, k):
        return lax.rem(v + (k % 4), 4)

    yp, ym, y2 = ring(y, 1), ring(y, 3), ring(y, 2)
    partner = 2 * y + other

    barrier = pltpu.get_barrier_semaphore()
    peers = [(z * 4 + ring(x, o), tp) for o in (1, 3, 2)]
    peers += [(ring(z, o) * 4 + x, tp) for o in (1, 3, 2)]
    peers += [(sp, 2 * near + c) for near in (yp, ym) for c in range(2)] + [(sp, partner)]
    for peer in peers:
        pl.semaphore_signal(barrier, inc=1, device_id=peer, device_id_type=MESH)

    own_rows = pl.ds(pl.multiple_of(sp * SHARD, SHARD), SHARD)
    ow_rows = pl.ds(pl.multiple_of(tp * 256, 256), 256)
    own_cols = pl.ds(pl.multiple_of(tp * OC, OC), OC)
    loads = [
        (f_on, fon_v), (f_rev, frev_v), (surge, sur_t.at[pl.ds(0, HEADS)]), (glc, glc_v), (query, que_v),
        (values, val_v), (gate, gat_v), (head_gain, hg_v), (residual, res_v), (norm_gain, ng_v),
        (up_w, wu.at[own_rows]), (down_w, wd.at[own_rows]),
        (out_w.at[:, own_cols], owc.at[ow_rows]),
    ]
    loads = [pltpu.make_async_copy(a, b, in_sem.at[i]) for i, (a, b) in enumerate(loads)]
    for copy in loads:
        copy.start()

    pl.semaphore_wait(barrier, len(peers))

    def remote(src, dst, ss_, rs_, dev):
        return pltpu.make_async_remote_copy(
            src_ref=src, dst_ref=dst, send_sem=ss_, recv_sem=rs_, device_id=dev, device_id_type=MESH
        )

    started = []

    def go(copy):
        copy.start()
        started.append(copy)

    weights = ((up_w, wu), (down_w, wd))

    def sp_at(half, i, j):
        return ring(z, j) * 4 + ring(x, i) if half == 0 else ring(z, i) * 4 + ring(x, j)

    def piece(t, half, i, j, part):
        start, size = (0, 2 * QUARTER) if part is None else (part * QUARTER, QUARTER)
        first = sp_at(half, i, j) * SHARD + half * 2 * QUARTER + start
        return weights[t][1].at[pl.ds(pl.multiple_of(first, QUARTER), size)]

    FWD = (0, -1, 1, 2)

    def w_copy(t, half, slot, i, j, part, to, src=None):
        ref = piece(t, half, i, j, part)
        return remote(
            ref if src is None else src, ref, w_send.at[t, half, slot], w_recv.at[t, half, slot],
            (sp_at(half, *to), tp),
        )

    def w_go(*args, **kw):
        copy = w_copy(*args, **kw)
        copy.start()
        started.append(copy)

    def w_got(t, half, slot, i, j, part):
        w_copy(t, half, slot, i, j, part, (1, 0)).wait_recv()

    def w_second(t, half, n, src=None):
        i = FWD[n]
        w_go(t, half, 4 + 4 * n, i, 0, None, (0, 1), src=src)
        w_go(t, half, 5 + 4 * n, i, 0, None, (0, -1), src=src)

    def w_second_forward(t, half, n):
        i = FWD[n]
        w_got(t, half, 4 + 4 * n, i, -1, None)
        w_go(t, half, 6 + 4 * n, i, -1, 0, (0, 1))
        w_got(t, half, 5 + 4 * n, i, 1, None)
        w_go(t, half, 7 + 4 * n, i, 1, 1, (0, -1))

    def level0a(t):
        for half in range(2):
            src = weights[t][0].at[pl.ds(half * 2 * QUARTER, 2 * QUARTER)]
            w_go(t, half, 0, 0, 0, None, (1, 0), src=src)
            w_go(t, half, 1, 0, 0, None, (-1, 0), src=src)

    def level0b(t, half):
        src = weights[t][0].at[pl.ds(half * 2 * QUARTER, 2 * QUARTER)]
        w_second(t, half, 0, src=src)

    def level1p(t):
        for half in range(2):
            w_got(t, half, 0, -1, 0, None)
            w_go(t, half, 2, -1, 0, 0, (1, 0))
            w_got(t, half, 1, 1, 0, None)
            w_go(t, half, 3, 1, 0, 1, (-1, 0))

    def level1s(t):
        for half in range(2):
            w_second(t, half, 1)
            w_second(t, half, 2)

    def level1b(t):
        for half in range(2):
            w_second_forward(t, half, 0)

    def level2a(t, half):
        w_got(t, half, 2, 2, 0, 0)
        w_got(t, half, 3, 2, 0, 1)
        w_second(t, half, 3)

    def level2b(t, half):
        w_second_forward(t, half, 1)
        w_second_forward(t, half, 2)

    def level3(t, half):
        w_second_forward(t, half, 3)

    def level4(t, half, blocks):
        for n in blocks:
            w_got(t, half, 6 + 4 * n, FWD[n], 2, 0)
            w_got(t, half, 7 + 4 * n, FWD[n], 2, 1)

    mark("w0")
    level0a(0)

    def ow_cols(to):
        return pl.ds(pl.multiple_of(to * OC, OC), OC)

    def ow_rows_of(source, k=None):
        first, size = (0, 256) if k is None else (k * 128, 128)
        return pl.ds(pl.multiple_of(source * 256 + first, 128), size)

    near = (yp, ym)

    def ow_leg1(k, c):
        return remote(
            out_w.at[pl.ds(k * 128, 128), ow_cols(2 * y2 + c)], relay.at[k, c],
            ow_send.at[2 * k + c], ow_recv.at[2 * k + c], (sp, 2 * near[k] + core),
        )

    def ow_direct(k, c):
        return remote(
            out_w.at[:, ow_cols(2 * near[k] + c)], owc.at[ow_rows],
            ow_send.at[4 + 2 * k + c], ow_recv.at[4 + 2 * k + core], (sp, 2 * near[k] + c),
        )

    def ow_partner():
        return remote(
            out_w.at[:, ow_cols(partner)], owc.at[ow_rows], ow_send.at[8], ow_recv.at[8], (sp, partner)
        )

    def ow_leg2(k, c):
        return remote(
            relay.at[k, c], owc.at[ow_rows_of(2 * near[1 - k] + core, k)],
            ow_send.at[9 + 2 * k + c], ow_recv.at[9 + 2 * k + core], (sp, 2 * near[k] + c),
        )

    def ow_forward():
        for k in range(2):
            for c in range(2):
                ow_leg1(k, c).wait_recv()
                go(ow_leg2(k, c))

    def ow_wait():
        def landed(rows, sem):
            ref = owc.at[rows]
            remote(ref, ref, ow_send.at[8], ow_recv.at[sem], (sp, partner)).wait_recv()

        landed(ow_rows_of(partner), 8)
        for k in range(2):
            for c in range(2):
                landed(ow_rows_of(2 * near[1 - k] + c), 4 + 2 * k + c)
        for k in range(2):
            for c in range(2):
                landed(ow_rows_of(2 * y2 + c, k), 9 + 2 * k + c)

    for k in range(2):
        for c in range(2):
            go(ow_leg1(k, c))
    for k in range(2):
        for c in range(2):
            go(ow_direct(k, c))
    go(ow_partner())

    mark("loadwait")
    for copy in loads[:7]:
        copy.wait()

    mark("pass1")
    row_id = lax.broadcasted_iota(jnp.int32, (BLK, BLK), 0)
    col_id = lax.broadcasted_iota(jnp.int32, (BLK, BLK), 1)
    lower, upper = row_id >= col_id, row_id <= col_id
    run_state[...] = jnp.zeros_like(run_state)
    run_log[...] = jnp.zeros_like(run_log)
    sur_v[...] = jnp.concatenate([sur_t[0:HEADS, :], jnp.zeros((8 - HEADS, TOK), F32)], axis=0).T
    sums = tuple(
        jnp.concatenate([jnp.where(tri, 1.0, 0.0)] * 3, axis=1).astype(BF16) for tri in (lower, upper)
    )

    def split3(v):
        a = v.astype(BF16)
        rest = v - a.astype(F32)
        b = rest.astype(BF16)
        return jnp.concatenate([a, b, (rest - b.astype(F32)).astype(BF16)], axis=0)

    def pass1_block(d, blk):
        logits = (fon_v, frev_v)[d]
        mid_at, end_at = ((BLK // 2 - 1, BLK - 1), (BLK // 2, 0))[d]
        rows = pl.ds(pl.multiple_of(blk * BLK, BLK), BLK)
        key = glc_v[d : d + 1, :] / (1.0 + jnp.exp(logits[rows, :].astype(F32)))
        sg = sur_v[rows, :]
        sg = jnp.concatenate(
            [jnp.broadcast_to(sg[:, h : h + 1], (BLK, HD)) for h in range(HEADS)], axis=1
        )
        run = dot(sums[d], split3(jnp.log1p(-key) + sg))
        mid, end = run[mid_at : mid_at + 1, :], run[end_at : end_at + 1, :]
        away = mid - run
        rel[d, rows, :] = away
        k = key * jnp.exp(away)
        kr[d, rows, :] = k.astype(BF16)
        tail = (k * jnp.exp(end - mid)).astype(BF16)
        v = val_v[rows, :]
        new = [
            dot(v[:, h * HD : (h + 1) * HD], tail[:, h * HD : (h + 1) * HD], FIRST)
            for h in range(HEADS)
        ]
        em[d, blk] = jnp.broadcast_to(jnp.exp(mid), (8, CH))
        return end, new

    def pass1(step, carry):
        blocks = [
            (d, step * UNROLL + u if d == 0 else NB - 1 - (step * UNROLL + u))
            for u in range(UNROLL)
            for d in range(2)
        ]
        parts = [pass1_block(d, blk) for d, blk in blocks]
        for (d, blk), (end, new) in zip(blocks, parts):
            gone = run_log[d, 0:1, :]
            elx[d, blk] = jnp.broadcast_to(jnp.exp(gone), (8, CH))
            run_log[d] = jnp.broadcast_to(gone + end, (8, CH))
            decay = jnp.exp(end)
            for h in range(HEADS):
                hs = slice(h * HD, (h + 1) * HD)
                state = run_state[d, hs, :]
                sx[d, blk, hs, :] = state.astype(BF16)
                run_state[d, hs, :] = state * decay[:, hs] + new[h]
        return carry

    lax.fori_loop(0, NB // UNROLL, pass1, 0)

    mark("stsend")
    def store_state(ref, at, d, state, log):
        ref[at, d, 0:CH, :] = state.astype(BF16)
        high = log.astype(BF16).astype(F32)
        rest = log - high
        ref[at, d, CH:ST_ROWS, :] = jnp.concatenate(
            [high[:, :HD], high[:, HD:], rest[:, :HD], rest[:, HD:], jnp.zeros((12, HD), F32)], axis=0
        ).astype(BF16)

    def load_log(ref, at, d):
        tail = ref[at, d, CH:ST_ROWS, :].astype(F32)
        return [tail[h : h + 1, :] + tail[2 + h : 3 + h, :] for h in range(HEADS)]

    for d in range(2):
        store_state(row_in, x, d, run_state[d], run_log[d, 0:1, :])

    def row_copy(o):
        return remote(
            row_in.at[x], row_in.at[x], st_send.at[o - 1], st_recv.at[o - 1],
            (z * 4 + ring(x, o), tp),
        )

    def row_got(o):
        ref = row_in.at[ring(x, -o)]
        remote(ref, ref, st_send.at[o - 1], st_recv.at[o - 1], (z * 4 + ring(x, o), tp)).wait_recv()

    def col_copy(o):
        ref = col_in.at[z, lax.div(z + o, 4)]
        return remote(
            ref, ref, st_send.at[o + 2], st_recv.at[o + 2], (ring(z, o) * 4 + x, tp)
        )

    def col_got(o):
        ref = col_in.at[ring(z, -o), lax.div(z + 4 - o, 4) * -1 + 1]
        remote(ref, ref, st_send.at[o + 2], st_recv.at[o + 2], (ring(z, o) * 4 + x, tp)).wait_recv()

    for o in (1, 3, 2):
        copy = row_copy(o)
        copy.start()
        started.append(copy)
    mark("l0b")
    level0b(0, 0)
    level0b(0, 1)

    def pass2_block(blk):
        rows = pl.ds(pl.multiple_of(blk * BLK, BLK), BLK)
        v = val_v[rows, :]
        q = que_v[rows, :].astype(F32)
        q = q * sigmoid(q) * (HD ** -0.5)
        for d in range(2):
            qd[d, rows, :] = (q * jnp.exp(-rel[d, rows, :])).astype(BF16)
        for h in range(HEADS):
            hs = slice(h * HD, (h + 1) * HD)
            fwd = dot(qd[0, rows, hs], kr[0, rows, hs], LAST)
            bwd = dot(qd[1, rows, hs], kr[1, rows, hs], LAST)
            score = jnp.where(lower, fwd, 0.0) + jnp.where(upper, bwd, 0.0)
            o_v[rows, hs] = dot(score.astype(BF16), v[:, hs])

    def by_blocks(body):
        def step(i, carry):
            for u in range(UNROLL):
                body(i * UNROLL + u)
            return carry

        lax.fori_loop(0, NB // UNROLL, step, 0)

    mark("pass2")
    by_blocks(pass2_block)


    mark("owfwd")
    ow_forward()
    level1p(0)
    mark("roww")
    for o in (1, 3, 2):
        row_got(o)
    mark("rowc")
    for d in range(2):
        state = jnp.zeros((CH, HD), F32)
        log = [jnp.zeros((1, HD), F32)] * HEADS
        for j in range(4) if d == 0 else range(3, -1, -1):
            own = load_log(row_in, j, d)
            state = jnp.concatenate(
                [
                    state[h * HD : (h + 1) * HD] * jnp.exp(own[h])
                    + row_in[j, d, h * HD : (h + 1) * HD, :].astype(F32)
                    for h in range(HEADS)
                ],
                axis=0,
            )
            log = [log[h] + own[h] for h in range(HEADS)]
        store_state(col_in, z, d, state, jnp.concatenate(log, axis=1))
    for o in (1, 3, 2):
        copy = col_copy(o)
        copy.start()
        started.append(copy)
    sin[...] = jnp.zeros_like(sin)
    mark("colw")
    for o in (1, 3, 2):
        col_got(o)
    level1s(0)
    mark("combine")

    def chain(ref, at):
        def body(i, carry):
            d = lax.div(i + 4 - at, 4)
            j = (1 - d) * i + d * (3 + at - i)
            own = load_log(ref, j, d)
            for h in range(HEADS):
                hs = slice(h * HD, (h + 1) * HD)
                sin[d, hs, :] = sin[d, hs, :] * jnp.exp(own[h]) + ref[j, d, hs, :].astype(F32)
            return carry

        lax.fori_loop(0, 3, body, 0)

    chain(col_in, z)
    chain(row_in, x)

    for copy in loads[6:10]:
        if copy is not loads[6]:
            copy.wait()

    def pass3_block(blk):
        rows = pl.ds(pl.multiple_of(blk * BLK, BLK), BLK)
        for h in range(HEADS):
            hs = slice(h * HD, (h + 1) * HD)
            mixed = o_v[rows, hs]
            for d in range(2):
                qs = (qd[d, rows, hs].astype(F32) * em[d, blk, 0:1, hs]).astype(BF16)
                state = sx[d, blk, hs, :].astype(F32) + elx[d, blk, 0:1, hs] * sin[d, hs, :]
                mixed = mixed + dot(qs, state.astype(BF16), LAST)
            norm = mixed * lax.rsqrt(jnp.mean(mixed * mixed, axis=-1, keepdims=True) + EPS)
            g = gat_v[rows, hs].astype(F32)
            ga[tp, rows, hs] = (norm * hg_v[0:1, :] * (g * sigmoid(g))).astype(BF16)

    mark("pass3")
    by_blocks(pass3_block)

    HALF = TOK // 2

    class Gather:
        def __init__(self, buf, send_sem, recv_sem):
            self.buf, self.ss, self.rs = buf, send_sem, recv_sem

        def copy(self, k, slot, part, to):
            ref = self.buf.at[slot]
            if part is not None:
                ref = self.buf.at[slot, pl.ds(part * HALF, HALF)]
            return remote(ref, ref, self.ss.at[k], self.rs.at[k], (sp, to))

        def go(self, *args):
            copy = self.copy(*args)
            copy.start()
            started.append(copy)

        def got(self, k, slot, part):
            self.copy(k, slot, part, partner).wait_recv()

        def own(self):
            right, left = 2 * yp + core, 2 * ym + core
            self.go(0, tp, 0, right)
            self.go(3, tp, 1, left)
            self.go(6, tp, None, partner)
            self.go(1, tp, 1, right)
            self.go(2, tp, 0, left)

        def forward(self):
            left, right = 2 * ym + core, 2 * yp + core
            self.got(0, left, 0)
            self.go(4, left, 0, right)
            self.go(7, left, 0, partner)
            self.got(3, right, 1)
            self.go(5, right, 1, left)
            self.go(8, right, 1, partner)

        def from_side(self):
            left, right = 2 * ym + core, 2 * yp + core
            self.got(1, left, 1)
            self.go(9, left, 1, partner)
            self.got(2, right, 0)
            self.go(10, right, 0, partner)

        def from_far(self):
            far = 2 * y2 + core
            self.got(4, far, 0)
            self.go(11, far, 0, partner)
            self.got(5, far, 1)
            self.go(12, far, 1, partner)

        def other_core(self, chip):
            block = 2 * chip + other
            for k, part in {id(ym): ((7, 0), (9, 1)), id(yp): ((8, 1), (10, 0)), id(y2): ((11, 0), (12, 1))}[
                id(chip)
            ]:
                self.got(k, block, part)

    gathered = Gather(ga, g_send, g_recv)
    mark("gown")
    gathered.own()

    mark("owwait")
    for copy in loads[10:13]:
        copy.wait()
    ow_wait()

    def project(block, first=False):
        def tile(n, carry):
            cols = pl.ds(pl.multiple_of(n * 256, 256), 256)
            part = dot(ga[block], owc[pl.ds(pl.multiple_of(block * 256, 256), 256), cols])
            att[:, cols] = part if first else att[:, cols] + part
            return carry

        lax.fori_loop(0, OC // 256, tile, 0)

    mark("proj0")
    project(tp, True)
    mark("gpart")
    gathered.got(6, partner, None)
    project(partner)
    mark("lev2a_0")
    level1b(0)
    level2a(0, 0)
    level2a(0, 1)
    mark("gfwd")
    gathered.forward()
    mark("gside")
    gathered.from_side()
    mark("proj2")
    project(2 * ym + core)
    project(2 * yp + core)
    mark("lev2b_0")
    level2b(0, 0)
    level2b(0, 1)
    level0a(1)
    mark("gpart2")
    gathered.other_core(ym)
    project(2 * ym + other)
    gathered.other_core(yp)
    project(2 * yp + other)
    mark("gfar")
    gathered.from_far()
    project(2 * y2 + core)
    gathered.other_core(y2)
    project(2 * y2 + other)

    TILE = 128

    def middle(i, carry):
        rows = pl.ds(pl.multiple_of(i * TILE, TILE), TILE)
        xa[tp, rows, :] = (res_v[rows, :].astype(F32) + att[rows, :]).astype(BF16)
        return carry

    mark("middle")
    lax.fori_loop(0, TOK // TILE, middle, 0)

    spread = Gather(xa, x_send, x_recv)
    spread.own()
    def scale(chip, c, first=False):
        block = 2 * chip + c
        gain = ng_v[:, pl.ds(pl.multiple_of(block * OC, OC), OC)]
        cols = pl.ds(pl.multiple_of(c * OC, OC), OC)

        def body(i, carry):
            rows = pl.ds(pl.multiple_of(i * TILE, TILE), TILE)
            v = xa[block, rows, :].astype(F32)
            sq = v * v
            sq = (sq[:, 0:128] + sq[:, 128:256]) + (sq[:, 256:384] + sq[:, 384:512])
            ss[rows, :] = sq if first else ss[rows, :] + sq
            xg[rows, cols] = (v * gain).astype(BF16)
            return carry

        lax.fori_loop(0, TOK // TILE, body, 0)

    def lift(chip, first=False):
        def tile(n, carry):
            cols = pl.ds(pl.multiple_of(n * 256, 256), 256)
            part = dot(xg[...], wu[pl.ds(pl.multiple_of(chip * 2 * OC, 2 * OC), 2 * OC), cols])
            acc[:, cols] = part if first else acc[:, cols] + part
            return carry

        lax.fori_loop(0, FFL // 256, tile, 0)

    def lift_one(chip, c):
        def tile(n, carry):
            cols = pl.ds(pl.multiple_of(n * 256, 256), 256)
            rows = pl.ds(pl.multiple_of((chip * 2 + c) * OC, OC), OC)
            part = dot(xg[:, pl.ds(pl.multiple_of(c * OC, OC), OC)], wu[rows, cols])
            acc[:, cols] = acc[:, cols] + part
            return carry

        lax.fori_loop(0, FFL // 256, tile, 0)

    mark("scale0")
    scale(y, core, True)
    spread.got(6, partner, None)
    scale(y, other)
    mark("lev3_0")
    level3(0, 0)
    level3(0, 1)
    level0b(1, 0)
    level0b(1, 1)
    mark("xfwd")
    spread.forward()
    mark("lev1a_1")
    level1p(1)
    level1s(1)
    mark("lev4_0")
    level4(0, 0, range(4))
    level4(0, 1, range(4))
    mark("lift0")
    lift(y, True)
    mark("xside")
    spread.from_side()
    mark("lift1")
    scale(ym, core)
    lift_one(ym, core)
    spread.other_core(ym)
    scale(ym, other)
    lift_one(ym, other)
    mark("lev1_1")
    level1b(1)
    mark("lift2")
    scale(yp, core)
    spread.other_core(yp)
    scale(yp, other)
    lift(yp)
    mark("lev2a_1")
    level2a(1, 1)
    mark("xfar")
    spread.from_far()
    mark("lift3")
    scale(y2, core)
    lift_one(y2, core)
    spread.other_core(y2)
    scale(y2, other)
    lift_one(y2, other)

    def activate(i, carry):
        rows = pl.ds(pl.multiple_of(i * TILE, TILE), TILE)
        total = jnp.sum(ss[rows, :], axis=-1, keepdims=True)
        v = jnp.maximum(acc[rows, :] * lax.rsqrt(total / D + EPS), 0.0)
        hid[rows, :] = (v * v).astype(BF16)
        return carry

    mark("act")
    lax.fori_loop(0, TOK // TILE, activate, 0)


    SHARDS = (
        (1, 0), (0, 0), (1, 1), (1, -1), (1, 2),
        (0, 1), (0, -1), (0, 2), (2, 2), (2, 1), (2, -1),
    )

    class Step:
        def __init__(self, n):
            self.n = n
            dx, dz = SHARDS[n]
            self.single = n >= 5
            self.dx = dx % 2
            zs = ring(z, dz)
            column = lax.rem(x + dx, 2)
            self.keep = lax.div(ring(x, dx), 2) == core
            self.kept = jnp.where(self.keep, 1, 0)
            self.slot = self.dx * 4 + zs
            self.first = zs * 4 + column
            self.delta = lax.rem(zs + 4 - y, 4)
            self.odd = lax.rem(self.delta, 2) == 1
            self.far = self.delta == 2
            self.k = lax.div(self.delta, 2)
            self.to = 2 * lax.rem(y + self.delta, 4) + core

        def chip(self):
            return remote(
                pp.at[0, self.slot], d2r.at[self.slot], c_send.at[self.n], c_recv.at[self.n], (sp, partner)
            )

        def half(self, k):
            return pl.ds(pl.multiple_of(k * HALF, HALF), HALF)

        def out_far(self, k):
            return remote(
                pp.at[1, self.slot, self.half(k)], ra.at[self.slot], r_send.at[self.n, k],
                r_recv.at[self.n], (sp, 2 * (yp, ym)[k] + core),
            )

        def out_near(self, k):
            return remote(
                pp.at[1, self.slot, self.half(k)], ee.at[self.k, self.dx, self.half(k)],
                e_send.at[self.n, k], e_recv.at[self.k, self.dx, k], (sp, self.to),
            )

        def compute(self, *others):
            mark("comp%d" % self.n)

            def part(j, carry):
                i, first, slot = j, self.first, self.slot
                if others:
                    i = self.kept
                    first = first + j * (others[0].first - first)
                    slot = slot + j * (others[0].slot - slot)
                elif self.single:
                    i = self.kept
                first = (first + 2 * (other + i * (core - other))) * SHARD
                rows = wd[pl.ds(pl.multiple_of(first, SHARD), SHARD), :]
                pp[i, slot] = dot(hid[...], rows, LAST).astype(BF16)
                if others:
                    for g, step in enumerate((self, *others)):
                        pl.when(jnp.logical_and(i == 0, j == g))(lambda step=step: step.chip().start())
                else:
                    pl.when(i == 0)(lambda: self.chip().start())
                return carry

            if self.single and not others:
                part(0, 0)
            else:
                lax.fori_loop(0, 2, part, 0)

        def when_kept(self, body):
            if self.single:
                pl.when(self.keep)(body)
            else:
                body()

        def chip_sum(self):
            mark("cs%d" % self.n)
            self.when_kept(self.chip_sum_kept)

        def chip_sum_kept(self):
            self.chip().wait_recv()

            def add(i, carry):
                rows = pl.ds(pl.multiple_of(i * TILE, TILE), TILE)
                total = pp[1, self.slot, rows, :].astype(F32) + d2r[self.slot, rows, :].astype(F32)
                pp[1, self.slot, rows, :] = total.astype(BF16)
                return carry

            lax.fori_loop(0, TOK // TILE, add, 0)

            @pl.when(self.far)
            def _():
                self.out_far(0).start()
                self.out_far(1).start()

            @pl.when(self.odd)
            def _():
                self.out_near(1 - self.k).start()

        def join(self):
            mark("jn%d" % self.n)
            self.when_kept(self.join_kept)

        def join_kept(self):
            @pl.when(self.odd)
            def _():
                remote(
                    ra.at[self.slot], ra.at[self.slot], r_send.at[self.n, 0], r_recv.at[self.n],
                    (sp, self.to),
                ).wait_recv()

                def add(i, carry):
                    rows = pl.ds(pl.multiple_of(self.k * HALF + i * TILE, TILE), TILE)
                    got = ra[self.slot, pl.ds(pl.multiple_of(i * TILE, TILE), TILE), :]
                    total = pp[1, self.slot, rows, :].astype(F32) + got.astype(F32)
                    pp[1, self.slot, rows, :] = total.astype(BF16)
                    return carry

                lax.fori_loop(0, HALF // TILE, add, 0)
                self.out_near(self.k).start()

        def drain(self):
            if self.single:
                pl.when(jnp.logical_not(self.keep))(lambda: self.chip().wait_send())
            else:
                self.chip().wait_send()
            self.when_kept(self.drain_kept)

        def drain_kept(self):
            @pl.when(self.far)
            def _():
                self.out_far(0).wait_send()
                self.out_far(1).wait_send()

            @pl.when(self.odd)
            def _():
                self.out_near(1 - self.k).wait_send()
                self.out_near(self.k).wait_send()

    steps = [Step(n) for n in range(11)]
    steps[0].compute()
    steps[5].compute(steps[6])
    steps[0].chip_sum()
    steps[5].chip_sum()
    mark("lev2_1")
    level2b(1, 0)
    level2a(1, 0)
    level2b(1, 1)
    steps[2].compute()
    steps[6].chip_sum()
    steps[3].compute()
    mark("w7")
    level4(1, 0, (0,))
    level4(1, 1, (0,))
    steps[7].compute()
    steps[2].chip_sum()
    steps[3].chip_sum()
    steps[7].chip_sum()
    steps[1].compute()
    steps[1].chip_sum()
    mark("w4")
    level4(1, 0, (1, 2))
    level3(1, 1)
    steps[4].compute()
    steps[0].join()
    steps[7].join()
    steps[4].chip_sum()
    mark("w30")
    level3(1, 0)
    steps[2].join()
    steps[5].join()
    steps[6].join()
    steps[3].join()
    mark("w5")
    level4(1, 1, (1, 2))
    steps[9].compute(steps[10])
    steps[9].chip_sum()
    steps[10].chip_sum()
    steps[4].join()
    mark("w8")
    level4(1, 0, (3,))
    level4(1, 1, (3,))
    steps[8].compute()
    steps[8].chip_sum()
    steps[1].join()
    for n in (9, 10, 8):
        steps[n].join()
    mark("ewait")

    for dx in range(2):
        slot = dx * 4 + y
        for k in range(2):
            for half in range(2):
                rows = pl.ds(half * HALF, HALF)
                remote(
                    ee.at[k, dx, rows], ee.at[k, dx, rows], e_send.at[0, 0], e_recv.at[k, dx, half],
                    (sp, partner),
                ).wait_recv()
        cols = pl.ds(pl.multiple_of(lax.rem(x + dx, 2) * SHARD, SHARD), SHARD)

        def finish(i, carry):
            rows = pl.ds(pl.multiple_of(i * TILE, TILE), TILE)
            total = pp[1, slot, rows, :].astype(F32)
            total = total + (ee[0, dx, rows, :].astype(F32) + ee[1, dx, rows, :].astype(F32))
            out[rows, cols] = (xa[tp, rows, cols].astype(F32) + total).astype(BF16)
            return carry

        lax.fori_loop(0, TOK // TILE, finish, 0)
    mark("final")
    for copy in started:
        copy.wait_send()
    for step in steps:
        step.drain()
    mark(None)


def per_device(
    residual, values, forget_onward, forget_reverse, surge_log_decay, gate_limit_complement,
    readout_query, output_gate, head_norm_gain, output_weight, mixer_norm_gain, up_weight,
    down_weight,
):
    any_spec = pl.BlockSpec(memory_space=pl.ANY)
    vmem, dma = pltpu.VMEM, pltpu.SemaphoreType.DMA
    scratch = [
        vmem((TOK, OC), BF16), vmem((TOK, CH), BF16), vmem((TOK, CH), BF16), vmem((TOK, CH), BF16),
        vmem((8, TOK), F32), vmem((TOK, 8), F32), vmem((2, CH), F32), vmem((TOK, CH), BF16), vmem((TOK, CH), BF16),
        vmem((1, HD), F32), vmem((1, D), F32),
        vmem((D, FFL), BF16), vmem((D, FFL), BF16), vmem((2048, OC), BF16),
        vmem((8, TOK, CH), BF16), vmem((8, TOK, OC), BF16),
        vmem((2, TOK, CH), BF16), vmem((2, TOK, CH), BF16), vmem((2, NB, CH, HD), BF16),
        vmem((2, NB, 8, CH), F32), vmem((2, NB, 8, CH), F32),
        vmem((2, CH, HD), F32), vmem((2, 8, CH), F32),
        vmem((4, 2, ST_ROWS, HD), BF16), vmem((4, 2, ST_ROWS, HD), BF16), vmem((2, CH, HD), F32),
        vmem((TOK, CH), F32), vmem((TOK, OC), F32),
        vmem((TOK, 2 * OC), BF16), vmem((TOK, HD), F32), vmem((TOK, FFL), F32), vmem((TOK, FFL), BF16),
        vmem((2, 8, TOK, SHARD), BF16), vmem((8, TOK, SHARD), BF16),
        vmem((8, TOK // 2, SHARD), BF16), vmem((2, 2, TOK, SHARD), BF16),
        vmem((2, 2, 128, OC), BF16), vmem((2, TOK, CH), F32),
        dma((13,)), dma((2, 2, 20)), dma((2, 2, 20)), dma((13,)), dma((13,)), dma((6,)), dma((6,)),
        dma((13,)), dma((13,)), dma((13,)), dma((13,)), dma((11,)), dma((11,)), dma((11, 2)), dma((11,)),
        dma((11, 2)), dma((2, 2, 2)),
    ]
    return pl.pallas_call(
        kernel,
        out_shape=pltpu.VMEM((TOK, OC), BF16),
        in_specs=[any_spec] * 13,
        out_specs=pl.BlockSpec(memory_space=pltpu.VMEM),
        scratch_shapes=scratch,
        compiler_params=pltpu.CompilerParams(
            collective_id=0, has_side_effects=True, vmem_limit_bytes=66_000_000
        ),
        name="layer",
    )(
        residual, values, forget_onward, forget_reverse, surge_log_decay.T, gate_limit_complement,
        readout_query, output_gate, head_norm_gain.reshape(1, HD), output_weight,
        mixer_norm_gain.reshape(1, D), up_weight, down_weight,
    )


def solution(mesh):
    both = P("sp", "tp")
    placed = (
        both, both, both, both, both, P(None, "tp"), both, both, P(), P("tp", None), P(), both, both,
    )
    return jax.shard_map(
        per_device, mesh=mesh, in_specs=placed, out_specs=both, check_vma=False
    )
```

```python
import functools

import jax
import jax.numpy as jnp
from jax import lax
from jax.experimental import pallas as pl
from jax.experimental.pallas import tpu as pltpu
from jax.sharding import PartitionSpec as P

D = 4096
HD = 128
HEADS = 2
CH = HEADS * HD
TOK = 768
BLK = 64
UNROLL = 3
NB = TOK // BLK
OC = 512
FFL = 1024
SHARD = 256
QUARTER = 64
EPS = 1e-06
MESH = pl.DeviceIdType.MESH
F32 = jnp.float32
BF16 = jnp.bfloat16
ST_ROWS = 272


def dot(a, b, dims=(((1,), (0,)), ((), ()))):
    return lax.dot_general(a, b, dims, preferred_element_type=F32)


LAST = (((1,), (1,)), ((), ()))
FIRST = (((0,), (0,)), ((), ()))


def sigmoid(x):
    return 1.0 / (1.0 + jnp.exp(-x))


def kernel(
    residual, values, f_on, f_rev, surge, glc, query, gate, head_gain, out_w,
    norm_gain, up_w, down_w,
    out,
    res_v, val_v, fon_v, frev_v, sur_t, sur_v, glc_v, que_v, gat_v, hg_v, ng_v,
    wu, wd, owc, ga, xa,
    qd, kr, sx, em, elx, run_state, run_log, row_in, col_in, sin, o_v, att,
    xg, ss, acc, hid,
    pp, d2r, ra, ee, relay, rel,
    in_sem, w_send, w_recv, ow_send, ow_recv, st_send, st_recv,
    g_send, g_recv, x_send, x_recv, c_send, c_recv, r_send, r_recv, e_send, e_recv,
):
    sp, tp = lax.axis_index("sp"), lax.axis_index("tp")
    x, z = lax.rem(sp, 4), lax.div(sp, 4)
    core, y = lax.rem(tp, 2), lax.div(tp, 2)
    other = 1 - core

    cur = [None]

    def mark(name):
        if cur[0] is not None:
            cur[0].__exit__(None, None, None)
        cur[0] = jax.named_scope(name) if name else None
        if name:
            cur[0].__enter__()

    mark("start")

    def ring(v, k):
        return lax.rem(v + (k % 4), 4)

    yp, ym, y2 = ring(y, 1), ring(y, 3), ring(y, 2)
    partner = 2 * y + other

    barrier = pltpu.get_barrier_semaphore()
    peers = [(z * 4 + ring(x, o), tp) for o in (1, 3, 2)]
    peers += [(ring(z, o) * 4 + x, tp) for o in (1, 3, 2)]
    peers += [(sp, 2 * near + c) for near in (yp, ym) for c in range(2)] + [(sp, partner)]
    for peer in peers:
        pl.semaphore_signal(barrier, inc=1, device_id=peer, device_id_type=MESH)

    own_rows = pl.ds(pl.multiple_of(sp * SHARD, SHARD), SHARD)
    ow_rows = pl.ds(pl.multiple_of(tp * 256, 256), 256)
    own_cols = pl.ds(pl.multiple_of(tp * OC, OC), OC)
    loads = [
        (f_on, fon_v), (f_rev, frev_v), (surge, sur_t.at[pl.ds(0, HEADS)]), (glc, glc_v), (query, que_v),
        (values, val_v), (gate, gat_v), (head_gain, hg_v), (residual, res_v), (norm_gain, ng_v),
        (up_w, wu.at[own_rows]), (down_w, wd.at[own_rows]),
        (out_w.at[:, own_cols], owc.at[ow_rows]),
    ]
    loads = [pltpu.make_async_copy(a, b, in_sem.at[i]) for i, (a, b) in enumerate(loads)]
    for copy in loads:
        copy.start()

    pl.semaphore_wait(barrier, len(peers))

    def remote(src, dst, ss_, rs_, dev):
        return pltpu.make_async_remote_copy(
            src_ref=src, dst_ref=dst, send_sem=ss_, recv_sem=rs_, device_id=dev, device_id_type=MESH
        )

    started = []

    def go(copy):
        copy.start()
        started.append(copy)

    weights = ((up_w, wu), (down_w, wd))

    def sp_at(half, i, j):
        return ring(z, j) * 4 + ring(x, i) if half == 0 else ring(z, i) * 4 + ring(x, j)

    def piece(t, half, i, j, part):
        start, size = (0, 2 * QUARTER) if part is None else (part * QUARTER, QUARTER)
        first = sp_at(half, i, j) * SHARD + half * 2 * QUARTER + start
        return weights[t][1].at[pl.ds(pl.multiple_of(first, QUARTER), size)]

    FWD = (0, -1, 1, 2)

    def w_copy(t, half, slot, i, j, part, to, src=None):
        ref = piece(t, half, i, j, part)
        return remote(
            ref if src is None else src, ref, w_send.at[t, half, slot], w_recv.at[t, half, slot],
            (sp_at(half, *to), tp),
        )

    def w_go(*args, **kw):
        copy = w_copy(*args, **kw)
        copy.start()
        started.append(copy)

    def w_got(t, half, slot, i, j, part):
        w_copy(t, half, slot, i, j, part, (1, 0)).wait_recv()

    def w_second(t, half, n, src=None):
        i = FWD[n]
        w_go(t, half, 4 + 4 * n, i, 0, None, (0, 1), src=src)
        w_go(t, half, 5 + 4 * n, i, 0, None, (0, -1), src=src)

    def w_second_forward(t, half, n):
        i = FWD[n]
        w_got(t, half, 4 + 4 * n, i, -1, None)
        w_go(t, half, 6 + 4 * n, i, -1, 0, (0, 1))
        w_got(t, half, 5 + 4 * n, i, 1, None)
        w_go(t, half, 7 + 4 * n, i, 1, 1, (0, -1))

    def level0a(t):
        for half in range(2):
            src = weights[t][0].at[pl.ds(half * 2 * QUARTER, 2 * QUARTER)]
            w_go(t, half, 0, 0, 0, None, (1, 0), src=src)
            w_go(t, half, 1, 0, 0, None, (-1, 0), src=src)

    def level0b(t, half):
        src = weights[t][0].at[pl.ds(half * 2 * QUARTER, 2 * QUARTER)]
        w_second(t, half, 0, src=src)

    def level1p(t):
        for half in range(2):
            w_got(t, half, 0, -1, 0, None)
            w_go(t, half, 2, -1, 0, 0, (1, 0))
            w_got(t, half, 1, 1, 0, None)
            w_go(t, half, 3, 1, 0, 1, (-1, 0))

    def level1s(t):
        for half in range(2):
            w_second(t, half, 1)
            w_second(t, half, 2)

    def level1b(t):
        for half in range(2):
            w_second_forward(t, half, 0)

    def level2a(t, half):
        w_got(t, half, 2, 2, 0, 0)
        w_got(t, half, 3, 2, 0, 1)
        w_second(t, half, 3)

    def level2b(t, half):
        w_second_forward(t, half, 1)
        w_second_forward(t, half, 2)

    def level3(t, half):
        w_second_forward(t, half, 3)

    def level4(t, half, blocks):
        for n in blocks:
            w_got(t, half, 6 + 4 * n, FWD[n], 2, 0)
            w_got(t, half, 7 + 4 * n, FWD[n], 2, 1)

    mark("w0")
    level0a(0)

    def ow_cols(to):
        return pl.ds(pl.multiple_of(to * OC, OC), OC)

    def ow_rows_of(source, k=None):
        first, size = (0, 256) if k is None else (k * 128, 128)
        return pl.ds(pl.multiple_of(source * 256 + first, 128), size)

    near = (yp, ym)

    def ow_leg1(k, c):
        return remote(
            out_w.at[pl.ds(k * 128, 128), ow_cols(2 * y2 + c)], relay.at[k, c],
            ow_send.at[2 * k + c], ow_recv.at[2 * k + c], (sp, 2 * near[k] + core),
        )

    def ow_direct(k, c):
        return remote(
            out_w.at[:, ow_cols(2 * near[k] + c)], owc.at[ow_rows],
            ow_send.at[4 + 2 * k + c], ow_recv.at[4 + 2 * k + core], (sp, 2 * near[k] + c),
        )

    def ow_partner():
        return remote(
            out_w.at[:, ow_cols(partner)], owc.at[ow_rows], ow_send.at[8], ow_recv.at[8], (sp, partner)
        )

    def ow_leg2(k, c):
        return remote(
            relay.at[k, c], owc.at[ow_rows_of(2 * near[1 - k] + core, k)],
            ow_send.at[9 + 2 * k + c], ow_recv.at[9 + 2 * k + core], (sp, 2 * near[k] + c),
        )

    def ow_forward():
        for k in range(2):
            for c in range(2):
                ow_leg1(k, c).wait_recv()
                go(ow_leg2(k, c))

    def ow_wait():
        def landed(rows, sem):
            ref = owc.at[rows]
            remote(ref, ref, ow_send.at[8], ow_recv.at[sem], (sp, partner)).wait_recv()

        landed(ow_rows_of(partner), 8)
        for k in range(2):
            for c in range(2):
                landed(ow_rows_of(2 * near[1 - k] + c), 4 + 2 * k + c)
        for k in range(2):
            for c in range(2):
                landed(ow_rows_of(2 * y2 + c, k), 9 + 2 * k + c)

    for k in range(2):
        for c in range(2):
            go(ow_leg1(k, c))
    for k in range(2):
        for c in range(2):
            go(ow_direct(k, c))
    go(ow_partner())

    mark("loadwait")
    for copy in loads[:7]:
        copy.wait()

    mark("pass1")
    row_id = lax.broadcasted_iota(jnp.int32, (BLK, BLK), 0)
    col_id = lax.broadcasted_iota(jnp.int32, (BLK, BLK), 1)
    lower, upper = row_id >= col_id, row_id <= col_id
    run_state[...] = jnp.zeros_like(run_state)
    run_log[...] = jnp.zeros_like(run_log)
    sur_v[...] = jnp.concatenate([sur_t[0:HEADS, :], jnp.zeros((8 - HEADS, TOK), F32)], axis=0).T
    sums = tuple(
        jnp.concatenate([jnp.where(tri, 1.0, 0.0)] * 3, axis=1).astype(BF16) for tri in (lower, upper)
    )

    def split3(v):
        a = v.astype(BF16)
        rest = v - a.astype(F32)
        b = rest.astype(BF16)
        return jnp.concatenate([a, b, (rest - b.astype(F32)).astype(BF16)], axis=0)

    def pass1_block(d, blk):
        logits = (fon_v, frev_v)[d]
        mid_at, end_at = ((BLK // 2 - 1, BLK - 1), (BLK // 2, 0))[d]
        rows = pl.ds(pl.multiple_of(blk * BLK, BLK), BLK)
        key = glc_v[d : d + 1, :] / (1.0 + jnp.exp(logits[rows, :].astype(F32)))
        sg = sur_v[rows, :]
        sg = jnp.concatenate(
            [jnp.broadcast_to(sg[:, h : h + 1], (BLK, HD)) for h in range(HEADS)], axis=1
        )
        run = dot(sums[d], split3(jnp.log1p(-key) + sg))
        mid, end = run[mid_at : mid_at + 1, :], run[end_at : end_at + 1, :]
        away = mid - run
        rel[d, rows, :] = away
        k = key * jnp.exp(away)
        kr[d, rows, :] = k.astype(BF16)
        tail = (k * jnp.exp(end - mid)).astype(BF16)
        v = val_v[rows, :]
        new = [
            dot(v[:, h * HD : (h + 1) * HD], tail[:, h * HD : (h + 1) * HD], FIRST)
            for h in range(HEADS)
        ]
        em[d, blk] = jnp.broadcast_to(jnp.exp(mid), (8, CH))
        return end, new

    def pass1(step, carry):
        blocks = [
            (d, step * UNROLL + u if d == 0 else NB - 1 - (step * UNROLL + u))
            for u in range(UNROLL)
            for d in range(2)
        ]
        parts = [pass1_block(d, blk) for d, blk in blocks]
        for (d, blk), (end, new) in zip(blocks, parts):
            gone = run_log[d, 0:1, :]
            elx[d, blk] = jnp.broadcast_to(jnp.exp(gone), (8, CH))
            run_log[d] = jnp.broadcast_to(gone + end, (8, CH))
            decay = jnp.exp(end)
            for h in range(HEADS):
                hs = slice(h * HD, (h + 1) * HD)
                state = run_state[d, hs, :]
                sx[d, blk, hs, :] = state.astype(BF16)
                run_state[d, hs, :] = state * decay[:, hs] + new[h]
        return carry

    lax.fori_loop(0, NB // UNROLL, pass1, 0)

    mark("stsend")
    def store_state(ref, at, d, state, log):
        ref[at, d, 0:CH, :] = state.astype(BF16)
        high = log.astype(BF16).astype(F32)
        rest = log - high
        ref[at, d, CH:ST_ROWS, :] = jnp.concatenate(
            [high[:, :HD], high[:, HD:], rest[:, :HD], rest[:, HD:], jnp.zeros((12, HD), F32)], axis=0
        ).astype(BF16)

    def load_log(ref, at, d):
        tail = ref[at, d, CH:ST_ROWS, :].astype(F32)
        return [tail[h : h + 1, :] + tail[2 + h : 3 + h, :] for h in range(HEADS)]

    for d in range(2):
        store_state(row_in, x, d, run_state[d], run_log[d, 0:1, :])

    def row_copy(o):
        return remote(
            row_in.at[x], row_in.at[x], st_send.at[o - 1], st_recv.at[o - 1],
            (z * 4 + ring(x, o), tp),
        )

    def row_got(o):
        ref = row_in.at[ring(x, -o)]
        remote(ref, ref, st_send.at[o - 1], st_recv.at[o - 1], (z * 4 + ring(x, o), tp)).wait_recv()

    def col_copy(o):
        ref = col_in.at[z, lax.div(z + o, 4)]
        return remote(
            ref, ref, st_send.at[o + 2], st_recv.at[o + 2], (ring(z, o) * 4 + x, tp)
        )

    def col_got(o):
        ref = col_in.at[ring(z, -o), lax.div(z + 4 - o, 4) * -1 + 1]
        remote(ref, ref, st_send.at[o + 2], st_recv.at[o + 2], (ring(z, o) * 4 + x, tp)).wait_recv()

    for o in (1, 3, 2):
        copy = row_copy(o)
        copy.start()
        started.append(copy)
    mark("l0b")
    level0b(0, 0)
    level0b(0, 1)

    def pass2_block(blk):
        rows = pl.ds(pl.multiple_of(blk * BLK, BLK), BLK)
        v = val_v[rows, :]
        q = que_v[rows, :].astype(F32)
        q = q * sigmoid(q) * (HD ** -0.5)
        for d in range(2):
            qd[d, rows, :] = (q * jnp.exp(-rel[d, rows, :])).astype(BF16)
        for h in range(HEADS):
            hs = slice(h * HD, (h + 1) * HD)
            fwd = dot(qd[0, rows, hs], kr[0, rows, hs], LAST)
            bwd = dot(qd[1, rows, hs], kr[1, rows, hs], LAST)
            score = jnp.where(lower, fwd, 0.0) + jnp.where(upper, bwd, 0.0)
            o_v[rows, hs] = dot(score.astype(BF16), v[:, hs])

    def by_blocks(body):
        def step(i, carry):
            for u in range(UNROLL):
                body(i * UNROLL + u)
            return carry

        lax.fori_loop(0, NB // UNROLL, step, 0)

    mark("pass2")
    by_blocks(pass2_block)


    mark("owfwd")
    ow_forward()
    level1p(0)
    mark("roww")
    for o in (1, 3, 2):
        row_got(o)
    mark("rowc")
    for d in range(2):
        state = jnp.zeros((CH, HD), F32)
        log = [jnp.zeros((1, HD), F32)] * HEADS
        for j in range(4) if d == 0 else range(3, -1, -1):
            own = load_log(row_in, j, d)
            state = jnp.concatenate(
                [
                    state[h * HD : (h + 1) * HD] * jnp.exp(own[h])
                    + row_in[j, d, h * HD : (h + 1) * HD, :].astype(F32)
                    for h in range(HEADS)
                ],
                axis=0,
            )
            log = [log[h] + own[h] for h in range(HEADS)]
        store_state(col_in, z, d, state, jnp.concatenate(log, axis=1))
    for o in (1, 3, 2):
        copy = col_copy(o)
        copy.start()
        started.append(copy)
    sin[...] = jnp.zeros_like(sin)
    level1s(0)
    mark("colw")
    for o in (1, 3, 2):
        col_got(o)
    mark("combine")

    def chain(ref, at):
        def body(i, carry):
            d = lax.div(i + 4 - at, 4)
            j = (1 - d) * i + d * (3 + at - i)
            own = load_log(ref, j, d)
            for h in range(HEADS):
                hs = slice(h * HD, (h + 1) * HD)
                sin[d, hs, :] = sin[d, hs, :] * jnp.exp(own[h]) + ref[j, d, hs, :].astype(F32)
            return carry

        lax.fori_loop(0, 3, body, 0)

    chain(col_in, z)
    chain(row_in, x)

    for copy in loads[6:10]:
        if copy is not loads[6]:
            copy.wait()

    def pass3_block(blk):
        rows = pl.ds(pl.multiple_of(blk * BLK, BLK), BLK)
        for h in range(HEADS):
            hs = slice(h * HD, (h + 1) * HD)
            mixed = o_v[rows, hs]
            for d in range(2):
                qs = (qd[d, rows, hs].astype(F32) * em[d, blk, 0:1, hs]).astype(BF16)
                state = sx[d, blk, hs, :].astype(F32) + elx[d, blk, 0:1, hs] * sin[d, hs, :]
                mixed = mixed + dot(qs, state.astype(BF16), LAST)
            norm = mixed * lax.rsqrt(jnp.mean(mixed * mixed, axis=-1, keepdims=True) + EPS)
            g = gat_v[rows, hs].astype(F32)
            ga[tp, rows, hs] = (norm * hg_v[0:1, :] * (g * sigmoid(g))).astype(BF16)

    mark("pass3")
    by_blocks(pass3_block)

    HALF = TOK // 2

    class Gather:
        def __init__(self, buf, send_sem, recv_sem):
            self.buf, self.ss, self.rs = buf, send_sem, recv_sem

        def copy(self, k, slot, part, to):
            ref = self.buf.at[slot]
            if part is not None:
                ref = self.buf.at[slot, pl.ds(part * HALF, HALF)]
            return remote(ref, ref, self.ss.at[k], self.rs.at[k], (sp, to))

        def go(self, *args):
            copy = self.copy(*args)
            copy.start()
            started.append(copy)

        def got(self, k, slot, part):
            self.copy(k, slot, part, partner).wait_recv()

        def own(self):
            right, left = 2 * yp + core, 2 * ym + core
            self.go(0, tp, 0, right)
            self.go(3, tp, 1, left)
            self.go(6, tp, None, partner)
            self.go(1, tp, 1, right)
            self.go(2, tp, 0, left)

        def forward(self):
            left, right = 2 * ym + core, 2 * yp + core
            self.got(0, left, 0)
            self.go(4, left, 0, right)
            self.go(7, left, 0, partner)
            self.got(3, right, 1)
            self.go(5, right, 1, left)
            self.go(8, right, 1, partner)

        def from_side(self):
            left, right = 2 * ym + core, 2 * yp + core
            self.got(1, left, 1)
            self.go(9, left, 1, partner)
            self.got(2, right, 0)
            self.go(10, right, 0, partner)

        def from_far(self):
            far = 2 * y2 + core
            self.got(4, far, 0)
            self.go(11, far, 0, partner)
            self.got(5, far, 1)
            self.go(12, far, 1, partner)

        def other_core(self, chip):
            block = 2 * chip + other
            for k, part in {id(ym): ((7, 0), (9, 1)), id(yp): ((8, 1), (10, 0)), id(y2): ((11, 0), (12, 1))}[
                id(chip)
            ]:
                self.got(k, block, part)

    gathered = Gather(ga, g_send, g_recv)
    mark("gown")
    gathered.own()

    mark("owwait")
    for copy in loads[10:13]:
        copy.wait()
    ow_wait()

    def project(block, first=False):
        def tile(n, carry):
            cols = pl.ds(pl.multiple_of(n * 256, 256), 256)
            part = dot(ga[block], owc[pl.ds(pl.multiple_of(block * 256, 256), 256), cols])
            att[:, cols] = part if first else att[:, cols] + part
            return carry

        lax.fori_loop(0, OC // 256, tile, 0)

    mark("proj0")
    project(tp, True)
    mark("gpart")
    gathered.got(6, partner, None)
    project(partner)
    mark("lev2a_0")
    level1b(0)
    level2a(0, 0)
    level2a(0, 1)
    mark("gfwd")
    gathered.forward()
    mark("gside")
    gathered.from_side()
    mark("proj2")
    project(2 * ym + core)
    project(2 * yp + core)
    mark("lev2b_0")
    level2b(0, 0)
    level2b(0, 1)
    level0a(1)
    mark("gpart2")
    gathered.other_core(ym)
    project(2 * ym + other)
    gathered.other_core(yp)
    project(2 * yp + other)
    mark("gfar")
    gathered.from_far()
    project(2 * y2 + core)
    gathered.other_core(y2)
    project(2 * y2 + other)

    TILE = 128

    def middle(i, carry):
        rows = pl.ds(pl.multiple_of(i * TILE, TILE), TILE)
        xa[tp, rows, :] = (res_v[rows, :].astype(F32) + att[rows, :]).astype(BF16)
        return carry

    mark("middle")
    lax.fori_loop(0, TOK // TILE, middle, 0)

    spread = Gather(xa, x_send, x_recv)
    spread.own()
    def scale(chip, c, first=False):
        block = 2 * chip + c
        gain = ng_v[:, pl.ds(pl.multiple_of(block * OC, OC), OC)]
        cols = pl.ds(pl.multiple_of(c * OC, OC), OC)

        def body(i, carry):
            rows = pl.ds(pl.multiple_of(i * TILE, TILE), TILE)
            v = xa[block, rows, :].astype(F32)
            sq = v * v
            sq = (sq[:, 0:128] + sq[:, 128:256]) + (sq[:, 256:384] + sq[:, 384:512])
            ss[rows, :] = sq if first else ss[rows, :] + sq
            xg[rows, cols] = (v * gain).astype(BF16)
            return carry

        lax.fori_loop(0, TOK // TILE, body, 0)

    def lift(chip, first=False):
        def tile(n, carry):
            cols = pl.ds(pl.multiple_of(n * 256, 256), 256)
            part = dot(xg[...], wu[pl.ds(pl.multiple_of(chip * 2 * OC, 2 * OC), 2 * OC), cols])
            acc[:, cols] = part if first else acc[:, cols] + part
            return carry

        lax.fori_loop(0, FFL // 256, tile, 0)

    def lift_one(chip, c):
        def tile(n, carry):
            cols = pl.ds(pl.multiple_of(n * 256, 256), 256)
            rows = pl.ds(pl.multiple_of((chip * 2 + c) * OC, OC), OC)
            part = dot(xg[:, pl.ds(pl.multiple_of(c * OC, OC), OC)], wu[rows, cols])
            acc[:, cols] = acc[:, cols] + part
            return carry

        lax.fori_loop(0, FFL // 256, tile, 0)

    mark("scale0")
    scale(y, core, True)
    spread.got(6, partner, None)
    scale(y, other)
    mark("lev3_0")
    level3(0, 0)
    level3(0, 1)
    level0b(1, 0)
    level0b(1, 1)
    mark("xfwd")
    spread.forward()
    mark("lev1a_1")
    level1p(1)
    level1s(1)
    mark("lev4_0")
    level4(0, 0, range(4))
    level4(0, 1, range(4))
    mark("lift0")
    lift(y, True)
    mark("xside")
    spread.from_side()
    mark("lift1")
    scale(ym, core)
    lift_one(ym, core)
    spread.other_core(ym)
    scale(ym, other)
    lift_one(ym, other)
    mark("lev1_1")
    level1b(1)
    mark("lift2")
    scale(yp, core)
    spread.other_core(yp)
    scale(yp, other)
    lift(yp)
    mark("lev2a_1")
    level2a(1, 1)
    mark("xfar")
    spread.from_far()
    mark("lift3")
    scale(y2, core)
    lift_one(y2, core)
    spread.other_core(y2)
    scale(y2, other)
    lift_one(y2, other)

    def activate(i, carry):
        rows = pl.ds(pl.multiple_of(i * TILE, TILE), TILE)
        total = jnp.sum(ss[rows, :], axis=-1, keepdims=True)
        v = jnp.maximum(acc[rows, :] * lax.rsqrt(total / D + EPS), 0.0)
        hid[rows, :] = (v * v).astype(BF16)
        return carry

    mark("act")
    lax.fori_loop(0, TOK // TILE, activate, 0)


    SHARDS = (
        (1, 0), (0, 0), (1, 1), (1, -1), (1, 2),
        (0, 1), (0, -1), (0, 2), (2, 2), (2, 1), (2, -1),
    )

    class Step:
        def __init__(self, n):
            self.n = n
            dx, dz = SHARDS[n]
            self.single = n >= 5
            self.dx = dx % 2
            zs = ring(z, dz)
            column = lax.rem(x + dx, 2)
            self.keep = lax.div(ring(x, dx), 2) == core
            self.kept = jnp.where(self.keep, 1, 0)
            self.slot = self.dx * 4 + zs
            self.first = zs * 4 + column
            self.delta = lax.rem(zs + 4 - y, 4)
            self.odd = lax.rem(self.delta, 2) == 1
            self.far = self.delta == 2
            self.k = lax.div(self.delta, 2)
            self.to = 2 * lax.rem(y + self.delta, 4) + core

        def chip(self):
            return remote(
                pp.at[0, self.slot], d2r.at[self.slot], c_send.at[self.n], c_recv.at[self.n], (sp, partner)
            )

        def half(self, k):
            return pl.ds(pl.multiple_of(k * HALF, HALF), HALF)

        def out_far(self, k):
            return remote(
                pp.at[1, self.slot, self.half(k)], ra.at[self.slot], r_send.at[self.n, k],
                r_recv.at[self.n], (sp, 2 * (yp, ym)[k] + core),
            )

        def out_near(self, k):
            return remote(
                pp.at[1, self.slot, self.half(k)], ee.at[self.k, self.dx, self.half(k)],
                e_send.at[self.n, k], e_recv.at[self.k, self.dx, k], (sp, self.to),
            )

        def compute(self, *others):
            mark("comp%d" % self.n)

            def part(j, carry):
                i, first, slot = j, self.first, self.slot
                if others:
                    i = self.kept
                    first = first + j * (others[0].first - first)
                    slot = slot + j * (others[0].slot - slot)
                elif self.single:
                    i = self.kept
                first = (first + 2 * (other + i * (core - other))) * SHARD
                rows = wd[pl.ds(pl.multiple_of(first, SHARD), SHARD), :]
                pp[i, slot] = dot(hid[...], rows, LAST).astype(BF16)
                if others:
                    for g, step in enumerate((self, *others)):
                        pl.when(jnp.logical_and(i == 0, j == g))(lambda step=step: step.chip().start())
                else:
                    pl.when(i == 0)(lambda: self.chip().start())
                return carry

            if self.single and not others:
                part(0, 0)
            else:
                lax.fori_loop(0, 2, part, 0)

        def when_kept(self, body):
            if self.single:
                pl.when(self.keep)(body)
            else:
                body()

        def chip_sum(self):
            mark("cs%d" % self.n)
            self.when_kept(self.chip_sum_kept)

        def chip_sum_kept(self):
            self.chip().wait_recv()

            def add(i, carry):
                rows = pl.ds(pl.multiple_of(i * TILE, TILE), TILE)
                total = pp[1, self.slot, rows, :].astype(F32) + d2r[self.slot, rows, :].astype(F32)
                pp[1, self.slot, rows, :] = total.astype(BF16)
                return carry

            lax.fori_loop(0, TOK // TILE, add, 0)

            @pl.when(self.far)
            def _():
                self.out_far(0).start()
                self.out_far(1).start()

            @pl.when(self.odd)
            def _():
                self.out_near(1 - self.k).start()

        def join(self):
            mark("jn%d" % self.n)
            self.when_kept(self.join_kept)

        def join_kept(self):
            @pl.when(self.odd)
            def _():
                remote(
                    ra.at[self.slot], ra.at[self.slot], r_send.at[self.n, 0], r_recv.at[self.n],
                    (sp, self.to),
                ).wait_recv()

                def add(i, carry):
                    rows = pl.ds(pl.multiple_of(self.k * HALF + i * TILE, TILE), TILE)
                    got = ra[self.slot, pl.ds(pl.multiple_of(i * TILE, TILE), TILE), :]
                    total = pp[1, self.slot, rows, :].astype(F32) + got.astype(F32)
                    pp[1, self.slot, rows, :] = total.astype(BF16)
                    return carry

                lax.fori_loop(0, HALF // TILE, add, 0)
                self.out_near(self.k).start()

        def drain(self):
            if self.single:
                pl.when(jnp.logical_not(self.keep))(lambda: self.chip().wait_send())
            else:
                self.chip().wait_send()
            self.when_kept(self.drain_kept)

        def drain_kept(self):
            @pl.when(self.far)
            def _():
                self.out_far(0).wait_send()
                self.out_far(1).wait_send()

            @pl.when(self.odd)
            def _():
                self.out_near(1 - self.k).wait_send()
                self.out_near(self.k).wait_send()

    steps = [Step(n) for n in range(11)]
    steps[0].compute()
    steps[5].compute(steps[6])
    steps[0].chip_sum()
    steps[5].chip_sum()
    mark("lev2_1")
    level2b(1, 0)
    level2a(1, 0)
    level2b(1, 1)
    steps[2].compute()
    steps[6].chip_sum()
    steps[3].compute()
    mark("w7")
    level4(1, 0, (0,))
    level4(1, 1, (0,))
    steps[7].compute()
    steps[2].chip_sum()
    steps[3].chip_sum()
    steps[7].chip_sum()
    steps[1].compute()
    steps[1].chip_sum()
    mark("w4")
    level4(1, 0, (1, 2))
    level3(1, 1)
    steps[4].compute()
    steps[0].join()
    steps[7].join()
    steps[4].chip_sum()
    mark("w30")
    level3(1, 0)
    steps[2].join()
    steps[5].join()
    steps[6].join()
    steps[3].join()
    mark("w5")
    level4(1, 1, (1, 2))
    steps[9].compute(steps[10])
    steps[9].chip_sum()
    steps[10].chip_sum()
    steps[4].join()
    mark("w8")
    level4(1, 0, (3,))
    level4(1, 1, (3,))
    steps[8].compute()
    steps[8].chip_sum()
    steps[1].join()
    for n in (9, 10, 8):
        steps[n].join()
    mark("ewait")

    for dx in range(2):
        slot = dx * 4 + y
        for k in range(2):
            for half in range(2):
                rows = pl.ds(half * HALF, HALF)
                remote(
                    ee.at[k, dx, rows], ee.at[k, dx, rows], e_send.at[0, 0], e_recv.at[k, dx, half],
                    (sp, partner),
                ).wait_recv()
        cols = pl.ds(pl.multiple_of(lax.rem(x + dx, 2) * SHARD, SHARD), SHARD)

        def finish(i, carry):
            rows = pl.ds(pl.multiple_of(i * TILE, TILE), TILE)
            total = pp[1, slot, rows, :].astype(F32)
            total = total + (ee[0, dx, rows, :].astype(F32) + ee[1, dx, rows, :].astype(F32))
            out[rows, cols] = (xa[tp, rows, cols].astype(F32) + total).astype(BF16)
            return carry

        lax.fori_loop(0, TOK // TILE, finish, 0)
    mark("final")
    for copy in started:
        copy.wait_send()
    for step in steps:
        step.drain()
    mark(None)


def per_device(
    residual, values, forget_onward, forget_reverse, surge_log_decay, gate_limit_complement,
    readout_query, output_gate, head_norm_gain, output_weight, mixer_norm_gain, up_weight,
    down_weight,
):
    any_spec = pl.BlockSpec(memory_space=pl.ANY)
    vmem, dma = pltpu.VMEM, pltpu.SemaphoreType.DMA
    scratch = [
        vmem((TOK, OC), BF16), vmem((TOK, CH), BF16), vmem((TOK, CH), BF16), vmem((TOK, CH), BF16),
        vmem((8, TOK), F32), vmem((TOK, 8), F32), vmem((2, CH), F32), vmem((TOK, CH), BF16), vmem((TOK, CH), BF16),
        vmem((1, HD), F32), vmem((1, D), F32),
        vmem((D, FFL), BF16), vmem((D, FFL), BF16), vmem((2048, OC), BF16),
        vmem((8, TOK, CH), BF16), vmem((8, TOK, OC), BF16),
        vmem((2, TOK, CH), BF16), vmem((2, TOK, CH), BF16), vmem((2, NB, CH, HD), BF16),
        vmem((2, NB, 8, CH), F32), vmem((2, NB, 8, CH), F32),
        vmem((2, CH, HD), F32), vmem((2, 8, CH), F32),
        vmem((4, 2, ST_ROWS, HD), BF16), vmem((4, 2, ST_ROWS, HD), BF16), vmem((2, CH, HD), F32),
        vmem((TOK, CH), F32), vmem((TOK, OC), F32),
        vmem((TOK, 2 * OC), BF16), vmem((TOK, HD), F32), vmem((TOK, FFL), F32), vmem((TOK, FFL), BF16),
        vmem((2, 8, TOK, SHARD), BF16), vmem((8, TOK, SHARD), BF16),
        vmem((8, TOK // 2, SHARD), BF16), vmem((2, 2, TOK, SHARD), BF16),
        vmem((2, 2, 128, OC), BF16), vmem((2, TOK, CH), F32),
        dma((13,)), dma((2, 2, 20)), dma((2, 2, 20)), dma((13,)), dma((13,)), dma((6,)), dma((6,)),
        dma((13,)), dma((13,)), dma((13,)), dma((13,)), dma((11,)), dma((11,)), dma((11, 2)), dma((11,)),
        dma((11, 2)), dma((2, 2, 2)),
    ]
    return pl.pallas_call(
        kernel,
        out_shape=pltpu.VMEM((TOK, OC), BF16),
        in_specs=[any_spec] * 13,
        out_specs=pl.BlockSpec(memory_space=pltpu.VMEM),
        scratch_shapes=scratch,
        compiler_params=pltpu.CompilerParams(
            collective_id=0, has_side_effects=True, vmem_limit_bytes=66_000_000
        ),
        name="layer",
    )(
        residual, values, forget_onward, forget_reverse, surge_log_decay.T, gate_limit_complement,
        readout_query, output_gate, head_norm_gain.reshape(1, HD), output_weight,
        mixer_norm_gain.reshape(1, D), up_weight, down_weight,
    )


def solution(mesh):
    both = P("sp", "tp")
    placed = (
        both, both, both, both, both, P(None, "tp"), both, both, P(), P("tp", None), P(), both, both,
    )
    return jax.shard_map(
        per_device, mesh=mesh, in_specs=placed, out_specs=both, check_vma=False
    )
```
